512 devices in a mesh: sp: 64 (over z, y), tp: 8 (over x, core).
Axes of the slice: x: 4, y: 8, z: 8, core: 2. Of those that a mesh axis runs over, the one named last changes fastest.
Arguments:
- tokens: bfloat16 [12288, 4096], P('sp'), may hold values from -6 to 6
- norm_gain: float32 [4096], replicated, may hold values from 0.1 to 1.9
- conv_value: bfloat16 [4096, 2048], P('sp', 'tp'), may hold values from -0.09375 to 0.09375
- conv_gate: bfloat16 [4096, 2048], P('sp', 'tp'), may hold values from -0.09375 to 0.09375
- state_feed: bfloat16 [4096, 2048], P('sp', 'tp'), may hold values from -0.09375 to 0.09375
- conv_taps: float32 [31, 2048], P(None, 'tp'), may hold values from -1 to 1
- chan_gain: float32 [2048], replicated, may hold values from 0.1 to 1.9
- chan_shift: float32 [2048], replicated, may hold values from -3 to 3
- conv_project: bfloat16 [2048, 4096], P('sp', 'tp'), may hold values from -0.125 to 0.125
- decay_rate: float32 [128, 64], P('tp'), may hold values from 0.1 to 3
- frequency: float32 [128, 64], P('tp'), may hold values from 0.1 to 3
- input_real: float32 [128, 64, 16], P('tp'), may hold values from -0.01953125 to 0.01953125
- input_imag: float32 [128, 64, 16], P('tp'), may hold values from -0.01953125 to 0.01953125
- output_real: float32 [128, 16, 64], P('tp'), may hold values from -0.5 to 0.5
- output_imag: float32 [128, 16, 64], P('tp'), may hold values from -0.5 to 0.5
- skip_gain: float32 [2048], P('tp'), may hold values from -3 to 3
- state_value: bfloat16 [2048, 4096], P('sp', 'tp'), may hold values from -0.125 to 0.125
- state_gate: bfloat16 [2048, 4096], P('sp', 'tp'), may hold values from -0.125 to 0.125
- initial_state: float32 [2, 128, 64], P(None, 'tp'), may hold values from -5 to 5
Outputs:
- mixer_out: bfloat16 [12288, 4096], P('sp', 'tp')
- final_state: float32 [2, 128, 64], P(None, 'tp')
The draws below stay inside these ranges and needn't reach their ends.
All inputs are finite; a program needn't handle non-finite values.
Results may differ from the reference program's by a relative error of at most 0.0085.
Values may be sent and summed in bfloat16 or wider, within the bound.
A program may use at most 64 MiB of HBM per device.

```python
import math
import jax
import jax.numpy as jnp
from jax import lax

D = 4096
CH = 2048
GROUP = 16
STATE = 64
KERNEL = 31
TOKENS = 12288
GROUPS = 128


def steps_of(rng, extent, split, low, largest):
    def one(dim, shards_of):
        steps = jax.random.uniform(jax.random.fold_in(jax.random.fold_in(rng, 6), dim), (shards_of,), jnp.float32, low / len(split), largest / len(split))
        return jnp.repeat(jnp.exp(steps), extent[dim] // shards_of).reshape((-1,) + (1,) * (len(extent) - dim - 1))

    factor_of = one(*split[0])
    for cut in split[1:]:
        factor_of = factor_of * one(*cut)
    return factor_of


def bell_draw(rng, extent, scale, bound, split=(), held_as=jnp.bfloat16):
    result = jax.random.normal(rng, extent, jnp.float32) * scale
    if len(split) > 0:
        result = steps_of(rng, extent, split, -0.22, 0.18) * result
    return jnp.clip(result, min=-bound, max=bound).astype(held_as)


def setup_inputs(seed: int = 0) -> dict:
    key_of = jax.random.split(jax.random.key(seed), 20)
    tokens = bell_draw(key_of[0], (TOKENS, D), 1.0, 6.0, ((0, 64),))
    norm_gain = jnp.clip(1.0 + 0.18 * jax.random.normal(key_of[1], (D,), jnp.float32), 0.1, 1.9)
    conv_value = bell_draw(key_of[2], (D, CH), D ** -0.5, 0.09375, ((0, 64), (1, 8)))
    conv_gate = bell_draw(key_of[3], (D, CH), D ** -0.5, 0.09375, ((0, 64), (1, 8)))
    state_feed = bell_draw(key_of[4], (D, CH), D ** -0.5, 0.09375, ((0, 64), (1, 8)))
    conv_taps = bell_draw(key_of[5], (KERNEL, CH), KERNEL ** -0.5, 1.0, ((1, 8),), jnp.float32)
    chan_gain = jnp.clip(1.0 + 0.18 * jax.random.normal(key_of[6], (CH,), jnp.float32), 0.1, 1.9)
    chan_shift = bell_draw(key_of[7], (CH,), 0.5, 3.0, (), jnp.float32)
    conv_project = bell_draw(key_of[8], (CH, D), CH ** -0.5, 0.125, ((0, 64), (1, 8)))
    decay_rate = jnp.clip(jnp.exp(math.log(3.0) - 3.4011974 * jax.random.uniform(key_of[9], (GROUPS, STATE), jnp.float32) ** steps_of(key_of[9], (GROUPS, STATE), ((0, 8),), -0.2, 0.2)), 0.1, 3.0)
    frequency = jnp.clip(0.1 + 2.9 * jax.random.uniform(key_of[10], (GROUPS, STATE), jnp.float32) ** steps_of(key_of[10], (GROUPS, STATE), ((0, 8),), -0.2, 0.2), 0.1, 3.0)
    input_real = bell_draw(key_of[11], (GROUPS, STATE, GROUP), (8 * TOKENS) ** -0.5, 0.01953125, ((0, 8),), jnp.float32)
    input_imag = bell_draw(key_of[12], (GROUPS, STATE, GROUP), (8 * TOKENS) ** -0.5, 0.01953125, ((0, 8),), jnp.float32)
    output_real = bell_draw(key_of[13], (GROUPS, GROUP, STATE), (2 * STATE) ** -0.5, 0.5, ((0, 8),), jnp.float32)
    output_imag = bell_draw(key_of[14], (GROUPS, GROUP, STATE), (2 * STATE) ** -0.5, 0.5, ((0, 8),), jnp.float32)
    skip_gain = bell_draw(key_of[15], (CH,), 0.5, 3.0, ((0, 8),), jnp.float32)
    state_value = bell_draw(key_of[16], (CH, D), CH ** -0.5, 0.125, ((0, 64), (1, 8)))
    state_gate = bell_draw(key_of[17], (CH, D), CH ** -0.5, 0.125, ((0, 64), (1, 8)))
    initial_state = bell_draw(key_of[18], (2, GROUPS, STATE), 1.0, 5.0, ((1, 8),), jnp.float32)
    return dict(tokens=tokens, norm_gain=norm_gain, conv_value=conv_value, conv_gate=conv_gate, state_feed=state_feed, conv_taps=conv_taps, chan_gain=chan_gain, chan_shift=chan_shift, conv_project=conv_project, decay_rate=decay_rate, frequency=frequency, input_real=input_real, input_imag=input_imag, output_real=output_real, output_imag=output_imag, skip_gain=skip_gain, state_value=state_value, state_gate=state_gate, initial_state=initial_state)


def reference(tokens, norm_gain, conv_value, conv_gate, state_feed, conv_taps, chan_gain, chan_shift, conv_project, decay_rate, frequency, input_real, input_imag, output_real, output_imag, skip_gain, state_value, state_gate, initial_state):
    highest = lax.Precision.HIGHEST
    floats = tokens.astype(jnp.float32)
    normed = (floats * lax.rsqrt(lax.optimization_barrier(jnp.mean(floats * floats, axis=1, keepdims=True)) + 1e-06) * norm_gain).astype(jnp.bfloat16)
    value_in = jnp.dot(normed, conv_value, preferred_element_type=jnp.float32)
    gate_in = jnp.dot(normed, conv_gate, preferred_element_type=jnp.float32)
    gated_linear = (value_in * jax.nn.sigmoid(gate_in)).astype(jnp.bfloat16)
    kernel = conv_taps.shape[0]
    length = tokens.shape[0]
    padded = jnp.pad(gated_linear.astype(jnp.float32), ((kernel - 1, 0), (0, 0)))
    conv_sum = jnp.zeros(gated_linear.shape, jnp.float32)
    for offset in range(kernel):
        conv_sum = conv_sum + conv_taps[offset] * padded[offset:offset + length]
    conv_out = conv_sum.astype(jnp.bfloat16)
    conv_full = conv_out.astype(jnp.float32)
    row_mean = lax.optimization_barrier(jnp.mean(conv_full, axis=1, keepdims=True))
    centred = conv_full - row_mean
    variance = lax.optimization_barrier(jnp.mean(centred * centred, axis=1, keepdims=True))
    conv_act = jax.nn.silu(centred * lax.rsqrt(variance + 1e-05) * chan_gain + chan_shift).astype(jnp.bfloat16)
    conv_branch = jnp.dot(conv_act, conv_project, preferred_element_type=jnp.float32)
    state_drive = jnp.dot(normed, state_feed, preferred_element_type=jnp.float32).astype(jnp.bfloat16)
    groups, state_size, group_size = input_real.shape
    rate_real = -decay_rate / TOKENS
    magnitude = jnp.exp(rate_real)
    step_real = magnitude * jnp.cos(frequency)
    step_imag = magnitude * jnp.sin(frequency)
    modulus = rate_real * rate_real + frequency * frequency
    lift_real = step_real - 1.0
    factor_real = (lift_real * rate_real + step_imag * frequency) / modulus
    factor_imag = (step_imag * rate_real - lift_real * frequency) / modulus
    drive_real = factor_real[..., None] * input_real - factor_imag[..., None] * input_imag
    drive_imag = factor_real[..., None] * input_imag + factor_imag[..., None] * input_real
    grouped = state_drive.astype(jnp.float32).reshape(length, groups, group_size)

    def advance(carried, token_in):
        prior_real, prior_imag = carried
        pushed_real = jnp.einsum('gph,gh->gp', drive_real, token_in, precision=highest)
        pushed_imag = jnp.einsum('gph,gh->gp', drive_imag, token_in, precision=highest)
        next_real = step_real * prior_real - step_imag * prior_imag + pushed_real
        next_imag = step_real * prior_imag + step_imag * prior_real + pushed_imag
        emitted = jnp.einsum('ghp,gp->gh', output_real, next_real, precision=highest) - jnp.einsum('ghp,gp->gh', output_imag, next_imag, precision=highest)
        return ((next_real, next_imag), emitted)
    (last_real, last_imag), responses = lax.scan(advance, (initial_state[0], initial_state[1]), grouped)
    response = responses.reshape(length, groups * group_size) + skip_gain * state_drive.astype(jnp.float32)
    activated = jax.nn.gelu(response).astype(jnp.bfloat16)
    state_values = jnp.dot(activated, state_value, preferred_element_type=jnp.float32)
    state_gates = jnp.dot(activated, state_gate, preferred_element_type=jnp.float32)
    mixer_out = (conv_branch + state_values * jax.nn.sigmoid(state_gates)).astype(jnp.bfloat16)
    final_state = jnp.stack([last_real, last_imag])
    return (mixer_out, final_state)
```

```python
import jax
import jax.numpy as jnp
from jax import lax
from jax.experimental import pallas as pl
from jax.experimental.pallas import tpu as pltpu
from jax.sharding import PartitionSpec as P

BF, F32 = jnp.bfloat16, jnp.float32
HIGHEST = lax.Precision.HIGHEST
MESH = pl.DeviceIdType.MESH
SIDE = 8
CHIPS = 4
NT = (((1,), (1,)), ((), ()))


def hops(direction, half):
    return SIDE // 2 if (direction > 0) == (half == 0) else SIDE // 2 - 1


SLOTS = [
    (direction, half, k)
    for direction in (1, -1)
    for half in (0, 1)
    for k in range(hops(direction, half))
]
SLOT_OF = {slot: at for at, slot in enumerate(SLOTS)}


def rotate(first_real, first_imag, second_real, second_imag):
    return (
        first_real * second_real - first_imag * second_imag,
        first_real * second_imag + first_imag * second_real,
    )


def iota(shape, dim):
    return lax.broadcasted_iota(jnp.int32, shape, dim)


def kernel(
    tokens, norm_gain, conv_value, conv_gate, state_feed, conv_taps, chan_gain, chan_shift,
    conv_project, decay_rate, frequency, input_real, input_imag, output_real, output_imag,
    skip_gain, state_value, state_gate, initial_state,
    out, final_state,
    ws1, wc1, ws2, wc2, raw, normed, result,
    power_r, power_i, undo_r, undo_i, drive_r, drive_i, emit, feed, scaled, summed, states,
    rows, finals, totals, gated, halo, padded, shifted, conv_all, act_all, conv_act, mixed,
    load_sem, ring_send, ring_recv, scan_send, scan_recv, halo_sem, tp_send, tp_recv,
):
    seq = lax.axis_index("sp")
    t = lax.axis_index("tp")
    z, y = seq // SIDE, seq % SIDE
    chip, core = t // 2, t % 2
    length = tokens.shape[0]
    groups, size, wide = input_real.shape
    flat = groups * size
    width = groups * wide

    def device(zz, yy, tt):
        return {"sp": zz * SIDE + yy, "tp": tt}

    def step_to(at, by, count):
        return lax.rem(at + by + count, count)

    def remote(src, dst, send, recv, to):
        return pltpu.make_async_remote_copy(
            src_ref=src, dst_ref=dst, send_sem=send, recv_sem=recv, device_id=to, device_id_type=MESH
        )

    events = []
    sent = []

    def at(time, fn):
        events.append((time, len(events), fn))

    loads = {}

    def load(name, index, src, dst):
        loads[name] = pltpu.make_async_copy(src, dst, load_sem.at[index])
        loads[name].start()

    load("ws1", 0, state_feed, ws1.at[z, y])
    load("wc1v", 1, conv_value, wc1.at[0, z, y])
    load("wc1g", 2, conv_gate, wc1.at[1, z, y])
    load("ws2v", 3, state_value, ws2.at[0, z, y])
    load("ws2g", 4, state_gate, ws2.at[1, z, y])
    load("wc2", 5, conv_project, wc2.at[z, y])
    load("raw", 6, tokens, raw)

    barrier = pltpu.get_barrier_semaphore()
    here = {"z": z, "y": y}
    following = lax.rem(seq + 1, SIDE * SIDE)
    preceding = lax.rem(seq + SIDE * SIDE - 1, SIDE * SIDE)
    partners = []
    for d in range(1, SIDE):
        partners.append(device(z, step_to(y, d, SIDE), t))
        partners.append(device(step_to(z, d, SIDE), y, t))
    for d in range(1, 2 * CHIPS):
        partners.append(device(z, y, step_to(t, d, 2 * CHIPS)))
    partners.append({"sp": following, "tp": t})
    partners.append({"sp": preceding, "tp": t})
    for partner in partners:
        pl.semaphore_signal(barrier, inc=1, device_id=partner, device_id_type=MESH)
    pl.semaphore_wait(barrier, len(partners))

    def ring(number, axis, block, start, tau, ready):
        position = here[axis]

        def neighbour(direction):
            beside = step_to(position, direction, SIDE)
            return device(beside, y, t) if axis == "z" else device(z, beside, t)

        def copy(direction, half, k, source):
            slot = SLOT_OF[(direction, half, k)]
            return remote(
                block(source, half), block(source, half),
                ring_send.at[number, slot], ring_recv.at[number, slot], neighbour(direction),
            )

        def send(direction, half, k):
            moving = copy(direction, half, k, step_to(position, -direction * k, SIDE))
            moving.start()
            sent.append(moving)

        def first():
            ready()
            for half in (0, 1):
                for direction in (1, -1):
                    send(direction, half, 0)

        at(start, first)

        def arrived(direction, half, k):
            source = step_to(position, -direction * (k + 1), SIDE)
            copy(direction, half, k, source).wait_recv()
            if k + 1 < hops(direction, half):
                send(direction, half, k + 1)

        last = start
        for k in range(SIDE // 2):
            for half in (0, 1):
                for direction in (1, -1):
                    if k < hops(direction, half):
                        time = start + tau * k + (half + 1) * tau / 2 + 1.7
                        last = max(last, time)
                        at(time, lambda a=direction, b=half, c=k: arrived(a, b, c))
        return last

    def nothing():
        pass

    def loaded(*names):
        def wait():
            for name in names:
                loads[name].wait()
        return wait

    quarter = SIDE // 2
    deep1, deep2 = ws1.shape[2] // 2, wc2.shape[2] // 2

    def rows_of(half, deep):
        return pl.ds(half * deep, deep)

    ring(0, "y", lambda i, h: ws1.at[z, i, rows_of(h, deep1)], 0.0, 0.8, loaded("ws1"))
    ring(1, "z", lambda i, h: wc1.at[h, i, y], 0.1, 1.4, loaded("wc1v", "wc1g"))
    s1 = ring(2, "z", lambda i, h: ws1.at[i, pl.ds(h * quarter, quarter)], 9.0, 5.6, nothing)
    c1 = ring(3, "y", lambda i, h: wc1.at[:, pl.ds(h * quarter, quarter), i], 12.5, 11.2, nothing)
    p2 = ring(4, "y", lambda i, h: ws2.at[h, z, i], 15.0, 3.0, loaded("ws2v", "ws2g"))
    s2 = ring(
        5, "z", lambda i, h: ws2.at[:, i, pl.ds(h * quarter, quarter)],
        max(p2 + 0.1, s1 - 2.0), 11.2, nothing,
    )
    p3 = ring(6, "z", lambda i, h: wc2.at[i, y, rows_of(h, deep2)], s1 + 3.0, 3.0, loaded("wc2"))
    c2 = ring(
        7, "y", lambda i, h: wc2.at[pl.ds(h * quarter, quarter), i],
        max(p3 + 0.1, c1 - 2.0), 5.6, nothing,
    )

    def normalise():
        loads["raw"].wait()
        def body(i, carry):
            part = pl.ds(pl.multiple_of(i * 16, 16), 16)
            value = raw[part, :].astype(F32)
            scale = lax.rsqrt(jnp.mean(value * value, axis=1, keepdims=True) + 1e-6)
            normed[part, :] = (value * scale * norm_gain[...]).astype(BF)
            return carry
        lax.fori_loop(0, length // 16, body, 0)

    def spread():
        return ((iota((size, flat), 1) & (size - 1)) == iota((size, flat), 0)).astype(F32)

    def owner():
        return (iota((groups, flat), 1) // size) == iota((groups, flat), 0)

    def as_row(table):
        wide_table = jnp.dot(table, spread(), precision=HIGHEST, preferred_element_type=F32)
        return jnp.sum(jnp.where(owner(), wide_table, 0.0), axis=0, keepdims=True)

    def as_table(row):
        return lax.dot_general(
            jnp.where(owner(), row, 0.0), spread(), NT, precision=HIGHEST, preferred_element_type=F32
        )

    total_tokens = length * SIDE * SIDE

    def tables():
        rate = -as_row(decay_rate[...]) / total_tokens
        turn = as_row(frequency[...])
        rows[0:1, :] = as_row(initial_state[0])
        rows[1:2, :] = as_row(initial_state[1])
        magnitude = jnp.exp(rate)
        step_r = magnitude * jnp.cos(turn)
        step_i = magnitude * jnp.sin(turn)
        modulus = rate * rate + turn * turn
        lift = step_r - 1.0
        factor_r = (lift * rate + step_i * turn) / modulus
        factor_i = (step_i * rate - lift * turn) / modulus
        count = iota((8, flat), 0) + 1
        block_r, block_i = jnp.ones((8, flat), F32), jnp.zeros((8, flat), F32)
        square_r, square_i = step_r, step_i
        for place in range(4):
            chosen = ((count >> place) & 1) == 1
            next_r, next_i = rotate(block_r, block_i, square_r, square_i)
            block_r = jnp.where(chosen, next_r, block_r)
            block_i = jnp.where(chosen, next_i, block_i)
            if place < 3:
                square_r, square_i = rotate(square_r, square_i, square_r, square_i)
        rows[2:3, :], rows[3:4, :] = square_r, square_i
        rows[4:5, :], rows[5:6, :] = factor_r, factor_i

        def body(i, carry):
            now_r, now_i = carry
            part = pl.ds(pl.multiple_of(i * 8, 8), 8)
            power_r[part, :], power_i[part, :] = now_r, now_i
            inverse = 1.0 / (now_r * now_r + now_i * now_i)
            un_r, un_i = rotate(now_r * inverse, -now_i * inverse, rows[4:5, :], rows[5:6, :])
            undo_r[part, :], undo_i[part, :] = un_r, un_i
            return rotate(now_r, now_i, rows[2:3, :], rows[3:4, :])
        lax.fori_loop(0, length // 8, body, (block_r, block_i))

    def matrices():
        tile = ((iota((wide, width), 1) & (wide - 1)) == iota((wide, width), 0)).astype(BF)
        for source, dest in ((input_real, drive_r), (input_imag, drive_i)):
            for g in range(groups):
                copied = jnp.dot(source[g].astype(BF), tile, preferred_element_type=F32)
                kept = iota((size, width), 1) // wide == g
                dest[g * size:(g + 1) * size, :] = jnp.where(kept, copied, 0.0).astype(BF)
        stretch = spread().astype(BF)
        for part, (source, sign) in enumerate(((output_real, 1.0), (output_imag, -1.0))):
            for g in range(groups):
                copied = jnp.dot((sign * source[g]).astype(BF), stretch, preferred_element_type=F32)
                kept = iota((wide, flat), 1) // size == g
                emit[g * wide:(g + 1) * wide, part * flat:(part + 1) * flat] = (
                    jnp.where(kept, copied, 0.0).astype(BF)
                )

    at(13.0, normalise)
    at(13.5, tables)
    at(13.6, matrices)

    chunk = 256

    def recur():
        drive = jnp.dot(
            normed[...], ws1[...].reshape(normed.shape[1], width), preferred_element_type=F32
        ).astype(BF)
        feed[...] = drive
        for j in range(flat // chunk):
            part = slice(j * chunk, (j + 1) * chunk)
            shift = slice(flat + j * chunk, flat + (j + 1) * chunk)
            push_r = lax.dot_general(drive, drive_r[part, :], NT, preferred_element_type=F32)
            push_i = lax.dot_general(drive, drive_i[part, :], NT, preferred_element_type=F32)
            back_r, back_i = rotate(undo_r[:, part], undo_i[:, part], push_r, push_i)
            scaled[:, part] = back_r.astype(BF)
            scaled[:, shift] = back_i.astype(BF)
        lower = (iota((length, length), 0) >= iota((length, length), 1)).astype(BF)
        for j in range(2 * flat // chunk):
            part = slice(j * chunk, (j + 1) * chunk)
            summed[:, part] = jnp.dot(lower, scaled[:, part], preferred_element_type=F32)
        end_r, end_i = rotate(
            power_r[length - 1:length, :], power_i[length - 1:length, :],
            summed[length - 1:length, 0:flat], summed[length - 1:length, flat:2 * flat],
        )
        finals[y, :, 0:flat], finals[y, :, flat:2 * flat] = end_r, end_i
        for d in range(1, SIDE):
            moving = remote(
                finals.at[y], finals.at[y], scan_send.at[0, d - 1], scan_recv.at[0, d - 1],
                device(z, step_to(y, d, SIDE), t),
            )
            moving.start()
            sent.append(moving)

    def scan_row():
        for d in range(1, SIDE):
            source = step_to(y, -d, SIDE)
            remote(
                finals.at[source], finals.at[source], scan_send.at[0, d - 1],
                scan_recv.at[0, d - 1], device(z, source, t),
            ).wait_recv()
        span_r, span_i = power_r[length - 1:length, :], power_i[length - 1:length, :]
        zero = jnp.zeros((1, flat), F32)
        sum_r, sum_i, before_r, before_i = zero, zero, zero, zero
        jump_r, jump_i = zero + 1.0, zero
        mine_r, mine_i = zero, zero
        for yy in range(SIDE):
            before_r, before_i = jnp.where(y == yy, sum_r, before_r), jnp.where(y == yy, sum_i, before_i)
            mine_r, mine_i = jnp.where(y == yy, jump_r, mine_r), jnp.where(y == yy, jump_i, mine_i)
            next_r, next_i = rotate(span_r, span_i, sum_r, sum_i)
            sum_r = next_r + finals[yy, :, 0:flat]
            sum_i = next_i + finals[yy, :, flat:2 * flat]
            jump_r, jump_i = rotate(span_r, span_i, jump_r, jump_i)
        rows[6:7, :], rows[7:8, :] = before_r, before_i
        rows[8:9, :], rows[9:10, :] = mine_r, mine_i
        rows[10:11, :], rows[11:12, :] = jump_r, jump_i
        totals[z, :, 0:flat], totals[z, :, flat:2 * flat] = sum_r, sum_i
        for d in range(1, SIDE):
            moving = remote(
                totals.at[z], totals.at[z], scan_send.at[1, d - 1], scan_recv.at[1, d - 1],
                device(step_to(z, d, SIDE), y, t),
            )
            moving.start()
            sent.append(moving)

    def scan_all():
        for d in range(1, SIDE):
            source = step_to(z, -d, SIDE)
            remote(
                totals.at[source], totals.at[source], scan_send.at[1, d - 1],
                scan_recv.at[1, d - 1], device(source, y, t),
            ).wait_recv()
        sum_r, sum_i = rows[0:1, :], rows[1:2, :]
        jump_r, jump_i = rows[10:11, :], rows[11:12, :]
        start_r, start_i = sum_r, sum_i
        for zz in range(SIDE):
            start_r, start_i = jnp.where(z == zz, sum_r, start_r), jnp.where(z == zz, sum_i, start_i)
            next_r, next_i = rotate(jump_r, jump_i, sum_r, sum_i)
            sum_r = next_r + totals[zz, :, 0:flat]
            sum_i = next_i + totals[zz, :, flat:2 * flat]
        final_state[0] = as_table(sum_r)
        final_state[1] = as_table(sum_i)
        lead_r, lead_i = rotate(rows[8:9, :], rows[9:10, :], start_r, start_i)
        entry_r, entry_i = lead_r + rows[6:7, :], lead_i + rows[7:8, :]
        for j in range(flat // chunk):
            part = slice(j * chunk, (j + 1) * chunk)
            shift = slice(flat + j * chunk, flat + (j + 1) * chunk)
            state_r, state_i = rotate(
                power_r[:, part], power_i[:, part],
                summed[:, part] + entry_r[:, part], summed[:, shift] + entry_i[:, part],
            )
            states[:, part] = state_r.astype(BF)
            states[:, shift] = state_i.astype(BF)
        answer = lax.dot_general(states[...], emit[...], NT, preferred_element_type=F32)
        answer = answer + skip_gain[...] * feed[...].astype(F32)
        act_all[t] = jax.nn.gelu(answer).astype(BF)
        share(0, act_all)

    other = t + 1 - 2 * core

    def share(number, blocks):
        moving = remote(
            blocks.at[t], blocks.at[t], tp_send.at[number, 0], tp_recv.at[number, 0],
            device(z, y, other),
        )
        moving.start()
        sent.append(moving)
        for d in range(1, CHIPS):
            moving = remote(
                blocks.at[t], blocks.at[t], tp_send.at[number, d], tp_recv.at[number, d],
                device(z, y, step_to(chip, d, CHIPS) * 2 + core),
            )
            moving.start()
            sent.append(moving)

    def pass_on(number, blocks):
        for d in (1, 3, 2):
            source = step_to(chip, -d, CHIPS) * 2 + core
            remote(
                blocks.at[source], blocks.at[source], tp_send.at[number, d], tp_recv.at[number, d],
                device(z, y, source),
            ).wait_recv()
            moving = remote(
                blocks.at[source], blocks.at[source], tp_send.at[number, 3 + d],
                tp_recv.at[number, 3 + d], device(z, y, other),
            )
            moving.start()
            sent.append(moving)

    def shared(number, blocks):
        remote(
            blocks.at[other], blocks.at[other], tp_send.at[number, 0], tp_recv.at[number, 0],
            device(z, y, other),
        ).wait_recv()
        for d in (1, 3, 2):
            source = step_to(chip, -d, CHIPS) * 2 + 1 - core
            remote(
                blocks.at[source], blocks.at[source], tp_send.at[number, 3 + d],
                tp_recv.at[number, 3 + d], device(z, y, other),
            ).wait_recv()

    at(s1 + 0.1, recur)
    at(s1 + 11.0, scan_row)
    at(s1 + 21.0, scan_all)
    at(s1 + 30.0, lambda: pass_on(0, act_all))

    edge = halo.shape[0]
    kernel_size = conv_taps.shape[0]

    def gate():
        value_in = jnp.dot(
            normed[...], wc1[0].reshape(normed.shape[1], width), preferred_element_type=F32
        )
        gate_in = jnp.dot(
            normed[...], wc1[1].reshape(normed.shape[1], width), preferred_element_type=F32
        )
        gated[...] = (value_in * jax.nn.sigmoid(gate_in)).astype(BF)
        moving = remote(
            gated.at[pl.ds(length - edge, edge)], halo, halo_sem.at[0], halo_sem.at[1],
            {"sp": following, "tp": t},
        )
        moving.start()
        sent.append(moving)
        padded[edge:edge + length, :] = gated[...].astype(F32)

    def convolve():
        remote(
            gated.at[pl.ds(length - edge, edge)], halo, halo_sem.at[0], halo_sem.at[1],
            {"sp": preceding, "tp": t},
        ).wait_recv()
        padded[0:edge, :] = jnp.where(seq > 0, halo[...].astype(F32), 0.0)
        lag = edge - (kernel_size - 1)
        for lane in range(width // 128):
            lanes = slice(lane * 128, (lane + 1) * 128)
            answer = jnp.zeros((length, 128), F32)
            for b in range(8):
                tall = length + (8 if b else 0)
                part = jnp.zeros((tall, 128), F32)
                for a in range(edge // 8 + 1):
                    k = 8 * a + b - lag
                    if 0 <= k < kernel_size:
                        part = part + conv_taps[k:k + 1, lanes] * padded[8 * a:8 * a + tall, lanes]
                if b:
                    shifted[b, :, :] = part
                    answer = answer + shifted[b, b:b + length, :]
                else:
                    answer = answer + part
            conv_all[t, :, lanes] = answer.astype(BF)
        share(1, conv_all)

    def channel_norm():
        count = 2 * CHIPS * width
        def body(i, carry):
            part = pl.ds(pl.multiple_of(i * 16, 16), 16)
            pieces = [conv_all[c, part, :].astype(F32) for c in range(2 * CHIPS)]
            total = pieces[0]
            for piece in pieces[1:]:
                total = total + piece
            mean = jnp.sum(total, axis=1, keepdims=True) / count
            pieces = [piece - mean for piece in pieces]
            total = pieces[0] * pieces[0]
            for piece in pieces[1:]:
                total = total + piece * piece
            scale = lax.rsqrt(jnp.sum(total, axis=1, keepdims=True) / count + 1e-5)
            for c, piece in enumerate(pieces):
                lanes = slice(c * width, (c + 1) * width)
                value = piece * scale * chan_gain[:, lanes] + chan_shift[:, lanes]
                conv_act[c, part, :] = jax.nn.silu(value).astype(BF)
            return carry
        lax.fori_loop(0, length // 16, body, 0)

    at(c1 + 0.1, gate)
    at(c1 + 7.0, convolve)
    at(c1 + 15.0, lambda: pass_on(1, conv_all))
    at(c1 + 16.5, lambda: (shared(1, conv_all), channel_norm()))

    columns = out.shape[1]

    def project(blocks, weights, lanes):
        total = None
        for c in range(2 * CHIPS):
            term = jnp.dot(
                blocks[c], weights[c].reshape(width, columns)[:, lanes], preferred_element_type=F32
            )
            total = term if total is None else total + term
        return total

    def state_out():
        shared(0, act_all)
        for n in range(columns // 256):
            lanes = slice(n * 256, (n + 1) * 256)
            mixed[:, lanes] = project(act_all, ws2.at[0], lanes) * jax.nn.sigmoid(
                project(act_all, ws2.at[1], lanes)
            )

    def conv_out():
        for n in range(columns // 256):
            lanes = slice(n * 256, (n + 1) * 256)
            result[:, lanes] = (mixed[:, lanes] + project(conv_act, wc2, lanes)).astype(BF)
        moving = pltpu.make_async_copy(result, out, load_sem.at[7])
        moving.start()
        for copy in sent:
            copy.wait_send()
        moving.wait()

    at(s2 + 0.1, state_out)
    at(max(s2, c2) + 0.2, conv_out)

    for _, _, fn in sorted(events, key=lambda e: e[:2]):
        fn()


def local(
    tokens, norm_gain, conv_value, conv_gate, state_feed, conv_taps, chan_gain, chan_shift,
    conv_project, decay_rate, frequency, input_real, input_imag, output_real, output_imag,
    skip_gain, state_value, state_gate, initial_state,
):
    length, features = tokens.shape
    groups, size, wide = input_real.shape
    flat, width = groups * size, groups * wide
    deep1, columns = conv_value.shape[0], conv_project.shape[1]
    deep2 = conv_project.shape[0]
    edge = 32
    args = (
        tokens, norm_gain.reshape(1, -1), conv_value, conv_gate, state_feed, conv_taps,
        chan_gain.reshape(1, -1), chan_shift.reshape(1, -1), conv_project, decay_rate, frequency,
        input_real, input_imag, output_real, output_imag, skip_gain.reshape(1, -1), state_value,
        state_gate, initial_state,
    )
    large = {0, 2, 3, 4, 8, 16, 17}
    anywhere = pl.BlockSpec(memory_space=pl.ANY)
    held = pl.BlockSpec(memory_space=pltpu.VMEM)
    vmem = pltpu.VMEM
    dma = pltpu.SemaphoreType.DMA
    return pl.pallas_call(
        kernel,
        out_shape=(
            jax.ShapeDtypeStruct((length, columns), BF),
            jax.ShapeDtypeStruct(initial_state.shape, F32),
        ),
        in_specs=[anywhere if i in large else held for i in range(len(args))],
        out_specs=(anywhere, held),
        scratch_shapes=[
            vmem((SIDE, SIDE, deep1, width), BF),
            vmem((2, SIDE, SIDE, deep1, width), BF),
            vmem((2, SIDE, SIDE, deep2, columns), BF),
            vmem((SIDE, SIDE, deep2, columns), BF),
            vmem((length, features), BF),
            vmem((length, features), BF),
            vmem((length, columns), BF),
            vmem((length, flat), F32),
            vmem((length, flat), F32),
            vmem((length, flat), F32),
            vmem((length, flat), F32),
            vmem((flat, width), BF),
            vmem((flat, width), BF),
            vmem((width, 2 * flat), BF),
            vmem((length, width), BF),
            vmem((length, 2 * flat), BF),
            vmem((length, 2 * flat), F32),
            vmem((length, 2 * flat), BF),
            vmem((16, flat), F32),
            vmem((SIDE, 1, 2 * flat), F32),
            vmem((SIDE, 1, 2 * flat), F32),
            vmem((length, width), BF),
            vmem((edge, width), BF),
            vmem((edge + length, width), F32),
            vmem((8, length + 8, 128), F32),
            vmem((2 * CHIPS, length, width), BF),
            vmem((2 * CHIPS, length, width), BF),
            vmem((2 * CHIPS, length, width), BF),
            vmem((length, columns), F32),
            dma((8,)),
            dma((8, len(SLOTS))),
            dma((8, len(SLOTS))),
            dma((2, SIDE - 1)),
            dma((2, SIDE - 1)),
            dma((2,)),
            dma((2, 7)),
            dma((2, 7)),
        ],
        compiler_params=pltpu.CompilerParams(
            collective_id=0, has_side_effects=True, vmem_limit_bytes=60 * 1024 * 1024
        ),
        name="mixer",
    )(*args)


def solution(mesh):
    in_specs = (
        P("sp", None), P(), P("sp", "tp"), P("sp", "tp"), P("sp", "tp"), P(None, "tp"), P(), P(),
        P("sp", "tp"), P("tp", None), P("tp", None), P("tp", None, None), P("tp", None, None),
        P("tp", None, None), P("tp", None, None), P("tp"), P("sp", "tp"), P("sp", "tp"),
        P(None, "tp", None),
    )
    out_specs = (P("sp", "tp"), P(None, "tp", None))
    return jax.shard_map(local, mesh=mesh, in_specs=in_specs, out_specs=out_specs, check_vma=False)
```

```python
import heapq

import jax
import jax.numpy as jnp
from jax import lax
from jax.experimental import pallas as pl
from jax.experimental.pallas import tpu as pltpu
from jax.sharding import PartitionSpec as P

BF, F32 = jnp.bfloat16, jnp.float32
HIGHEST = lax.Precision.HIGHEST
MESH = pl.DeviceIdType.MESH
SIDE = 8
CHIPS = 4
NT = (((1,), (1,)), ((), ()))


def hops(direction, half):
    return SIDE // 2 if (direction > 0) == (half == 0) else SIDE // 2 - 1


SLOTS = [
    (direction, half, k)
    for direction in (1, -1)
    for half in (0, 1)
    for k in range(hops(direction, half))
]
SLOT_OF = {slot: at for at, slot in enumerate(SLOTS)}


def rotate(first_real, first_imag, second_real, second_imag):
    return (
        first_real * second_real - first_imag * second_imag,
        first_real * second_imag + first_imag * second_real,
    )


def iota(shape, dim):
    return lax.broadcasted_iota(jnp.int32, shape, dim)


def kernel(
    tokens, norm_gain, conv_value, conv_gate, state_feed, conv_taps, chan_gain, chan_shift,
    conv_project, decay_rate, frequency, input_real, input_imag, output_real, output_imag,
    skip_gain, state_value, state_gate, initial_state,
    out, final_state,
    ws1, wc1, ws2, wc2, raw, normed, result,
    power_r, power_i, undo_r, undo_i, drive_r, drive_i, emit, feed, scaled, summed, states,
    rows, finals, totals, gated, halo, padded, shifted, conv_all, act_all, conv_act, mixed,
    load_sem, ring_send, ring_recv, scan_send, scan_recv, halo_sem, tp_send, tp_recv,
):
    seq = lax.axis_index("sp")
    t = lax.axis_index("tp")
    z, y = seq // SIDE, seq % SIDE
    chip, core = t // 2, t % 2
    length = tokens.shape[0]
    groups, wide, size = input_real.shape
    flat = groups * size
    width = groups * wide

    def device(zz, yy, tt):
        return {"sp": zz * SIDE + yy, "tp": tt}

    def step_to(at, by, count):
        return lax.rem(at + by + count, count)

    def remote(src, dst, send, recv, to):
        return pltpu.make_async_remote_copy(
            src_ref=src, dst_ref=dst, send_sem=send, recv_sem=recv, device_id=to, device_id_type=MESH
        )

    queue = []
    sent = []
    free = {}
    clock = [0.0, 0]

    def at(time, fn, cost=0.0):
        heapq.heappush(queue, (time, clock[1], cost, fn))
        clock[1] += 1

    def run():
        while queue:
            time, _, cost, fn = heapq.heappop(queue)
            clock[0] = max(clock[0], time)
            fn()
            clock[0] += cost

    def transit(link, size, count=1, rate=46.6e3):
        begin = max(clock[0], free.get(link, 0.0))
        free[link] = begin + size * count / rate
        return free[link] + 0.95 + 0.75 * count

    def when_all(number, fn):
        left = [number]

        def one():
            left[0] -= 1
            if left[0] == 0:
                fn()
        return one

    loads = {}

    def load(name, index, src, dst):
        loads[name] = pltpu.make_async_copy(src, dst, load_sem.at[index])
        loads[name].start()

    load("ws1", 0, state_feed, ws1.at[z, y])
    load("wc1v", 1, conv_value, wc1.at[0, z, y])
    load("wc1g", 2, conv_gate, wc1.at[1, z, y])
    load("ws2v", 3, state_value, ws2.at[0, z, y])
    load("ws2g", 4, state_gate, ws2.at[1, z, y])
    load("wc2", 5, conv_project, wc2.at[z, y])
    load("raw", 6, tokens, raw)

    barrier = pltpu.get_barrier_semaphore()
    here = {"z": z, "y": y}
    following = lax.rem(seq + 1, SIDE * SIDE)
    preceding = lax.rem(seq + SIDE * SIDE - 1, SIDE * SIDE)
    partners = []
    for d in range(1, SIDE):
        partners.append(device(z, step_to(y, d, SIDE), t))
        partners.append(device(step_to(z, d, SIDE), y, t))
    for d in range(1, 2 * CHIPS):
        partners.append(device(z, y, step_to(t, d, 2 * CHIPS)))
    partners.append({"sp": following, "tp": t})
    partners.append({"sp": preceding, "tp": t})
    for partner in partners:
        pl.semaphore_signal(barrier, inc=1, device_id=partner, device_id_type=MESH)
    pl.semaphore_wait(barrier, len(partners))

    def beside(axis, by):
        moved = step_to(here[axis], by, SIDE)
        return device(moved, y, t) if axis == "z" else device(z, moved, t)

    def ring(number, axis, block, size, done, nearly=None):
        position = here[axis]
        finished = when_all(len(SLOTS), done)
        passed = when_all(len(SLOTS) - 4, nearly or (lambda: None))

        def copy(direction, half, k, source):
            slot = SLOT_OF[(direction, half, k)]
            return remote(
                block(source, half), block(source, half),
                ring_send.at[number, slot], ring_recv.at[number, slot], beside(axis, direction),
            )

        def send(direction, half, k):
            moving = copy(direction, half, k, step_to(position, -direction * k, SIDE))
            moving.start()
            sent.append(moving)
            time = transit((axis, direction), size)
            at(time, lambda: arrived(direction, half, k))

        def arrived(direction, half, k):
            source = step_to(position, -direction * (k + 1), SIDE)
            copy(direction, half, k, source).wait_recv()
            if k + 1 < hops(direction, half):
                send(direction, half, k + 1)
                passed()
            finished()

        def first():
            for half in (0, 1):
                for direction in (1, -1):
                    send(direction, half, 0)
        return first

    def spread_out(sems, axis, block, size, done):
        position = here[axis]
        finished = when_all(SIDE - 1, done)

        def copy(d, source, to):
            return remote(block(source), block(source), sems[0](d), sems[1](d), to)

        def arrived(d):
            copy(d, step_to(position, -d, SIDE), beside(axis, -d)).wait_recv()
            finished()

        def first():
            for d in (4, 3, 5, 2, 6, 1, 7):
                moving = copy(d, position, beside(axis, d))
                moving.start()
                sent.append(moving)
                direction, count = (1, d) if d <= SIDE // 2 else (-1, SIDE - d)
                time = transit((axis, direction), size, count)
                at(time, lambda d=d: arrived(d))
        return first

    quarter = SIDE // 2
    deep1, deep2 = ws1.shape[2] // 2, wc2.shape[2] // 2
    piece = ws1.shape[2] * ws1.shape[3] * 2

    def rows_of(half, deep):
        return pl.ds(half * deep, deep)

    def after(*names):
        for name in names:
            loads[name].wait()

    def direct(number):
        return (
            lambda d: ring_send.at[number, d],
            lambda d: ring_recv.at[number, d],
        )

    def both(fn):
        return when_all(2, fn)

    state_in = ring(
        0, "z", lambda i, h: ws1.at[i, pl.ds(h * quarter, quarter)], 4 * piece,
        lambda: at(clock[0], recur, 1.8), lambda: go_sv(),
    )
    sv_big = ring(
        1, "z", lambda i, h: ws2.at[0, i, pl.ds(h * quarter, quarter)], 4 * piece,
        lambda: state_ready(), lambda: go_sg(),
    )
    sg_big = ring(
        2, "z", lambda i, h: ws2.at[1, i, pl.ds(h * quarter, quarter)], 4 * piece,
        lambda: state_ready(),
    )
    go_sv, go_sg = both(sv_big), both(sg_big)
    sg_small = ring(
        3, "y", lambda i, h: ws2.at[1, z, i, rows_of(h, deep2)], piece / 2, lambda: go_sg()
    )
    sv_small = ring(
        4, "y", lambda i, h: ws2.at[0, z, i, rows_of(h, deep2)], piece / 2,
        lambda: (go_sv(), sg_small()),
    )
    conv_in = ring(
        5, "y", lambda i, h: wc1.at[0, pl.ds(h * quarter, quarter), i], 4 * piece,
        lambda: gate_ready(), lambda: go_cg(),
    )
    cg_big = ring(
        6, "y", lambda i, h: wc1.at[1, pl.ds(h * quarter, quarter), i], 4 * piece,
        lambda: gate_ready(), lambda: go_cp(),
    )
    cp_big = ring(
        7, "y", lambda i, h: wc2.at[pl.ds(h * quarter, quarter), i], 4 * piece,
        lambda: conv_ready(),
    )
    go_cg, go_cp = both(cg_big), both(cp_big)
    cp_small = ring(
        8, "z", lambda i, h: wc2.at[i, y, rows_of(h, deep2)], piece / 2, lambda: go_cp()
    )
    cg_small = ring(
        9, "z", lambda i, h: wc1.at[1, i, y, rows_of(h, deep1)], piece / 2,
        lambda: (go_cg(), cp_small()),
    )
    sf_small = spread_out(direct(10), "y", lambda i: ws1.at[z, i], piece, state_in)
    cv_small = spread_out(direct(11), "z", lambda i: wc1.at[0, i, y], piece, conv_in)

    def begin():
        after("ws1")
        sf_small()
        after("wc1v")
        cv_small()
        after("wc1g")
        cg_small()

    at(0.0, begin)
    at(5.0, lambda: (after("ws2v", "ws2g", "wc2"), sv_small()))

    def normalise():
        loads["raw"].wait()
        def body(i, carry):
            part = pl.ds(pl.multiple_of(i * 16, 16), 16)
            value = raw[part, :].astype(F32)
            scale = lax.rsqrt(jnp.mean(value * value, axis=1, keepdims=True) + 1e-6)
            normed[part, :] = (value * scale * norm_gain[...]).astype(BF)
            return carry
        lax.fori_loop(0, length // 16, body, 0)

    def spread():
        return ((iota((size, flat), 1) & (size - 1)) == iota((size, flat), 0)).astype(F32)

    def owner():
        return (iota((groups, flat), 1) // size) == iota((groups, flat), 0)

    def as_row(table):
        wide_table = jnp.dot(table, spread(), precision=HIGHEST, preferred_element_type=F32)
        return jnp.sum(jnp.where(owner(), wide_table, 0.0), axis=0, keepdims=True)

    def as_table(row):
        return lax.dot_general(
            jnp.where(owner(), row, 0.0), spread(), NT, precision=HIGHEST, preferred_element_type=F32
        )

    total_tokens = length * SIDE * SIDE

    def tables():
        rate = -as_row(decay_rate[...]) / total_tokens
        turn = as_row(frequency[...])
        rows[0:1, :] = as_row(initial_state[0])
        rows[1:2, :] = as_row(initial_state[1])
        magnitude = jnp.exp(rate)
        step_r = magnitude * jnp.cos(turn)
        step_i = magnitude * jnp.sin(turn)
        modulus = rate * rate + turn * turn
        lift = step_r - 1.0
        factor_r = (lift * rate + step_i * turn) / modulus
        factor_i = (step_i * rate - lift * turn) / modulus
        count = iota((8, flat), 0) + 1
        block_r, block_i = jnp.ones((8, flat), F32), jnp.zeros((8, flat), F32)
        square_r, square_i = step_r, step_i
        for place in range(4):
            chosen = ((count >> place) & 1) == 1
            next_r, next_i = rotate(block_r, block_i, square_r, square_i)
            block_r = jnp.where(chosen, next_r, block_r)
            block_i = jnp.where(chosen, next_i, block_i)
            if place < 3:
                square_r, square_i = rotate(square_r, square_i, square_r, square_i)
        rows[2:3, :], rows[3:4, :] = square_r, square_i
        rows[4:5, :], rows[5:6, :] = factor_r, factor_i

        def body(i, carry):
            now_r, now_i = carry
            part = pl.ds(pl.multiple_of(i * 8, 8), 8)
            power_r[part, :], power_i[part, :] = now_r, now_i
            inverse = 1.0 / (now_r * now_r + now_i * now_i)
            un_r, un_i = rotate(now_r * inverse, -now_i * inverse, rows[4:5, :], rows[5:6, :])
            undo_r[part, :], undo_i[part, :] = un_r, un_i
            return rotate(now_r, now_i, rows[2:3, :], rows[3:4, :])
        lax.fori_loop(0, length // 8, body, (block_r, block_i))

    def matrices():
        stretch = spread().astype(BF)
        def fill(source, sign, dest, lanes):
            for g in range(groups):
                copied = jnp.dot((sign * source[g]).astype(BF), stretch, preferred_element_type=F32)
                kept = iota((wide, flat), 1) // size == g
                dest[g * wide:(g + 1) * wide, lanes] = jnp.where(kept, copied, 0.0).astype(BF)
        fill(input_real, 1.0, drive_r, slice(0, flat))
        fill(input_imag, 1.0, drive_i, slice(0, flat))
        fill(output_real, 1.0, emit, slice(0, flat))
        fill(output_imag, -1.0, emit, slice(flat, 2 * flat))

    at(8.0, normalise, 1.8)
    at(9.0, tables, 1.4)
    at(11.0, matrices, 1.0)

    chunk = 256

    def recur():
        drive = jnp.dot(
            normed[...], ws1[...].reshape(normed.shape[1], width), preferred_element_type=F32
        ).astype(BF)
        feed[...] = drive
        for j in range(flat // chunk):
            part = slice(j * chunk, (j + 1) * chunk)
            shift = slice(flat + j * chunk, flat + (j + 1) * chunk)
            push_r = jnp.dot(drive, drive_r[:, part], preferred_element_type=F32)
            push_i = jnp.dot(drive, drive_i[:, part], preferred_element_type=F32)
            back_r, back_i = rotate(undo_r[:, part], undo_i[:, part], push_r, push_i)
            scaled[:, part] = back_r.astype(BF)
            scaled[:, shift] = back_i.astype(BF)
        lower = (iota((length, length), 0) >= iota((length, length), 1)).astype(BF)
        for j in range(2 * flat // chunk):
            part = slice(j * chunk, (j + 1) * chunk)
            summed[:, part] = jnp.dot(lower, scaled[:, part], preferred_element_type=F32)
        end_r, end_i = rotate(
            power_r[length - 1:length, :], power_i[length - 1:length, :],
            summed[length - 1:length, 0:flat], summed[length - 1:length, flat:2 * flat],
        )
        finals[y, :, 0:flat], finals[y, :, flat:2 * flat] = end_r, end_i
        spread_out(
            scan_sems(0), "y", lambda i: finals.at[i], 8 * flat, lambda: at(clock[0], scan_row, 0.1)
        )()

    def scan_sems(number):
        return (
            lambda d: scan_send.at[number, d - 1],
            lambda d: scan_recv.at[number, d - 1],
        )

    def scan_row():
        span_r, span_i = power_r[length - 1:length, :], power_i[length - 1:length, :]
        zero = jnp.zeros((1, flat), F32)
        sum_r, sum_i, before_r, before_i = zero, zero, zero, zero
        jump_r, jump_i = zero + 1.0, zero
        mine_r, mine_i = zero, zero
        for yy in range(SIDE):
            before_r, before_i = jnp.where(y == yy, sum_r, before_r), jnp.where(y == yy, sum_i, before_i)
            mine_r, mine_i = jnp.where(y == yy, jump_r, mine_r), jnp.where(y == yy, jump_i, mine_i)
            next_r, next_i = rotate(span_r, span_i, sum_r, sum_i)
            sum_r = next_r + finals[yy, :, 0:flat]
            sum_i = next_i + finals[yy, :, flat:2 * flat]
            jump_r, jump_i = rotate(span_r, span_i, jump_r, jump_i)
        rows[6:7, :], rows[7:8, :] = before_r, before_i
        rows[8:9, :], rows[9:10, :] = mine_r, mine_i
        rows[10:11, :], rows[11:12, :] = jump_r, jump_i
        totals[z, :, 0:flat], totals[z, :, flat:2 * flat] = sum_r, sum_i
        spread_out(
            scan_sems(1), "z", lambda i: totals.at[i], 8 * flat, lambda: at(clock[0], scan_all, 2.5)
        )()

    def scan_all():
        sum_r, sum_i = rows[0:1, :], rows[1:2, :]
        jump_r, jump_i = rows[10:11, :], rows[11:12, :]
        start_r, start_i = sum_r, sum_i
        for zz in range(SIDE):
            start_r, start_i = jnp.where(z == zz, sum_r, start_r), jnp.where(z == zz, sum_i, start_i)
            next_r, next_i = rotate(jump_r, jump_i, sum_r, sum_i)
            sum_r = next_r + totals[zz, :, 0:flat]
            sum_i = next_i + totals[zz, :, flat:2 * flat]
        final_state[0] = as_table(sum_r)
        final_state[1] = as_table(sum_i)
        lead_r, lead_i = rotate(rows[8:9, :], rows[9:10, :], start_r, start_i)
        entry_r, entry_i = lead_r + rows[6:7, :], lead_i + rows[7:8, :]
        for j in range(flat // chunk):
            part = slice(j * chunk, (j + 1) * chunk)
            shift = slice(flat + j * chunk, flat + (j + 1) * chunk)
            state_r, state_i = rotate(
                power_r[:, part], power_i[:, part],
                summed[:, part] + entry_r[:, part], summed[:, shift] + entry_i[:, part],
            )
            states[:, part] = state_r.astype(BF)
            states[:, shift] = state_i.astype(BF)
        answer = lax.dot_general(states[...], emit[...], NT, preferred_element_type=F32)
        answer = answer + skip_gain[...] * feed[...].astype(F32)
        act_all[t] = jax.nn.gelu(answer).astype(BF)
        share(0, act_all, lambda: state_ready())

    other = t + 1 - 2 * core

    def share(number, blocks, done):
        finished = when_all(4, done)
        size = length * width * 2

        def copy(slot, source, to):
            return remote(
                blocks.at[source], blocks.at[source], tp_send.at[number, slot],
                tp_recv.at[number, slot], device(z, y, to),
            )

        def start(moving):
            moving.start()
            sent.append(moving)

        def near(d):
            source = other if d == 0 else step_to(chip, -d, CHIPS) * 2 + 1 - core
            copy(3 + d if d else 0, source, other).wait_recv()
            finished()

        def far(d):
            source = step_to(chip, -d, CHIPS) * 2 + core
            copy(d, source, source).wait_recv()
            start(copy(3 + d, source, other))
            at(transit("core", size, 1, 300e3), lambda: near(d))

        for d in (2, 1, 3):
            start(copy(d, t, step_to(chip, d, CHIPS) * 2 + core))
            time = transit(("x", -1 if d == 3 else 1), size, 2 if d == 2 else 1)
            at(time, lambda d=d: far(d))
        start(copy(0, t, other))
        at(transit("core", size, 1, 300e3), lambda: near(0))

    edge = halo.shape[0]
    kernel_size = conv_taps.shape[0]

    def gate():
        value_in = jnp.dot(
            normed[...], wc1[0].reshape(normed.shape[1], width), preferred_element_type=F32
        )
        gate_in = jnp.dot(
            normed[...], wc1[1].reshape(normed.shape[1], width), preferred_element_type=F32
        )
        gated[...] = (value_in * jax.nn.sigmoid(gate_in)).astype(BF)
        moving = remote(
            gated.at[pl.ds(length - edge, edge)], halo, halo_sem.at[0], halo_sem.at[1],
            {"sp": following, "tp": t},
        )
        moving.start()
        sent.append(moving)
        at(transit(("y", 1), edge * width * 2), convolve, 0.7)
        padded[edge:edge + length, :] = gated[...].astype(F32)

    def convolve():
        remote(
            gated.at[pl.ds(length - edge, edge)], halo, halo_sem.at[0], halo_sem.at[1],
            {"sp": preceding, "tp": t},
        ).wait_recv()
        padded[0:edge, :] = jnp.where(seq > 0, halo[...].astype(F32), 0.0)
        lag = edge - (kernel_size - 1)
        for lane in range(width // 128):
            lanes = slice(lane * 128, (lane + 1) * 128)
            answer = jnp.zeros((length, 128), F32)
            for b in range(8):
                tall = length + (8 if b else 0)
                part = jnp.zeros((tall, 128), F32)
                for a in range(edge // 8 + 1):
                    k = 8 * a + b - lag
                    if 0 <= k < kernel_size:
                        part = part + conv_taps[k:k + 1, lanes] * padded[8 * a:8 * a + tall, lanes]
                if b:
                    shifted[b, :, :] = part
                    answer = answer + shifted[b, b:b + length, :]
                else:
                    answer = answer + part
            conv_all[t, :, lanes] = answer.astype(BF)
        share(1, conv_all, lambda: at(clock[0], channel_norm, 2.0))

    def channel_norm():
        count = 2 * CHIPS * width
        def body(i, carry):
            part = pl.ds(pl.multiple_of(i * 16, 16), 16)
            pieces = [conv_all[c, part, :].astype(F32) for c in range(2 * CHIPS)]
            total = pieces[0]
            for piece in pieces[1:]:
                total = total + piece
            mean = jnp.sum(total, axis=1, keepdims=True) / count
            pieces = [piece - mean for piece in pieces]
            total = pieces[0] * pieces[0]
            for piece in pieces[1:]:
                total = total + piece * piece
            scale = lax.rsqrt(jnp.sum(total, axis=1, keepdims=True) / count + 1e-5)
            for c, piece in enumerate(pieces):
                lanes = slice(c * width, (c + 1) * width)
                value = piece * scale * chan_gain[:, lanes] + chan_shift[:, lanes]
                conv_act[c, part, :] = jax.nn.silu(value).astype(BF)
            return carry
        lax.fori_loop(0, length // 16, body, 0)
        conv_ready()

    columns = out.shape[1]

    def project(blocks, weights, lanes):
        total = None
        for c in range(2 * CHIPS):
            term = jnp.dot(
                blocks[c], weights[c].reshape(width, columns)[:, lanes], preferred_element_type=F32
            )
            total = term if total is None else total + term
        return total

    def state_out():
        for n in range(columns // 256):
            lanes = slice(n * 256, (n + 1) * 256)
            mixed[:, lanes] = project(act_all, ws2.at[0], lanes) * jax.nn.sigmoid(
                project(act_all, ws2.at[1], lanes)
            )
        conv_ready()

    def conv_out():
        for n in range(columns // 256):
            lanes = slice(n * 256, (n + 1) * 256)
            result[:, lanes] = (mixed[:, lanes] + project(conv_act, wc2, lanes)).astype(BF)
        moving = pltpu.make_async_copy(result, out, load_sem.at[7])
        moving.start()
        for copy in sent:
            copy.wait_send()
        moving.wait()

    state_ready = when_all(3, lambda: at(clock[0], state_out, 1.4))
    gate_ready = both(lambda: at(clock[0], gate, 1.0))
    conv_ready = when_all(3, lambda: at(clock[0], conv_out, 1.4))
    run()


def local(
    tokens, norm_gain, conv_value, conv_gate, state_feed, conv_taps, chan_gain, chan_shift,
    conv_project, decay_rate, frequency, input_real, input_imag, output_real, output_imag,
    skip_gain, state_value, state_gate, initial_state,
):
    length, features = tokens.shape
    groups, size, wide = input_real.shape
    flat, width = groups * size, groups * wide
    deep1, columns = conv_value.shape[0], conv_project.shape[1]
    deep2 = conv_project.shape[0]
    edge = 32
    args = (
        tokens, norm_gain.reshape(1, -1), conv_value, conv_gate, state_feed, conv_taps,
        chan_gain.reshape(1, -1), chan_shift.reshape(1, -1), conv_project, decay_rate, frequency,
        jnp.swapaxes(input_real, 1, 2), jnp.swapaxes(input_imag, 1, 2), output_real, output_imag,
        skip_gain.reshape(1, -1), state_value,
        state_gate, initial_state,
    )
    large = {0, 2, 3, 4, 8, 16, 17}
    anywhere = pl.BlockSpec(memory_space=pl.ANY)
    held = pl.BlockSpec(memory_space=pltpu.VMEM)
    vmem = pltpu.VMEM
    dma = pltpu.SemaphoreType.DMA
    return pl.pallas_call(
        kernel,
        out_shape=(
            jax.ShapeDtypeStruct((length, columns), BF),
            jax.ShapeDtypeStruct(initial_state.shape, F32),
        ),
        in_specs=[anywhere if i in large else held for i in range(len(args))],
        out_specs=(anywhere, held),
        scratch_shapes=[
            vmem((SIDE, SIDE, deep1, width), BF),
            vmem((2, SIDE, SIDE, deep1, width), BF),
            vmem((2, SIDE, SIDE, deep2, columns), BF),
            vmem((SIDE, SIDE, deep2, columns), BF),
            vmem((length, features), BF),
            vmem((length, features), BF),
            vmem((length, columns), BF),
            vmem((length, flat), F32),
            vmem((length, flat), F32),
            vmem((length, flat), F32),
            vmem((length, flat), F32),
            vmem((width, flat), BF),
            vmem((width, flat), BF),
            vmem((width, 2 * flat), BF),
            vmem((length, width), BF),
            vmem((length, 2 * flat), BF),
            vmem((length, 2 * flat), F32),
            vmem((length, 2 * flat), BF),
            vmem((16, flat), F32),
            vmem((SIDE, 1, 2 * flat), F32),
            vmem((SIDE, 1, 2 * flat), F32),
            vmem((length, width), BF),
            vmem((edge, width), BF),
            vmem((edge + length, width), F32),
            vmem((8, length + 8, 128), F32),
            vmem((2 * CHIPS, length, width), BF),
            vmem((2 * CHIPS, length, width), BF),
            vmem((2 * CHIPS, length, width), BF),
            vmem((length, columns), F32),
            dma((8,)),
            dma((12, len(SLOTS))),
            dma((12, len(SLOTS))),
            dma((2, SIDE - 1)),
            dma((2, SIDE - 1)),
            dma((2,)),
            dma((2, 7)),
            dma((2, 7)),
        ],
        compiler_params=pltpu.CompilerParams(
            collective_id=0, has_side_effects=True, vmem_limit_bytes=60 * 1024 * 1024
        ),
        name="mixer",
    )(*args)


def solution(mesh):
    in_specs = (
        P("sp", None), P(), P("sp", "tp"), P("sp", "tp"), P("sp", "tp"), P(None, "tp"), P(), P(),
        P("sp", "tp"), P("tp", None), P("tp", None), P("tp", None, None), P("tp", None, None),
        P("tp", None, None), P("tp", None, None), P("tp"), P("sp", "tp"), P("sp", "tp"),
        P(None, "tp", None),
    )
    out_specs = (P("sp", "tp"), P(None, "tp", None))
    return jax.shard_map(local, mesh=mesh, in_specs=in_specs, out_specs=out_specs, check_vma=False)
```

```python
import heapq

import jax
import jax.numpy as jnp
from jax import lax
from jax.experimental import pallas as pl
from jax.experimental.pallas import tpu as pltpu
from jax.sharding import PartitionSpec as P

BF, F32 = jnp.bfloat16, jnp.float32
HIGHEST = lax.Precision.HIGHEST
MESH = pl.DeviceIdType.MESH
SIDE = 8
CHIPS = 4
NT = (((1,), (1,)), ((), ()))


def hops(direction, half):
    return SIDE // 2 if (direction > 0) == (half == 0) else SIDE // 2 - 1


SLOTS = [
    (direction, half, k)
    for direction in (1, -1)
    for half in (0, 1)
    for k in range(hops(direction, half))
]
SLOT_OF = {slot: at for at, slot in enumerate(SLOTS)}


def rotate(first_real, first_imag, second_real, second_imag):
    return (
        first_real * second_real - first_imag * second_imag,
        first_real * second_imag + first_imag * second_real,
    )


def iota(shape, dim):
    return lax.broadcasted_iota(jnp.int32, shape, dim)


SMALL = (1, 5, 6, 7, 9, 10, 11, 12, 13, 14, 15, 18)


def kernel(*refs):
    (
        tokens, norm_gain, conv_value, conv_gate, state_feed, conv_taps, chan_gain, chan_shift,
        conv_project, decay_rate, frequency, input_real, input_imag, output_real, output_imag,
        skip_gain, state_value, state_gate, initial_state, out, final_out,
    ) = refs[:21]
    small = refs[21:21 + len(SMALL)]
    (
        ws1, wc1, ws2, wc2, stage_s1, stage_c1, stage_s2, stage_c2, raw, scale, normed, result,
        final_state, power_r, power_i, undo_r, undo_i, drive_r, drive_i, emit, feed, scaled, summed,
        states, rows, finals, totals, feed_half, feed_back, gated_half, gated_back, halo, padded,
        shifted, conv_all, act_all, conv_act, state_half, state_back, state_got, conv_half, conv_back,
        conv_got,
        load_sem, ring_send, ring_recv, scan_send, scan_recv, halo_sem, tp_send, tp_recv, pair_send,
        pair_recv,
    ) = refs[21 + len(SMALL):]
    seq = lax.axis_index("sp")
    t = lax.axis_index("tp")
    z, y = seq // SIDE, seq % SIDE
    chip, core = t // 2, t % 2
    length = tokens.shape[0]
    groups, wide, size = input_real.shape
    flat = groups * size
    width = groups * wide
    part_width = width // 2
    columns = out.shape[1]
    part_columns = columns // 2

    def device(zz, yy, tt):
        return {"sp": zz * SIDE + yy, "tp": tt}

    def step_to(at, by, count):
        return lax.rem(at + by + count, count)

    def remote(src, dst, send, recv, to):
        return pltpu.make_async_remote_copy(
            src_ref=src, dst_ref=dst, send_sem=send, recv_sem=recv, device_id=to, device_id_type=MESH
        )

    queue = []
    sent = []
    free = {}
    clock = [0.0, 0]

    def at(time, fn, cost=0.0):
        heapq.heappush(queue, (time, clock[1], cost, fn))
        clock[1] += 1

    def run():
        while queue:
            time, _, cost, fn = heapq.heappop(queue)
            clock[0] = max(clock[0], time)
            fn()
            clock[0] += cost

    def start(moving):
        moving.start()
        sent.append((clock[0], moving))

    def drain(before):
        kept = []
        for time, moving in sent:
            if time < before:
                moving.wait_send()
            else:
                kept.append((time, moving))
        sent[:] = kept

    def transit(link, size, count=1, rate=46.6e3):
        begin = max(clock[0], free.get(link, 0.0))
        free[link] = begin + size * count / rate
        return free[link] + 0.95 + 0.75 * count

    def when_all(number, fn):
        left = [number]

        def one():
            left[0] -= 1
            if left[0] == 0:
                fn()
        return one

    loads, counted = {}, []

    def load(name, src, dst):
        moving = pltpu.make_async_copy(src, dst, load_sem.at[len(counted)])
        moving.start()
        counted.append(name)
        loads.setdefault(name, []).append(moving)

    def after(*names):
        for name in names:
            for moving in loads.pop(name, []):
                moving.wait()

    here = {"z": z, "y": y}
    odd = {"z": z % 2, "y": y % 2}

    def lanes_from(half, count):
        return pl.ds(pl.multiple_of(half * count, count), count)

    def staged(name, axis, pieces, stage, own, count):
        for half in (0, 1):
            for i, source in enumerate(pieces):
                load(
                    name, source.at[:, half * count:(half + 1) * count],
                    stage.at[half, :, i * count:(i + 1) * count],
                )
        for i, source in enumerate(pieces):
            load(
                name, source.at[:, lanes_from(odd[axis], count)], own.at[:, i * count:(i + 1) * count]
            )

    staged("s1", "y", (state_feed,), stage_s1, ws1.at[z, y], part_width)
    staged("c1", "z", (conv_value, conv_gate), stage_c1, wc1.at[z, y], part_width)
    load("raw", tokens, raw)
    for i, place in enumerate(SMALL):
        load("small", refs[place], small[i])
    (
        norm_gain, conv_taps, chan_gain, chan_shift, decay_rate, frequency, input_real, input_imag,
        output_real, output_imag, skip_gain, initial_state,
    ) = small
    staged("s2", "y", (state_value, state_gate), stage_s2, ws2.at[z, y], part_columns)
    staged("c2", "z", (conv_project,), stage_c2, wc2.at[z, y], part_columns)

    barrier = pltpu.get_barrier_semaphore()
    following = lax.rem(seq + 1, SIDE * SIDE)
    preceding = lax.rem(seq + SIDE * SIDE - 1, SIDE * SIDE)
    partners = []
    for d in range(1, SIDE):
        partners.append(device(z, step_to(y, d, SIDE), t))
        partners.append(device(step_to(z, d, SIDE), y, t))
    for d in range(1, 2 * CHIPS):
        partners.append(device(z, y, step_to(t, d, 2 * CHIPS)))
    partners.append({"sp": following, "tp": t})
    partners.append({"sp": preceding, "tp": t})
    for partner in partners:
        pl.semaphore_signal(barrier, inc=1, device_id=partner, device_id_type=MESH)
    pl.semaphore_wait(barrier, len(partners))

    def beside(axis, by):
        moved = step_to(here[axis], by, SIDE)
        return device(moved, y, t) if axis == "z" else device(z, moved, t)

    def ring(number, axis, block, size, done, nearly=None):
        position = here[axis]
        finished = when_all(len(SLOTS), done)
        passed = when_all(len(SLOTS) - 4, nearly or (lambda: None))

        def copy(direction, half, k, source):
            slot = SLOT_OF[(direction, half, k)]
            return remote(
                block(source, half), block(source, half),
                ring_send.at[number, slot], ring_recv.at[number, slot], beside(axis, direction),
            )

        def send(direction, half, k):
            moving = copy(direction, half, k, step_to(position, -direction * k, SIDE))
            start(moving)
            time = transit((axis, direction), size)
            at(time, lambda: arrived(direction, half, k))

        def arrived(direction, half, k):
            source = step_to(position, -direction * (k + 1), SIDE)
            copy(direction, half, k, source).wait_recv()
            if k + 1 < hops(direction, half):
                send(direction, half, k + 1)
                passed()
            finished()

        def first():
            for half in (0, 1):
                for direction in (1, -1):
                    send(direction, half, 0)
        return first

    def spread_out(sems, axis, block, size, done):
        position = here[axis]
        finished = when_all(SIDE - 1, done)

        def copy(d, source, to):
            return remote(block(source), block(source), sems[0](d), sems[1](d), to)

        def arrived(d):
            copy(d, step_to(position, -d, SIDE), beside(axis, -d)).wait_recv()
            finished()

        def first():
            for d in (4, 3, 5, 2, 6, 1, 7):
                moving = copy(d, position, beside(axis, d))
                start(moving)
                direction, count = (1, d) if d <= SIDE // 2 else (-1, SIDE - d)
                time = transit((axis, direction), size, count)
                at(time, lambda d=d: arrived(d))
        return first

    def deal(number, axis, stage, block, size, done):
        position = here[axis]
        finished = when_all(SIDE - 1, done)

        def copy(d, source, to):
            half = odd[axis] if d % 2 == 0 else 1 - odd[axis]
            return remote(
                stage.at[half], block(source), ring_send.at[number, d], ring_recv.at[number, d], to
            )

        def arrived(d):
            copy(d, step_to(position, -d, SIDE), beside(axis, -d)).wait_recv()
            finished()

        def first():
            for d in (4, 3, 5, 2, 6, 1, 7):
                start(copy(d, position, beside(axis, d)))
                direction, count = (1, d) if d <= SIDE // 2 else (-1, SIDE - d)
                time = transit((axis, direction), size, count)
                at(time, lambda d=d: arrived(d))
        return first

    def mate(axis):
        other_one = here[axis] + 1 - 2 * odd[axis]
        return device(other_one, y, t) if axis == "z" else device(z, other_one, t)

    def hand_over(number, axis, src, dst, landing, size, done):
        start(remote(src, dst, pair_send.at[number], pair_recv.at[number], mate(axis)))
        time = max(transit((axis, 1), size), transit((axis, -1), size))

        def arrived():
            remote(src, landing, pair_send.at[number], pair_recv.at[number], mate(axis)).wait_recv()
            done()
        at(time, arrived)

    other = t + 1 - 2 * core

    def share(number, block, tall, size, done):
        finished = when_all(5, done)
        halves = (pl.ds(0, tall // 2), pl.ds(tall // 2, tall // 2))
        whole = pl.ds(0, tall)

        def copy(slot, source, part, to):
            return remote(
                block(source).at[part], block(source).at[part], tp_send.at[number, slot],
                tp_recv.at[number, slot], device(z, y, to),
            )

        def from_chip(d, which):
            return step_to(chip, -d, CHIPS) * 2 + which

        def near(slot, source, part):
            copy(slot, source, part, other).wait_recv()
            finished()

        def to_core(slot, d, part, amount):
            start(copy(slot, from_chip(d, core), part, other))
            source = from_chip(d, 1 - core)
            at(transit("core", amount, 1, 300e3), lambda: near(slot, source, part))

        def far(d):
            copy(d, from_chip(d, core), whole, from_chip(d, core)).wait_recv()
            half, onward, slot, hop = (0, 1, 2, 1) if d == 1 else (1, 3, 4, -1)
            start(copy(slot, from_chip(d, core), halves[half], from_chip(-onward, core)))
            at(transit(("x", hop), size / 2), lambda: farther(slot, half))
            to_core(4 + d, d, whole, size)

        def farther(slot, half):
            copy(slot, from_chip(2, core), halves[half], other).wait_recv()
            to_core(4 + slot, 2, halves[half], size / 2)

        for d, hop in ((1, 1), (3, -1)):
            start(copy(d, t, whole, step_to(chip, d, CHIPS) * 2 + core))
            at(transit(("x", hop), size), lambda d=d: far(d))
        start(copy(0, t, whole, other))
        at(transit("core", size, 1, 300e3), lambda: near(0, other, whole))

    quarter = SIDE // 2
    unit1 = ws1.shape[2] * part_width * 2

    def both(fn):
        return when_all(2, fn)

    s1_big = ring(
        0, "z", lambda i, h: ws1.at[i, pl.ds(h * quarter, quarter)], 4 * unit1,
        lambda: (s1_own(), s1_far()), lambda: go_s2(),
    )
    s2_big = ring(
        1, "z", lambda i, h: ws2.at[i, pl.ds(h * quarter, quarter)], 8 * unit1,
        lambda: (state_own(), state_far()),
    )
    c1_big = ring(
        2, "y", lambda i, h: wc1.at[pl.ds(h * quarter, quarter), i], 8 * unit1,
        lambda: (c1_own(), c1_far()), lambda: go_c2(),
    )
    c2_big = ring(
        3, "y", lambda i, h: wc2.at[pl.ds(h * quarter, quarter), i], 4 * unit1,
        lambda: (conv_own(), conv_far()),
    )
    go_s2, go_c2 = both(s2_big), both(c2_big)
    s1_small = deal(4, "y", stage_s1, lambda i: ws1.at[z, i], unit1, s1_big)
    c1_small = deal(5, "z", stage_c1, lambda i: wc1.at[i, y], 2 * unit1, c1_big)
    s2_small = deal(6, "y", stage_s2, lambda i: ws2.at[z, i], 2 * unit1, lambda: go_s2())
    c2_small = deal(7, "z", stage_c2, lambda i: wc2.at[i, y], unit1, lambda: go_c2())

    def begin():
        after("s1")
        s1_small()
        after("c1")
        c1_small()

    def begin_second():
        after("s2", "c2")
        c2_small()
        s2_small()

    at(0.0, begin)
    at(10.0, begin_second)

    step = normed.shape[3]

    def measure():
        after("raw", "small")
        def body(i, carry):
            part = pl.ds(pl.multiple_of(i * 16, 16), 16)
            value = raw[part, :].astype(F32)
            mean = jnp.mean(value * value, axis=1, keepdims=True)
            scale[part, :] = jnp.broadcast_to(lax.rsqrt(mean + 1e-6), (16, 128))
            return carry
        lax.fori_loop(0, length // 16, body, 0)
        normalise(t)
        for i, axis in ((1, "y"), (2, "z")):
            hand_over(
                i, axis, normed.at[0, t], normed.at[i, t], normed.at[i, t], length * step * 2,
                lambda i=i: share(
                    i, lambda c: normed.at[i, c], length, length * step * 2,
                    (lambda: s1_far()) if i == 1 else (lambda: c1_far()),
                ),
            )

    def normalise(c):
        lanes = lanes_from(c, step)
        value = raw[:, lanes].astype(F32)
        normed[0, c] = (value * scale[:, 0:1] * norm_gain[:, lanes]).astype(BF)

    def normalise_all():
        def body(c, carry):
            pl.when(c != t)(lambda: normalise(c))
            return carry
        lax.fori_loop(0, 2 * CHIPS, body, 0)

    def spread():
        return ((iota((size, flat), 1) & (size - 1)) == iota((size, flat), 0)).astype(F32)

    def owner():
        return (iota((groups, flat), 1) // size) == iota((groups, flat), 0)

    def as_row(table):
        wide_table = jnp.dot(table, spread(), precision=HIGHEST, preferred_element_type=F32)
        return jnp.sum(jnp.where(owner(), wide_table, 0.0), axis=0, keepdims=True)

    def as_table(row):
        return lax.dot_general(
            jnp.where(owner(), row, 0.0), spread(), NT, precision=HIGHEST, preferred_element_type=F32
        )

    total_tokens = length * SIDE * SIDE

    def tables():
        rate = -as_row(decay_rate[...]) / total_tokens
        turn = as_row(frequency[...])
        rows[0:1, :] = as_row(initial_state[0])
        rows[1:2, :] = as_row(initial_state[1])
        magnitude = jnp.exp(rate)
        step_r = magnitude * jnp.cos(turn)
        step_i = magnitude * jnp.sin(turn)
        modulus = rate * rate + turn * turn
        lift = step_r - 1.0
        factor_r = (lift * rate + step_i * turn) / modulus
        factor_i = (step_i * rate - lift * turn) / modulus
        count = iota((8, flat), 0) + 1
        block_r, block_i = jnp.ones((8, flat), F32), jnp.zeros((8, flat), F32)
        square_r, square_i = step_r, step_i
        for place in range(4):
            chosen = ((count >> place) & 1) == 1
            next_r, next_i = rotate(block_r, block_i, square_r, square_i)
            block_r = jnp.where(chosen, next_r, block_r)
            block_i = jnp.where(chosen, next_i, block_i)
            if place < 3:
                square_r, square_i = rotate(square_r, square_i, square_r, square_i)
        rows[2:3, :], rows[3:4, :] = square_r, square_i
        rows[4:5, :], rows[5:6, :] = factor_r, factor_i

        def body(i, carry):
            now_r, now_i = carry
            part = pl.ds(pl.multiple_of(i * 8, 8), 8)
            power_r[part, :], power_i[part, :] = now_r, now_i
            inverse = 1.0 / (now_r * now_r + now_i * now_i)
            un_r, un_i = rotate(now_r * inverse, -now_i * inverse, rows[4:5, :], rows[5:6, :])
            undo_r[part, :], undo_i[part, :] = un_r, un_i
            return rotate(now_r, now_i, rows[2:3, :], rows[3:4, :])
        lax.fori_loop(0, length // 8, body, (block_r, block_i))

    def matrices():
        stretch = spread().astype(BF)
        def fill(source, sign, dest, lanes):
            for g in range(groups):
                copied = jnp.dot((sign * source[g]).astype(BF), stretch, preferred_element_type=F32)
                kept = iota((wide, flat), 1) // size == g
                dest[g * wide:(g + 1) * wide, lanes] = jnp.where(kept, copied, 0.0).astype(BF)
        fill(input_real, 1.0, drive_r, slice(0, flat))
        fill(input_imag, 1.0, drive_i, slice(0, flat))
        fill(output_real, 1.0, emit, slice(0, flat))
        fill(output_imag, -1.0, emit, slice(flat, 2 * flat))

    at(0.5, measure, 1.0)
    at(6.0, normalise_all, 1.5)
    at(8.0, tables, 1.4)
    at(9.0, matrices, 1.0)

    chunk = 256

    def project_in(i, weights):
        count = weights.shape[3]
        total = None
        for c in range(2 * CHIPS):
            term = jnp.dot(normed[i, c], weights[c].reshape(step, count), preferred_element_type=F32)
            total = term if total is None else total + term
        return total

    def feed_own():
        feed_half[odd["y"]] = project_in(0, ws1).astype(BF)
        recur_ready()

    def feed_far():
        feed_back[...] = project_in(1, ws1).astype(BF)
        hand_over(
            3, "y", feed_back, feed_half.at[odd["y"]], feed_half.at[1 - odd["y"]],
            length * part_width * 2, lambda: recur_ready(),
        )

    s1_own = when_all(1, lambda: at(clock[0], feed_own, 0.6))
    s1_far = both(lambda: at(clock[0], feed_far, 0.6))
    recur_ready = both(lambda: at(clock[0], recur, 1.4))

    def recur():
        feed[:, 0:part_width] = feed_half[0]
        feed[:, part_width:width] = feed_half[1]
        drive = feed[...]
        for j in range(flat // chunk):
            part = slice(j * chunk, (j + 1) * chunk)
            shift = slice(flat + j * chunk, flat + (j + 1) * chunk)
            push_r = jnp.dot(drive, drive_r[:, part], preferred_element_type=F32)
            push_i = jnp.dot(drive, drive_i[:, part], preferred_element_type=F32)
            back_r, back_i = rotate(undo_r[:, part], undo_i[:, part], push_r, push_i)
            scaled[:, part] = back_r.astype(BF)
            scaled[:, shift] = back_i.astype(BF)
        lower = (iota((length, length), 0) >= iota((length, length), 1)).astype(BF)
        for j in range(2 * flat // chunk):
            part = slice(j * chunk, (j + 1) * chunk)
            summed[:, part] = jnp.dot(lower, scaled[:, part], preferred_element_type=F32)
        end_r, end_i = rotate(
            power_r[length - 1:length, :], power_i[length - 1:length, :],
            summed[length - 1:length, 0:flat], summed[length - 1:length, flat:2 * flat],
        )
        finals[y, :, 0:flat], finals[y, :, flat:2 * flat] = end_r, end_i
        spread_out(
            scan_sems(0), "y", lambda i: finals.at[i], 8 * flat, lambda: at(clock[0], scan_row, 0.1)
        )()

    def scan_sems(number):
        return (
            lambda d: scan_send.at[number, d - 1],
            lambda d: scan_recv.at[number, d - 1],
        )

    def scan_row():
        span_r, span_i = power_r[length - 1:length, :], power_i[length - 1:length, :]
        zero = jnp.zeros((1, flat), F32)
        sum_r, sum_i, before_r, before_i = zero, zero, zero, zero
        jump_r, jump_i = zero + 1.0, zero
        mine_r, mine_i = zero, zero
        for yy in range(SIDE):
            before_r, before_i = jnp.where(y == yy, sum_r, before_r), jnp.where(y == yy, sum_i, before_i)
            mine_r, mine_i = jnp.where(y == yy, jump_r, mine_r), jnp.where(y == yy, jump_i, mine_i)
            next_r, next_i = rotate(span_r, span_i, sum_r, sum_i)
            sum_r = next_r + finals[yy, :, 0:flat]
            sum_i = next_i + finals[yy, :, flat:2 * flat]
            jump_r, jump_i = rotate(span_r, span_i, jump_r, jump_i)
        rows[6:7, :], rows[7:8, :] = before_r, before_i
        rows[8:9, :], rows[9:10, :] = mine_r, mine_i
        rows[10:11, :], rows[11:12, :] = jump_r, jump_i
        totals[z, :, 0:flat], totals[z, :, flat:2 * flat] = sum_r, sum_i
        spread_out(
            scan_sems(1), "z", lambda i: totals.at[i], 8 * flat, lambda: at(clock[0], scan_all, 2.5)
        )()

    def scan_all():
        sum_r, sum_i = rows[0:1, :], rows[1:2, :]
        jump_r, jump_i = rows[10:11, :], rows[11:12, :]
        start_r, start_i = sum_r, sum_i
        for zz in range(SIDE):
            start_r, start_i = jnp.where(z == zz, sum_r, start_r), jnp.where(z == zz, sum_i, start_i)
            next_r, next_i = rotate(jump_r, jump_i, sum_r, sum_i)
            sum_r = next_r + totals[zz, :, 0:flat]
            sum_i = next_i + totals[zz, :, flat:2 * flat]
        final_state[0] = as_table(sum_r)
        final_state[1] = as_table(sum_i)
        load("final", final_state, final_out)
        lead_r, lead_i = rotate(rows[8:9, :], rows[9:10, :], start_r, start_i)
        entry_r, entry_i = lead_r + rows[6:7, :], lead_i + rows[7:8, :]
        for j in range(flat // chunk):
            part = slice(j * chunk, (j + 1) * chunk)
            shift = slice(flat + j * chunk, flat + (j + 1) * chunk)
            state_r, state_i = rotate(
                power_r[:, part], power_i[:, part],
                summed[:, part] + entry_r[:, part], summed[:, shift] + entry_i[:, part],
            )
            states[:, part] = state_r.astype(BF)
            states[:, shift] = state_i.astype(BF)
        answer = lax.dot_general(states[...], emit[...], NT, preferred_element_type=F32)
        answer = answer + skip_gain[...] * feed[...].astype(F32)
        act_all[0, t] = jax.nn.gelu(answer).astype(BF)
        exchange(3, "y", act_all, lambda: state_own(), lambda: state_far())

    def exchange(number, axis, blocks, own, far):
        amount = length * width * 2
        hand_over(
            number + 1, axis, blocks.at[0, t], blocks.at[1, t], blocks.at[1, t], amount,
            lambda: share(number + 1, lambda c: blocks.at[1, c], length, amount, far),
        )
        share(number, lambda c: blocks.at[0, c], length, amount, own)

    edge = halo.shape[1]
    kernel_size = conv_taps.shape[0]

    def gate(i):
        pair = project_in(i, wc1)
        return (pair[:, 0:part_width] * jax.nn.sigmoid(pair[:, part_width:width])).astype(BF)

    def gate_own():
        gated_half[odd["z"]] = gate(0)
        gate_ready()

    def gate_far():
        gated_back[...] = gate(2)
        hand_over(
            5, "z", gated_back, gated_half.at[odd["z"]], gated_half.at[1 - odd["z"]],
            length * part_width * 2, lambda: gate_ready(),
        )

    c1_own = when_all(1, lambda: at(clock[0], gate_own, 0.7))
    c1_far = both(lambda: at(clock[0], gate_far, 0.7))
    gate_ready = both(lambda: at(clock[0], pass_edge, 0.1))
    last = pl.ds(length - edge, edge)

    def pass_edge():
        start(
            remote(
                gated_half.at[:, last], halo, halo_sem.at[0], halo_sem.at[1],
                {"sp": following, "tp": t},
            )
        )
        at(transit(("y", 1), edge * width * 2), convolve, 0.7)
        for half in (0, 1):
            lanes = slice(half * part_width, (half + 1) * part_width)
            padded[edge:edge + length, lanes] = gated_half[half].astype(F32)

    def convolve():
        remote(
            gated_half.at[:, last], halo, halo_sem.at[0], halo_sem.at[1],
            {"sp": preceding, "tp": t},
        ).wait_recv()
        for half in (0, 1):
            lanes = slice(half * part_width, (half + 1) * part_width)
            padded[0:edge, lanes] = jnp.where(seq > 0, halo[half].astype(F32), 0.0)
        lag = edge - (kernel_size - 1)
        for lane in range(width // 128):
            lanes = slice(lane * 128, (lane + 1) * 128)
            answer = jnp.zeros((length, 128), F32)
            for b in range(8):
                tall = length + (8 if b else 0)
                part = jnp.zeros((tall, 128), F32)
                for a in range(edge // 8 + 1):
                    k = 8 * a + b - lag
                    if 0 <= k < kernel_size:
                        part = part + conv_taps[k:k + 1, lanes] * padded[8 * a:8 * a + tall, lanes]
                if b:
                    shifted[b, :, :] = part
                    answer = answer + shifted[b, b:b + length, :]
                else:
                    answer = answer + part
            conv_all[0, t, :, lanes] = answer.astype(BF)
        exchange(
            6, "z", conv_all, lambda: at(clock[0], lambda: channel_norm(0), 2.5),
            lambda: at(clock[0], lambda: channel_norm(1), 2.5),
        )

    def channel_norm(which):
        count = 2 * CHIPS * width
        def body(i, carry):
            part = pl.ds(pl.multiple_of(i * 16, 16), 16)
            pieces = [conv_all[which, c, part, :].astype(F32) for c in range(2 * CHIPS)]
            total = pieces[0]
            for piece in pieces[1:]:
                total = total + piece
            mean = jnp.sum(total, axis=1, keepdims=True) / count
            pieces = [piece - mean for piece in pieces]
            total = pieces[0] * pieces[0]
            for piece in pieces[1:]:
                total = total + piece * piece
            scale = lax.rsqrt(jnp.sum(total, axis=1, keepdims=True) / count + 1e-5)
            for c, piece in enumerate(pieces):
                lanes = slice(c * width, (c + 1) * width)
                value = piece * scale * chan_gain[:, lanes] + chan_shift[:, lanes]
                conv_act[which, c, part, :] = jax.nn.silu(value).astype(BF)
            return carry
        lax.fori_loop(0, length // 16, body, 0)
        (conv_far if which else conv_own)()

    def project(blocks, i, weights):
        count = weights.shape[3]
        total = None
        for c in range(2 * CHIPS):
            term = jnp.dot(
                blocks[i, c], weights[c].reshape(width, count), preferred_element_type=F32
            )
            total = term if total is None else total + term
        return total

    def state_out(i):
        pair = project(act_all, i, ws2)
        return pair[:, 0:part_columns] * jax.nn.sigmoid(pair[:, part_columns:columns])

    def state_out_own():
        state_half[odd["y"]] = state_out(0)
        finish_ready()

    def state_out_far():
        state_back[...] = state_out(1).astype(BF)
        hand_over(
            6, "y", state_back, state_got, state_got, length * part_columns * 2, state_returned
        )

    def state_returned():
        state_half[1 - odd["y"]] = state_got[...].astype(F32)
        finish_ready()

    def conv_out_own():
        conv_half[odd["z"]] = project(conv_act, 0, wc2)
        finish_ready()

    def conv_out_far():
        conv_back[...] = project(conv_act, 1, wc2).astype(BF)
        hand_over(8, "z", conv_back, conv_got, conv_got, length * part_columns * 2, conv_returned)

    def conv_returned():
        conv_half[1 - odd["z"]] = conv_got[...].astype(F32)
        finish_ready()

    state_own = both(lambda: at(clock[0], state_out_own, 0.8))
    state_far = both(lambda: at(clock[0], state_out_far, 0.8))
    conv_own = both(lambda: at(clock[0], conv_out_own, 0.6))
    conv_far = both(lambda: at(clock[0], conv_out_far, 0.6))
    finish_ready = when_all(4, lambda: at(clock[0], finish, 0.5))

    def finish():
        for half in (0, 1):
            lanes = slice(half * part_columns, (half + 1) * part_columns)
            result[:, lanes] = (state_half[half] + conv_half[half]).astype(BF)
        load("out", result, out)
        drain(1e9)
        after("final", "out")

    at(35.0, lambda: drain(25.0))
    at(48.0, lambda: drain(38.0))
    at(57.0, lambda: drain(50.0))
    run()


def local(
    tokens, norm_gain, conv_value, conv_gate, state_feed, conv_taps, chan_gain, chan_shift,
    conv_project, decay_rate, frequency, input_real, input_imag, output_real, output_imag,
    skip_gain, state_value, state_gate, initial_state,
):
    length, features = tokens.shape
    groups, size, wide = input_real.shape
    flat, width = groups * size, groups * wide
    deep1, columns = conv_value.shape[0], conv_project.shape[1]
    deep2 = conv_project.shape[0]
    edge = 32
    args = (
        tokens, norm_gain.reshape(1, -1), conv_value, conv_gate, state_feed, conv_taps,
        chan_gain.reshape(1, -1), chan_shift.reshape(1, -1), conv_project, decay_rate, frequency,
        jnp.swapaxes(input_real, 1, 2), jnp.swapaxes(input_imag, 1, 2), output_real, output_imag,
        skip_gain.reshape(1, -1), state_value, state_gate, initial_state,
    )
    anywhere = pl.BlockSpec(memory_space=pl.ANY)
    vmem = pltpu.VMEM
    dma = pltpu.SemaphoreType.DMA
    many = 2 * CHIPS
    return pl.pallas_call(
        kernel,
        out_shape=(
            jax.ShapeDtypeStruct((length, columns), BF),
            jax.ShapeDtypeStruct(initial_state.shape, F32),
        ),
        in_specs=[anywhere] * len(args),
        out_specs=(anywhere, anywhere),
        scratch_shapes=[
            *(vmem(args[i].shape, args[i].dtype) for i in SMALL),
            vmem((SIDE, SIDE, deep1, width // 2), BF),
            vmem((SIDE, SIDE, deep1, width), BF),
            vmem((SIDE, SIDE, deep2, columns), BF),
            vmem((SIDE, SIDE, deep2, columns // 2), BF),
            vmem((2, deep1, width // 2), BF),
            vmem((2, deep1, width), BF),
            vmem((2, deep2, columns), BF),
            vmem((2, deep2, columns // 2), BF),
            vmem((length, features), BF),
            vmem((length, 128), F32),
            vmem((3, many, length, features // many), BF),
            vmem((length, columns), BF),
            vmem(initial_state.shape, F32),
            *(vmem((length, flat), F32) for _ in range(4)),
            vmem((width, flat), BF),
            vmem((width, flat), BF),
            vmem((width, 2 * flat), BF),
            vmem((length, width), BF),
            vmem((length, 2 * flat), BF),
            vmem((length, 2 * flat), F32),
            vmem((length, 2 * flat), BF),
            vmem((16, flat), F32),
            vmem((SIDE, 1, 2 * flat), F32),
            vmem((SIDE, 1, 2 * flat), F32),
            vmem((2, length, width // 2), BF),
            vmem((length, width // 2), BF),
            vmem((2, length, width // 2), BF),
            vmem((length, width // 2), BF),
            vmem((2, edge, width // 2), BF),
            vmem((edge + length, width), F32),
            vmem((8, length + 8, 128), F32),
            *(vmem((2, many, length, width), BF) for _ in range(3)),
            *(
                vmem(shape, held)
                for _ in range(2)
                for shape, held in (
                    ((2, length, columns // 2), F32),
                    ((length, columns // 2), BF),
                    ((length, columns // 2), BF),
                )
            ),
            dma((40,)),
            dma((8, len(SLOTS))),
            dma((8, len(SLOTS))),
            dma((2, SIDE - 1)),
            dma((2, SIDE - 1)),
            dma((2,)),
            dma((8, 9)),
            dma((8, 9)),
            dma((9,)),
            dma((9,)),
        ],
        compiler_params=pltpu.CompilerParams(
            collective_id=0, has_side_effects=True, vmem_limit_bytes=62 * 1024 * 1024
        ),
        name="mixer",
    )(*args)


def solution(mesh):
    in_specs = (
        P("sp", None), P(), P("sp", "tp"), P("sp", "tp"), P("sp", "tp"), P(None, "tp"), P(), P(),
        P("sp", "tp"), P("tp", None), P("tp", None), P("tp", None, None), P("tp", None, None),
        P("tp", None, None), P("tp", None, None), P("tp"), P("sp", "tp"), P("sp", "tp"),
        P(None, "tp", None),
    )
    out_specs = (P("sp", "tp"), P(None, "tp", None))
    return jax.shard_map(local, mesh=mesh, in_specs=in_specs, out_specs=out_specs, check_vma=False)
```

```python
import heapq

import jax
import jax.numpy as jnp
from jax import lax
from jax.experimental import pallas as pl
from jax.experimental.pallas import tpu as pltpu
from jax.sharding import PartitionSpec as P

BF, F32 = jnp.bfloat16, jnp.float32
HIGHEST = lax.Precision.HIGHEST
MESH = pl.DeviceIdType.MESH
SIDE = 8
WINDOW = (2, 2, 9, 2)
WHEN = (16.0, 14.0, 12.0)
CLASSES = ((0,), (1, 7, 2, 6), (3, 5, 4))
CHIPS = 4
NT = (((1,), (1,)), ((), ()))


def hops(direction, half):
    return SIDE // 2 if (direction > 0) == (half == 0) else SIDE // 2 - 1


def slot_of(direction, half, k):
    return k if direction > 0 else hops(1, half) + k


def rotate(first_real, first_imag, second_real, second_imag):
    return (
        first_real * second_real - first_imag * second_imag,
        first_real * second_imag + first_imag * second_real,
    )


def iota(shape, dim):
    return lax.broadcasted_iota(jnp.int32, shape, dim)


SMALL = (1, 5, 6, 7, 9, 10, 11, 12, 13, 14, 15, 18)


def kernel(*refs):
    (
        tokens, norm_gain, conv_value, conv_gate, state_feed, conv_taps, chan_gain, chan_shift,
        conv_project, decay_rate, frequency, input_real, input_imag, output_real, output_imag,
        skip_gain, state_value, state_gate, initial_state, out, final_out,
    ) = refs[:21]
    small = refs[21:21 + len(SMALL)]
    (
        ws1, wc1, ws2, wc2, stage_s1, stage_c1, stage_s2, stage_c2, raw, scale, normed, result,
        final_state, power_r, power_i, undo_r, undo_i, drive_r, drive_i, emit, feed, scaled, summed,
        states, rows, finals, totals, feed_half, feed_back, gated_half, gated_back, halo, padded,
        shifted, conv_all, act_all, conv_act, state_half, state_back, state_got, conv_half, conv_back,
        conv_got,
        load_sem, ring_send, ring_recv, scan_send, scan_recv, halo_sem, tp_send, tp_recv, pair_send,
        pair_recv, deal_send, deal_recv,
    ) = refs[21 + len(SMALL):]
    seq = lax.axis_index("sp")
    t = lax.axis_index("tp")
    z, y = seq // SIDE, seq % SIDE
    chip, core = t // 2, t % 2
    length = tokens.shape[0]
    groups, wide, size = input_real.shape
    flat = groups * size
    width = groups * wide
    part_width = width // 2
    columns = out.shape[1]
    part_columns = columns // 2

    def device(zz, yy, tt):
        return {"sp": zz * SIDE + yy, "tp": tt}

    def step_to(at, by, count):
        return lax.rem(at + by + count, count)

    def remote(src, dst, send, recv, to):
        return pltpu.make_async_remote_copy(
            src_ref=src, dst_ref=dst, send_sem=send, recv_sem=recv, device_id=to, device_id_type=MESH
        )

    queue = []
    sent = []
    free = {}
    clock = [0.0, 0]

    def at(time, fn, cost=0.0):
        heapq.heappush(queue, (time, clock[1], cost, fn))
        clock[1] += 1

    def run():
        while queue:
            time, _, cost, fn = heapq.heappop(queue)
            clock[0] = max(clock[0], time)
            fn()
            clock[0] += cost

    def start(moving):
        moving.start()
        sent.append((clock[0], moving))

    closing = []

    def drain(before):
        kept = []
        for time, moving in sent:
            if time < before:
                moving.wait_send()
            else:
                kept.append((time, moving))
        sent[:] = kept

    def transit(link, size, count=1, rate=46.6e3):
        begin = max(clock[0], free.get(link, 0.0))
        free[link] = begin + size * count / rate
        return free[link] + 0.95 + 0.75 * count

    def when_all(number, fn):
        left = [number]

        def one():
            left[0] -= 1
            if left[0] == 0:
                fn()
        return one

    loads, counted = {}, []

    def load(name, src, dst):
        if name not in counted:
            counted.append(name)
        moving = pltpu.make_async_copy(src, dst, load_sem.at[counted.index(name)])
        moving.start()
        loads[name] = moving

    def bytes_of(ref, sem):
        pltpu.make_async_copy(ref, ref, sem).wait()

    def after(name, three=None):
        if three is None:
            loads[name].wait()
        else:
            bytes_of(three, load_sem.at[counted.index(name)])

    here = {"z": z, "y": y}
    odd = {"z": z % 2, "y": y % 2}

    def lanes_from(half, count):
        return pl.ds(pl.multiple_of(half * count, count), count)

    def staged(name, axis, pieces, stage, own, count):
        for half in (0, 1):
            for i, source in enumerate(pieces):
                load(
                    name, source.at[:, half * count:(half + 1) * count],
                    stage.at[half, :, i * count:(i + 1) * count],
                )
        for i, source in enumerate(pieces):
            load(
                name, source.at[:, lanes_from(odd[axis], count)], own.at[:, i * count:(i + 1) * count]
            )

    staged("s1", "y", (state_feed,), stage_s1, ws1.at[z, y], part_width)
    staged("c1", "z", (conv_value, conv_gate), stage_c1, wc1.at[z, y], part_width)
    load("raw", tokens, raw)
    for i, place in enumerate(SMALL):
        load(place, refs[place], small[i])
    (
        norm_gain, conv_taps, chan_gain, chan_shift, decay_rate, frequency, input_real, input_imag,
        output_real, output_imag, skip_gain, initial_state,
    ) = small
    staged("s2", "y", (state_value, state_gate), stage_s2, ws2.at[z, y], part_columns)
    staged("c2", "z", (conv_project,), stage_c2, wc2.at[z, y], part_columns)

    barrier = pltpu.get_barrier_semaphore()
    following = lax.rem(seq + 1, SIDE * SIDE)
    preceding = lax.rem(seq + SIDE * SIDE - 1, SIDE * SIDE)
    partners = []
    for d in range(1, SIDE):
        partners.append(device(z, step_to(y, d, SIDE), t))
        partners.append(device(step_to(z, d, SIDE), y, t))
    for d in range(1, 2 * CHIPS):
        partners.append(device(z, y, step_to(t, d, 2 * CHIPS)))
    partners.append({"sp": following, "tp": t})
    partners.append({"sp": preceding, "tp": t})
    for partner in partners:
        pl.semaphore_signal(barrier, inc=1, device_id=partner, device_id_type=MESH)
    pl.semaphore_wait(barrier, len(partners))

    def beside(axis, by):
        moved = step_to(here[axis], by, SIDE)
        return device(moved, y, t) if axis == "z" else device(z, moved, t)

    def spread_out(number, axis, blocks, size, done):
        position = here[axis]
        all_others = blocks.at[pl.ds(0, SIDE - 1)]
        latest = 0.0
        for d in (4, 3, 5, 2, 6, 1, 7):
            remote(
                blocks.at[position], blocks.at[position], scan_send.at[number],
                scan_recv.at[number], beside(axis, d),
            ).start()
            direction, count = (1, d) if d <= SIDE // 2 else (-1, SIDE - d)
            latest = max(latest, transit((axis, direction), size, count))

        def arrived():
            bytes_of(all_others, scan_recv.at[number])
            done()
        at(latest, arrived)
        closing.append(lambda: bytes_of(all_others, scan_send.at[number]))

    def trains(number, axis, across, stage, block, several, size, window, done, nearly=None):
        position, lane = here[axis], here[across]
        members = [
            (which, direction, k)
            for which in range(len(CLASSES)) for direction in (1, -1) for k in range(SIDE // 2)
            if any(k < hops(direction, d % 2) for d in CLASSES[which])
        ]
        finished = when_all(len(members), done)
        passed = when_all(len(CLASSES), nearly or (lambda: None))
        ready, active = [], [0]
        left = [len(c) * (SIDE - 1) for c in CLASSES]

        def dealt(d, source, to):
            half = odd[across] if d % 2 == 0 else 1 - odd[across]
            return remote(
                stage.at[half], block(position, source), deal_send.at[number],
                deal_recv.at[number, int(d in CLASSES[-1])], to,
            )

        def slot(which, direction, k):
            return members.index((which, direction, k))

        def copy(which, d, direction, k, source):
            held = block(source, step_to(lane, -d, SIDE))
            return remote(
                held, held, ring_send.at[number], ring_recv.at[number, slot(which, direction, k)],
                beside(axis, direction),
            )

        def send(which, direction, k):
            time = 0.0
            for d in CLASSES[which]:
                if k < hops(direction, d % 2):
                    copy(which, d, direction, k, step_to(position, -direction * k, SIDE)).start()
                    time = transit((axis, direction), size)
                    left[which] -= 1
            at(time, lambda: arrived(which, direction, k))
            if left[which] == 0:
                active[0] -= 1
                passed()

        def arrived(which, direction, k):
            count = sum(k < hops(direction, d % 2) for d in CLASSES[which])
            bytes_of(several(count), ring_recv.at[number, slot(which, direction, k)])
            if any(k + 1 < hops(direction, d % 2) for d in CLASSES[which]):
                send(which, direction, k + 1)
                inject()
            finished()

        def inject():
            while ready and active[0] < window[0]:
                which = ready.pop(0)
                active[0] += 1
                for direction in (1, -1):
                    send(which, direction, 0)

        def received(which):
            count = len(CLASSES[2]) if which else SIDE - 1 - len(CLASSES[2])
            bytes_of(several(count), deal_recv.at[number, which])
            ready.extend([2] if which else list(range(1, len(CLASSES) - 1)))
            inject()

        def deal():
            for which, members_of in enumerate(((1, 7, 2, 6), CLASSES[-1])):
                time = 0.0
                for d in members_of:
                    dealt(d, lane, beside(across, d)).start()
                    direction, count = (1, d) if d <= SIDE // 2 else (-1, SIDE - d)
                    time = max(time, transit((across, direction), size, count))
                at(time, lambda which=which: received(which))
            ready.insert(0, 0)
            inject()

        def go(amount):
            window[0] = amount
            inject()

        closing.append(lambda: bytes_of(block(pl.ds(0, SIDE - 1), pl.ds(0, SIDE)), ring_send.at[number]))
        closing.append(lambda: bytes_of(several(SIDE - 1), deal_send.at[number]))
        return deal, go

    def mate(axis):
        other_one = here[axis] + 1 - 2 * odd[axis]
        return device(other_one, y, t) if axis == "z" else device(z, other_one, t)

    def hand_over(number, axis, src, dst, landing, size, done):
        start(remote(src, dst, pair_send.at[number], pair_recv.at[number], mate(axis)))
        time = max(transit((axis, 1), size), transit((axis, -1), size))

        def arrived():
            remote(src, landing, pair_send.at[number], pair_recv.at[number], mate(axis)).wait_recv()
            done()
        at(time, arrived)

    other = t + 1 - 2 * core

    def share(number, block, tall, size, done):
        halves = (pl.ds(0, tall // 2), pl.ds(tall // 2, tall // 2))
        whole = pl.ds(0, tall)
        near_sem = tp_recv.at[number, 0]

        def copy(slot, source, part, to):
            return remote(
                block(source).at[part], block(source).at[part], tp_send.at[number],
                tp_recv.at[number, slot], device(z, y, to),
            )

        def from_chip(d, which):
            return step_to(chip, -d, CHIPS) * 2 + which

        def near():
            bytes_of(block(pl.ds(0, CHIPS)), near_sem)
            done()

        latest = [0.0]
        all_near = when_all(5, lambda: at(latest[0], near))

        def to_core(source, part, amount):
            copy(0, source, part, other).start()
            latest[0] = max(latest[0], transit("core", amount, 1, 300e3))
            all_near()

        def far(d):
            copy(d, from_chip(d, core), whole, from_chip(d, core)).wait_recv()
            half, onward, slot, hop = (0, 1, 2, 1) if d == 1 else (1, 3, 4, -1)
            copy(slot, from_chip(d, core), halves[half], from_chip(-onward, core)).start()
            at(transit(("x", hop), size / 2), lambda: farther(slot, half))
            to_core(from_chip(d, core), whole, size)

        def farther(slot, half):
            copy(slot, from_chip(2, core), halves[half], other).wait_recv()
            to_core(from_chip(2, core), halves[half], size / 2)

        for d, hop in ((1, 1), (3, -1)):
            copy(d, t, whole, step_to(chip, d, CHIPS) * 2 + core).start()
            at(transit(("x", hop), size), lambda d=d: far(d))
        to_core(t, whole, size)
        closing.append(lambda: bytes_of(block(pl.ds(0, 2 * CHIPS - 1)), tp_send.at[number]))

    unit1 = ws1.shape[2] * part_width * 2

    def both(fn):
        return when_all(2, fn)

    deal_s1, _ = trains(
        0, "z", "y", stage_s1, lambda r, p: ws1.at[r, p], lambda n: ws1.at[0, pl.ds(0, n)], unit1, [WINDOW[0]],
        lambda: (s1_far(), s1_own()), lambda: go_s2(WINDOW[1]),
    )
    deal_c1, _ = trains(
        1, "y", "z", stage_c1, lambda r, p: wc1.at[p, r], lambda n: wc1.at[pl.ds(0, n), 0], 2 * unit1, [WINDOW[2]],
        lambda: (c1_far(), c1_own()), lambda: go_c2(WINDOW[3]),
    )
    deal_s2, go_s2 = trains(
        2, "z", "y", stage_s2, lambda r, p: ws2.at[r, p], lambda n: ws2.at[0, pl.ds(0, n)], 2 * unit1, [0],
        lambda: (state_own(), state_far()),
    )
    deal_c2, go_c2 = trains(
        3, "y", "z", stage_c2, lambda r, p: wc2.at[p, r], lambda n: wc2.at[pl.ds(0, n), 0], unit1, [0],
        lambda: (conv_own(), conv_far()),
    )

    def begin():
        after("s1", ws1.at[0, pl.ds(0, 3)])
        deal_s1()
        after("c1", wc1.at[0, pl.ds(0, 3)])
        deal_c1()

    at(0.0, begin)
    at(WHEN[0], lambda: (after("s2", ws2.at[0, pl.ds(0, 3)]), deal_s2()))
    at(WHEN[1], lambda: (after("c2", wc2.at[0, pl.ds(0, 3)]), deal_c2()))

    step = normed.shape[3]

    def measure():
        for name in ("raw", *SMALL):
            after(name)
        def body(i, carry):
            part = pl.ds(pl.multiple_of(i * 16, 16), 16)
            value = raw[part, :].astype(F32)
            mean = jnp.mean(value * value, axis=1, keepdims=True)
            scale[part, :] = jnp.broadcast_to(lax.rsqrt(mean + 1e-6), (16, 128))
            return carry
        lax.fori_loop(0, length // 16, body, 0, unroll=2)
        normalise(t)
        swap(1, "y", lambda: s1_far())
        at(WHEN[2], lambda: swap(2, "z", lambda: c1_far()))

    def swap(i, axis, done):
        for half in (0, 1):
            number = 2 * i - 2 + half
            relay(
                number, number, axis, normed.at[0], normed.at[i], half, length * step * 2, done
            )

    def relay(number, pair, axis, mine, theirs, half, size, done):
        part = pl.ds(half * length // 2, length // 2)
        hand_over(
            pair, axis, mine.at[t, part], theirs.at[t, part], theirs.at[t, part], size / 2,
            lambda: share(number, lambda c: theirs.at[c, part], length // 2, size / 2, done),
        )

    def normalise(c):
        lanes = lanes_from(c, step)
        value = raw[:, lanes].astype(F32)
        normed[0, c] = (value * scale[:, 0:1] * norm_gain[:, lanes]).astype(BF)

    def normalise_all():
        def body(c, carry):
            pl.when(c != t)(lambda: normalise(c))
            return carry
        lax.fori_loop(0, 2 * CHIPS, body, 0)

    def spread():
        return ((iota((size, flat), 1) & (size - 1)) == iota((size, flat), 0)).astype(F32)

    def owner():
        return (iota((groups, flat), 1) // size) == iota((groups, flat), 0)

    def as_row(table):
        wide_table = jnp.dot(table, spread(), precision=HIGHEST, preferred_element_type=F32)
        return jnp.sum(jnp.where(owner(), wide_table, 0.0), axis=0, keepdims=True)

    def as_table(row):
        return lax.dot_general(
            jnp.where(owner(), row, 0.0), spread(), NT, precision=HIGHEST, preferred_element_type=F32
        )

    total_tokens = length * SIDE * SIDE

    def tables():
        rate = -as_row(decay_rate[...]) / total_tokens
        turn = as_row(frequency[...])
        rows[0:1, :] = as_row(initial_state[0])
        rows[1:2, :] = as_row(initial_state[1])
        magnitude = jnp.exp(rate)
        step_r = magnitude * jnp.cos(turn)
        step_i = magnitude * jnp.sin(turn)
        modulus = rate * rate + turn * turn
        lift = step_r - 1.0
        factor_r = (lift * rate + step_i * turn) / modulus
        factor_i = (step_i * rate - lift * turn) / modulus
        count = iota((8, flat), 0) + 1
        block_r, block_i = jnp.ones((8, flat), F32), jnp.zeros((8, flat), F32)
        square_r, square_i = step_r, step_i
        for place in range(4):
            chosen = ((count >> place) & 1) == 1
            next_r, next_i = rotate(block_r, block_i, square_r, square_i)
            block_r = jnp.where(chosen, next_r, block_r)
            block_i = jnp.where(chosen, next_i, block_i)
            if place < 3:
                square_r, square_i = rotate(square_r, square_i, square_r, square_i)
        rows[2:3, :], rows[3:4, :] = square_r, square_i
        rows[4:5, :], rows[5:6, :] = factor_r, factor_i

        def body(i, carry):
            now_r, now_i = carry
            part = pl.ds(pl.multiple_of(i * 8, 8), 8)
            power_r[part, :], power_i[part, :] = now_r, now_i
            inverse = 1.0 / (now_r * now_r + now_i * now_i)
            un_r, un_i = rotate(now_r * inverse, -now_i * inverse, rows[4:5, :], rows[5:6, :])
            undo_r[part, :], undo_i[part, :] = un_r, un_i
            return rotate(now_r, now_i, rows[2:3, :], rows[3:4, :])
        lax.fori_loop(0, length // 8, body, (block_r, block_i))

    def matrices():
        stretch = spread().astype(BF)
        def fill(source, sign, dest, lanes):
            for g in range(groups):
                copied = jnp.dot((sign * source[g]).astype(BF), stretch, preferred_element_type=F32)
                kept = iota((wide, flat), 1) // size == g
                dest[g * wide:(g + 1) * wide, lanes] = jnp.where(kept, copied, 0.0).astype(BF)
        fill(input_real, 1.0, drive_r, slice(0, flat))
        fill(input_imag, 1.0, drive_i, slice(0, flat))
        fill(output_real, 1.0, emit, slice(0, flat))
        fill(output_imag, -1.0, emit, slice(flat, 2 * flat))

    at(0.5, measure, 1.0)
    at(6.0, normalise_all, 1.5)
    at(8.0, tables, 1.4)
    at(9.0, matrices, 1.0)

    chunk = 256

    def project_in(i, weights):
        count = weights.shape[3]
        total = None
        for c in range(2 * CHIPS):
            term = jnp.dot(normed[i, c], weights[c].reshape(step, count), preferred_element_type=F32)
            total = term if total is None else total + term
        return total

    def feed_own():
        feed_half[odd["y"]] = project_in(0, ws1).astype(BF)
        recur_ready()

    def feed_far():
        feed_back[...] = project_in(1, ws1).astype(BF)
        hand_over(
            4, "y", feed_back, feed_half.at[odd["y"]], feed_half.at[1 - odd["y"]],
            length * part_width * 2, lambda: recur_ready(),
        )

    s1_own = when_all(1, lambda: at(clock[0], feed_own, 0.6))
    s1_far = when_all(3, lambda: at(clock[0], feed_far, 0.6))
    recur_ready = both(lambda: at(clock[0], recur, 1.4))

    def recur():
        feed[:, 0:part_width] = feed_half[0]
        feed[:, part_width:width] = feed_half[1]
        drive = feed[...]
        for j in range(flat // chunk):
            part = slice(j * chunk, (j + 1) * chunk)
            shift = slice(flat + j * chunk, flat + (j + 1) * chunk)
            push_r = jnp.dot(drive, drive_r[:, part], preferred_element_type=F32)
            push_i = jnp.dot(drive, drive_i[:, part], preferred_element_type=F32)
            back_r, back_i = rotate(undo_r[:, part], undo_i[:, part], push_r, push_i)
            scaled[:, part] = back_r.astype(BF)
            scaled[:, shift] = back_i.astype(BF)
        lower = (iota((length, length), 0) >= iota((length, length), 1)).astype(BF)
        for j in range(2 * flat // chunk):
            part = slice(j * chunk, (j + 1) * chunk)
            summed[:, part] = jnp.dot(lower, scaled[:, part], preferred_element_type=F32)
        end_r, end_i = rotate(
            power_r[length - 1:length, :], power_i[length - 1:length, :],
            summed[length - 1:length, 0:flat], summed[length - 1:length, flat:2 * flat],
        )
        finals[y, :, 0:flat], finals[y, :, flat:2 * flat] = end_r, end_i
        spread_out(0, "y", finals, 8 * flat, lambda: at(clock[0], scan_row, 0.1))

    def scan_row():
        span_r, span_i = power_r[length - 1:length, :], power_i[length - 1:length, :]
        zero = jnp.zeros((1, flat), F32)
        sum_r, sum_i, before_r, before_i = zero, zero, zero, zero
        jump_r, jump_i = zero + 1.0, zero
        mine_r, mine_i = zero, zero
        for yy in range(SIDE):
            before_r, before_i = jnp.where(y == yy, sum_r, before_r), jnp.where(y == yy, sum_i, before_i)
            mine_r, mine_i = jnp.where(y == yy, jump_r, mine_r), jnp.where(y == yy, jump_i, mine_i)
            next_r, next_i = rotate(span_r, span_i, sum_r, sum_i)
            sum_r = next_r + finals[yy, :, 0:flat]
            sum_i = next_i + finals[yy, :, flat:2 * flat]
            jump_r, jump_i = rotate(span_r, span_i, jump_r, jump_i)
        rows[6:7, :], rows[7:8, :] = before_r, before_i
        rows[8:9, :], rows[9:10, :] = mine_r, mine_i
        rows[10:11, :], rows[11:12, :] = jump_r, jump_i
        totals[z, :, 0:flat], totals[z, :, flat:2 * flat] = sum_r, sum_i
        spread_out(1, "z", totals, 8 * flat, lambda: at(clock[0], scan_all, 2.5))

    def scan_all():
        sum_r, sum_i = rows[0:1, :], rows[1:2, :]
        jump_r, jump_i = rows[10:11, :], rows[11:12, :]
        start_r, start_i = sum_r, sum_i
        for zz in range(SIDE):
            start_r, start_i = jnp.where(z == zz, sum_r, start_r), jnp.where(z == zz, sum_i, start_i)
            next_r, next_i = rotate(jump_r, jump_i, sum_r, sum_i)
            sum_r = next_r + totals[zz, :, 0:flat]
            sum_i = next_i + totals[zz, :, flat:2 * flat]
        final_state[0] = as_table(sum_r)
        final_state[1] = as_table(sum_i)
        load("final", final_state, final_out)
        lead_r, lead_i = rotate(rows[8:9, :], rows[9:10, :], start_r, start_i)
        entry_r, entry_i = lead_r + rows[6:7, :], lead_i + rows[7:8, :]
        for j in range(flat // chunk):
            part = slice(j * chunk, (j + 1) * chunk)
            shift = slice(flat + j * chunk, flat + (j + 1) * chunk)
            state_r, state_i = rotate(
                power_r[:, part], power_i[:, part],
                summed[:, part] + entry_r[:, part], summed[:, shift] + entry_i[:, part],
            )
            states[:, part] = state_r.astype(BF)
            states[:, shift] = state_i.astype(BF)
        answer = lax.dot_general(states[...], emit[...], NT, preferred_element_type=F32)
        answer = answer + skip_gain[...] * feed[...].astype(F32)
        act_all[0, t] = jax.nn.gelu(answer).astype(BF)
        exchange(4, 5, "y", act_all, lambda: state_own(), lambda half: state_far())

    def exchange(number, pair, axis, blocks, own, far):
        amount = length * width * 2
        for half in (0, 1):
            relay(
                number + 1 + half, pair + half, axis, blocks.at[0], blocks.at[1], half, amount,
                lambda half=half: far(half),
            )
        share(number, lambda c: blocks.at[0, c], length, amount, own)

    edge = halo.shape[1]
    kernel_size = conv_taps.shape[0]

    def gate(i):
        pair = project_in(i, wc1)
        return (pair[:, 0:part_width] * jax.nn.sigmoid(pair[:, part_width:width])).astype(BF)

    def gate_own():
        gated_half[odd["z"]] = gate(0)
        gate_ready()

    def gate_far():
        gated_back[...] = gate(2)
        hand_over(
            7, "z", gated_back, gated_half.at[odd["z"]], gated_half.at[1 - odd["z"]],
            length * part_width * 2, lambda: gate_ready(),
        )

    c1_own = when_all(1, lambda: at(clock[0], gate_own, 0.7))
    c1_far = when_all(3, lambda: at(clock[0], gate_far, 0.7))
    gate_ready = both(lambda: at(clock[0], pass_edge, 0.1))
    last = pl.ds(length - edge, edge)

    def pass_edge():
        start(
            remote(
                gated_half.at[:, last], halo, halo_sem.at[0], halo_sem.at[1],
                {"sp": following, "tp": t},
            )
        )
        at(transit(("y", 1), edge * width * 2), convolve, 0.7)
        for half in (0, 1):
            lanes = slice(half * part_width, (half + 1) * part_width)
            padded[edge:edge + length, lanes] = gated_half[half].astype(F32)

    def convolve():
        remote(
            gated_half.at[:, last], halo, halo_sem.at[0], halo_sem.at[1],
            {"sp": preceding, "tp": t},
        ).wait_recv()
        for half in (0, 1):
            lanes = slice(half * part_width, (half + 1) * part_width)
            padded[0:edge, lanes] = jnp.where(seq > 0, halo[half].astype(F32), 0.0)
        lag = edge - (kernel_size - 1)
        for lane in range(width // 128):
            lanes = slice(lane * 128, (lane + 1) * 128)
            answer = jnp.zeros((length, 128), F32)
            for b in range(8):
                tall = length + (8 if b else 0)
                part = jnp.zeros((tall, 128), F32)
                for a in range(edge // 8 + 1):
                    k = 8 * a + b - lag
                    if 0 <= k < kernel_size:
                        part = part + conv_taps[k:k + 1, lanes] * padded[8 * a:8 * a + tall, lanes]
                if b:
                    shifted[b, :, :] = part
                    answer = answer + shifted[b, b:b + length, :]
                else:
                    answer = answer + part
            conv_all[0, t, :, lanes] = answer.astype(BF)
        exchange(
            7, 8, "z", conv_all, lambda: at(clock[0], lambda: channel_norm(0, 0, length), 2.4),
            lambda half: at(
                clock[0], lambda: channel_norm(1, half * length // 2, length // 2), 1.2
            ),
        )

    def channel_norm(which, first, tall):
        count = 2 * CHIPS * width
        def body(i, carry):
            part = pl.ds(pl.multiple_of(first + i * 16, 16), 16)
            pieces = [conv_all[which, c, part, :].astype(F32) for c in range(2 * CHIPS)]
            total = pieces[0]
            for piece in pieces[1:]:
                total = total + piece
            mean = jnp.sum(total, axis=1, keepdims=True) / count
            pieces = [piece - mean for piece in pieces]
            total = pieces[0] * pieces[0]
            for piece in pieces[1:]:
                total = total + piece * piece
            scale = lax.rsqrt(jnp.sum(total, axis=1, keepdims=True) / count + 1e-5)
            for c, piece in enumerate(pieces):
                lanes = slice(c * width, (c + 1) * width)
                value = piece * scale * chan_gain[:, lanes] + chan_shift[:, lanes]
                conv_act[which, c, part, :] = jax.nn.silu(value).astype(BF)
            return carry
        lax.fori_loop(0, tall // 16, body, 0, unroll=2)
        (conv_far if which else conv_own)()

    def project(blocks, i, weights):
        count = weights.shape[3]
        total = None
        for c in range(2 * CHIPS):
            term = jnp.dot(
                blocks[i, c], weights[c].reshape(width, count), preferred_element_type=F32
            )
            total = term if total is None else total + term
        return total

    def state_out(i):
        pair = project(act_all, i, ws2)
        return pair[:, 0:part_columns] * jax.nn.sigmoid(pair[:, part_columns:columns])

    def state_out_own():
        state_half[odd["y"]] = state_out(0)
        finish_ready()

    def state_out_far():
        state_back[...] = state_out(1).astype(BF)
        hand_over(
            10, "y", state_back, state_got, state_got, length * part_columns * 2, state_returned
        )

    def state_returned():
        state_half[1 - odd["y"]] = state_got[...].astype(F32)
        finish_ready()

    def conv_out_own():
        conv_half[odd["z"]] = project(conv_act, 0, wc2)
        finish_ready()

    def conv_out_far():
        conv_back[...] = project(conv_act, 1, wc2).astype(BF)
        hand_over(11, "z", conv_back, conv_got, conv_got, length * part_columns * 2, conv_returned)

    def conv_returned():
        conv_half[1 - odd["z"]] = conv_got[...].astype(F32)
        finish_ready()

    state_own = both(lambda: at(clock[0], state_out_own, 0.8))
    state_far = when_all(3, lambda: at(clock[0], state_out_far, 0.8))
    conv_own = both(lambda: at(clock[0], conv_out_own, 0.6))
    conv_far = when_all(3, lambda: at(clock[0], conv_out_far, 0.6))
    finish_ready = when_all(4, lambda: at(clock[0], finish, 0.5))

    def finish():
        for half in (0, 1):
            lanes = slice(half * part_columns, (half + 1) * part_columns)
            result[:, lanes] = (state_half[half] + conv_half[half]).astype(BF)
        load("out", result, out)
        drain(1e9)
        for wait in closing:
            wait()
        after("final")
        after("out")

    run()


def local(
    tokens, norm_gain, conv_value, conv_gate, state_feed, conv_taps, chan_gain, chan_shift,
    conv_project, decay_rate, frequency, input_real, input_imag, output_real, output_imag,
    skip_gain, state_value, state_gate, initial_state,
):
    length, features = tokens.shape
    groups, size, wide = input_real.shape
    flat, width = groups * size, groups * wide
    deep1, columns = conv_value.shape[0], conv_project.shape[1]
    deep2 = conv_project.shape[0]
    edge = 32
    args = (
        tokens, norm_gain.reshape(1, -1), conv_value, conv_gate, state_feed, conv_taps,
        chan_gain.reshape(1, -1), chan_shift.reshape(1, -1), conv_project, decay_rate, frequency,
        jnp.swapaxes(input_real, 1, 2), jnp.swapaxes(input_imag, 1, 2), output_real, output_imag,
        skip_gain.reshape(1, -1), state_value, state_gate, initial_state,
    )
    anywhere = pl.BlockSpec(memory_space=pl.ANY)
    vmem = pltpu.VMEM
    dma = pltpu.SemaphoreType.DMA
    many = 2 * CHIPS
    return pl.pallas_call(
        kernel,
        out_shape=(
            jax.ShapeDtypeStruct((length, columns), BF),
            jax.ShapeDtypeStruct(initial_state.shape, F32),
        ),
        in_specs=[anywhere] * len(args),
        out_specs=(anywhere, anywhere),
        scratch_shapes=[
            *(vmem(args[i].shape, args[i].dtype) for i in SMALL),
            vmem((SIDE, SIDE, deep1, width // 2), BF),
            vmem((SIDE, SIDE, deep1, width), BF),
            vmem((SIDE, SIDE, deep2, columns), BF),
            vmem((SIDE, SIDE, deep2, columns // 2), BF),
            vmem((2, deep1, width // 2), BF),
            vmem((2, deep1, width), BF),
            vmem((2, deep2, columns), BF),
            vmem((2, deep2, columns // 2), BF),
            vmem((length, features), BF),
            vmem((length, 128), F32),
            vmem((3, many, length, features // many), BF),
            vmem((length, columns), BF),
            vmem(initial_state.shape, F32),
            *(vmem((length, flat), F32) for _ in range(4)),
            vmem((width, flat), BF),
            vmem((width, flat), BF),
            vmem((width, 2 * flat), BF),
            vmem((length, width), BF),
            vmem((length, 2 * flat), BF),
            vmem((length, 2 * flat), F32),
            vmem((length, 2 * flat), BF),
            vmem((16, flat), F32),
            vmem((SIDE, 1, 2 * flat), F32),
            vmem((SIDE, 1, 2 * flat), F32),
            vmem((2, length, width // 2), BF),
            vmem((length, width // 2), BF),
            vmem((2, length, width // 2), BF),
            vmem((length, width // 2), BF),
            vmem((2, edge, width // 2), BF),
            vmem((edge + length, width), F32),
            vmem((8, length + 8, 128), F32),
            *(vmem((2, many, length, width), BF) for _ in range(3)),
            *(
                vmem(shape, held)
                for _ in range(2)
                for shape, held in (
                    ((2, length, columns // 2), F32),
                    ((length, columns // 2), BF),
                    ((length, columns // 2), BF),
                )
            ),
            dma((20,)),
            dma((4,)),
            dma((4, 23)),
            dma((2,)),
            dma((2,)),
            dma((2,)),
            dma((10,)),
            dma((10, 5)),
            dma((12,)),
            dma((12,)),
            dma((4,)),
            dma((4, 2)),
        ],
        compiler_params=pltpu.CompilerParams(
            collective_id=0, has_side_effects=True, vmem_limit_bytes=62 * 1024 * 1024
        ),
        name="mixer",
    )(*args)


def solution(mesh):
    in_specs = (
        P("sp", None), P(), P("sp", "tp"), P("sp", "tp"), P("sp", "tp"), P(None, "tp"), P(), P(),
        P("sp", "tp"), P("tp", None), P("tp", None), P("tp", None, None), P("tp", None, None),
        P("tp", None, None), P("tp", None, None), P("tp"), P("sp", "tp"), P("sp", "tp"),
        P(None, "tp", None),
    )
    out_specs = (P("sp", "tp"), P(None, "tp", None))
    return jax.shard_map(local, mesh=mesh, in_specs=in_specs, out_specs=out_specs, check_vma=False)
```

```python
import heapq

import jax
import jax.numpy as jnp
from jax import lax
from jax.experimental import pallas as pl
from jax.experimental.pallas import tpu as pltpu
from jax.sharding import PartitionSpec as P

BF, F32 = jnp.bfloat16, jnp.float32
HIGHEST = lax.Precision.HIGHEST
MESH = pl.DeviceIdType.MESH
SIDE = 8
WINDOW = (3, 2, 3, 2)
WHEN = (16.0, 10.0, 16.0)
CLASSES = ((0,), (1, 7, 2, 6), (3, 5, 4))
CHIPS = 4
NT = (((1,), (1,)), ((), ()))


def hops(direction, half):
    return SIDE // 2 if (direction > 0) == (half == 0) else SIDE // 2 - 1


def slot_of(direction, half, k):
    return k if direction > 0 else hops(1, half) + k


def rotate(first_real, first_imag, second_real, second_imag):
    return (
        first_real * second_real - first_imag * second_imag,
        first_real * second_imag + first_imag * second_real,
    )


def iota(shape, dim):
    return lax.broadcasted_iota(jnp.int32, shape, dim)


SMALL = (1, 5, 6, 7, 9, 10, 11, 12, 13, 14, 15, 18)


def kernel(*refs):
    (
        tokens, norm_gain, conv_value, conv_gate, state_feed, conv_taps, chan_gain, chan_shift,
        conv_project, decay_rate, frequency, input_real, input_imag, output_real, output_imag,
        skip_gain, state_value, state_gate, initial_state, out, final_out,
    ) = refs[:21]
    small = refs[21:21 + len(SMALL)]
    (
        ws1, wc1, ws2, wc2, stage_s1, stage_c1, stage_s2, stage_c2, raw, scale, normed, result,
        final_state, power_r, power_i, undo_r, undo_i, drive_r, drive_i, emit, feed, scaled, summed,
        states, rows, finals, totals, feed_half, feed_back, gated_half, gated_back, halo, padded,
        shifted, conv_all, act_all, conv_act, state_half, state_back, state_got, conv_half, conv_back,
        conv_got,
        load_sem, ring_send, ring_recv, scan_send, scan_recv, halo_sem, tp_send, tp_recv, pair_send,
        pair_recv, deal_send, deal_recv,
    ) = refs[21 + len(SMALL):]
    seq = lax.axis_index("sp")
    t = lax.axis_index("tp")
    z, y = seq // SIDE, seq % SIDE
    chip, core = t // 2, t % 2
    length = tokens.shape[0]
    groups, wide, size = input_real.shape
    flat = groups * size
    width = groups * wide
    part_width = width // 2
    columns = out.shape[1]
    part_columns = columns // 2

    def device(zz, yy, tt):
        return {"sp": zz * SIDE + yy, "tp": tt}

    def step_to(at, by, count):
        return lax.rem(at + by + count, count)

    def remote(src, dst, send, recv, to):
        return pltpu.make_async_remote_copy(
            src_ref=src, dst_ref=dst, send_sem=send, recv_sem=recv, device_id=to, device_id_type=MESH
        )

    queue = []
    sent = []
    free = {}
    clock = [0.0, 0]

    def at(time, fn, cost=0.0):
        heapq.heappush(queue, (time, clock[1], cost, fn))
        clock[1] += 1

    def run():
        while queue:
            time, _, cost, fn = heapq.heappop(queue)
            clock[0] = max(clock[0], time)
            fn()
            clock[0] += cost

    def start(moving):
        moving.start()
        sent.append((clock[0], moving))

    closing = []

    def drain(before):
        kept = []
        for time, moving in sent:
            if time < before:
                moving.wait_send()
            else:
                kept.append((time, moving))
        sent[:] = kept

    def transit(link, size, count=1, rate=50e3):
        begin = max(clock[0], free.get(link, 0.0))
        free[link] = begin + size * count / rate
        return free[link] + (0.8 if link == "core" else 1.9) + 0.6 * (count - (link == "core"))

    def when_all(number, fn):
        left = [number]

        def one():
            left[0] -= 1
            if left[0] == 0:
                fn()
        return one

    loads, counted = {}, []

    def load(name, src, dst):
        if name not in counted:
            counted.append(name)
        moving = pltpu.make_async_copy(src, dst, load_sem.at[counted.index(name)])
        moving.start()
        loads[name] = moving

    def bytes_of(ref, sem):
        pltpu.make_async_copy(ref, ref, sem).wait()

    def after(name, three=None):
        if three is None:
            loads[name].wait()
        else:
            bytes_of(three, load_sem.at[counted.index(name)])

    here = {"z": z, "y": y}
    odd = {"z": z % 2, "y": y % 2}

    def lanes_from(half, count):
        return pl.ds(pl.multiple_of(half * count, count), count)

    def staged(name, axis, pieces, stage, own, count):
        for half in (0, 1):
            for i, source in enumerate(pieces):
                load(
                    name, source.at[:, half * count:(half + 1) * count],
                    stage.at[half, :, i * count:(i + 1) * count],
                )
        for i, source in enumerate(pieces):
            load(
                name, source.at[:, lanes_from(odd[axis], count)], own.at[:, i * count:(i + 1) * count]
            )

    staged("s1", "y", (state_feed,), stage_s1, ws1.at[z, y], part_width)
    staged("c1", "z", (conv_value, conv_gate), stage_c1, wc1.at[z, y], part_width)
    load("raw", tokens, raw)
    for i, place in enumerate(SMALL):
        load(place, refs[place], small[i])
    (
        norm_gain, conv_taps, chan_gain, chan_shift, decay_rate, frequency, input_real, input_imag,
        output_real, output_imag, skip_gain, initial_state,
    ) = small
    staged("s2", "y", (state_value, state_gate), stage_s2, ws2.at[z, y], part_columns)
    staged("c2", "z", (conv_project,), stage_c2, wc2.at[z, y], part_columns)

    barrier = pltpu.get_barrier_semaphore()
    following = lax.rem(seq + 1, SIDE * SIDE)
    preceding = lax.rem(seq + SIDE * SIDE - 1, SIDE * SIDE)
    partners = []
    for d in range(1, SIDE):
        partners.append(device(z, step_to(y, d, SIDE), t))
        partners.append(device(step_to(z, d, SIDE), y, t))
    for d in range(1, 2 * CHIPS):
        partners.append(device(z, y, step_to(t, d, 2 * CHIPS)))
    partners.append({"sp": following, "tp": t})
    partners.append({"sp": preceding, "tp": t})
    for partner in partners:
        pl.semaphore_signal(barrier, inc=1, device_id=partner, device_id_type=MESH)
    pl.semaphore_wait(barrier, len(partners))

    def beside(axis, by):
        moved = step_to(here[axis], by, SIDE)
        return device(moved, y, t) if axis == "z" else device(z, moved, t)

    def spread_out(number, axis, blocks, size, done):
        position = here[axis]
        all_others = blocks.at[pl.ds(0, SIDE - 1)]
        latest = 0.0
        for d in (4, 3, 5, 2, 6, 1, 7):
            remote(
                blocks.at[position], blocks.at[position], scan_send.at[number],
                scan_recv.at[number], beside(axis, d),
            ).start()
            direction, count = (1, d) if d <= SIDE // 2 else (-1, SIDE - d)
            latest = max(latest, transit((axis, direction), size, count))

        def arrived():
            bytes_of(all_others, scan_recv.at[number])
            done()
        at(latest, arrived)
        closing.append(lambda: bytes_of(all_others, scan_send.at[number]))

    def trains(number, axis, across, stage, block, several, size, window, done, nearly=None):
        position, lane = here[axis], here[across]
        members = [
            (which, direction, k)
            for which in range(len(CLASSES)) for direction in (1, -1) for k in range(SIDE // 2)
            if any(k < hops(direction, d % 2) for d in CLASSES[which])
        ]
        finished = when_all(len(members), done)
        passed = when_all(len(CLASSES), nearly or (lambda: None))
        ready, active = [], [0]
        left = [len(c) * (SIDE - 1) for c in CLASSES]

        def dealt(d, source, to):
            half = odd[across] if d % 2 == 0 else 1 - odd[across]
            return remote(
                stage.at[half], block(position, source), deal_send.at[number],
                deal_recv.at[number, int(d in CLASSES[-1])], to,
            )

        def slot(which, direction, k):
            return members.index((which, direction, k))

        def copy(which, d, direction, k, source):
            held = block(source, step_to(lane, -d, SIDE))
            return remote(
                held, held, ring_send.at[number], ring_recv.at[number, slot(which, direction, k)],
                beside(axis, direction),
            )

        def send(which, direction, k):
            time = 0.0
            for d in CLASSES[which]:
                if k < hops(direction, d % 2):
                    copy(which, d, direction, k, step_to(position, -direction * k, SIDE)).start()
                    time = transit((axis, direction), size)
                    left[which] -= 1
            at(time, lambda: arrived(which, direction, k))
            if left[which] == 0:
                active[0] -= 1
                passed()

        def arrived(which, direction, k):
            count = sum(k < hops(direction, d % 2) for d in CLASSES[which])
            bytes_of(several(count), ring_recv.at[number, slot(which, direction, k)])
            if any(k + 1 < hops(direction, d % 2) for d in CLASSES[which]):
                send(which, direction, k + 1)
                inject()
            finished()

        def inject():
            while ready and active[0] < window[0]:
                which = ready.pop(0)
                active[0] += 1
                for direction in (1, -1):
                    send(which, direction, 0)

        def received(which):
            count = len(CLASSES[2]) if which else SIDE - 1 - len(CLASSES[2])
            bytes_of(several(count), deal_recv.at[number, which])
            ready.extend([2] if which else list(range(1, len(CLASSES) - 1)))
            inject()

        def deal():
            for which, members_of in enumerate(((1, 7, 2, 6), CLASSES[-1])):
                time = 0.0
                for d in members_of:
                    dealt(d, lane, beside(across, d)).start()
                    direction, count = (1, d) if d <= SIDE // 2 else (-1, SIDE - d)
                    time = max(time, transit((across, direction), size, count))
                at(time, lambda which=which: received(which))
            ready.insert(0, 0)
            inject()

        def go(amount):
            window[0] = amount
            inject()

        closing.append(lambda: bytes_of(block(pl.ds(0, SIDE - 1), pl.ds(0, SIDE)), ring_send.at[number]))
        closing.append(lambda: bytes_of(several(SIDE - 1), deal_send.at[number]))
        return deal, go

    def mate(axis):
        other_one = here[axis] + 1 - 2 * odd[axis]
        return device(other_one, y, t) if axis == "z" else device(z, other_one, t)

    def hand_over(number, axis, src, dst, landing, size, done):
        start(remote(src, dst, pair_send.at[number], pair_recv.at[number], mate(axis)))
        time = max(transit((axis, 1), size), transit((axis, -1), size))

        def arrived():
            remote(src, landing, pair_send.at[number], pair_recv.at[number], mate(axis)).wait_recv()
            done()
        at(time, arrived)

    other = t + 1 - 2 * core

    def share(number, block, size, done):
        near_sem = tp_recv.at[number, 0]

        def copy(slot, source, to):
            return remote(
                block(source), block(source), tp_send.at[number], tp_recv.at[number, slot],
                device(z, y, to),
            )

        def near():
            bytes_of(block(pl.ds(0, CHIPS)), near_sem)
            done()

        latest = [0.0]
        all_near = when_all(4, lambda: at(latest[0], near))

        def to_core(source):
            copy(0, source, other).start()
            latest[0] = max(latest[0], transit("core", size, 1, 200e3))
            all_near()

        def far(d):
            source = step_to(chip, -d, CHIPS) * 2 + core
            copy(d, source, source).wait_recv()
            to_core(source)

        for d in (2, 1, 3):
            copy(d, t, step_to(chip, d, CHIPS) * 2 + core).start()
            if d == 2:
                time = 0.6 + max(transit(("x", hop), size) for hop in (1, -1))
            else:
                time = transit(("x", 2 - d), size)
            at(time, lambda d=d: far(d))
        to_core(t)
        closing.append(lambda: bytes_of(block(pl.ds(0, 2 * CHIPS - 1)), tp_send.at[number]))

    unit1 = ws1.shape[2] * part_width * 2

    def both(fn):
        return when_all(2, fn)

    deal_s1, _ = trains(
        0, "z", "y", stage_s1, lambda r, p: ws1.at[r, p], lambda n: ws1.at[0, pl.ds(0, n)], unit1, [WINDOW[0]],
        lambda: (s1_far(), s1_own()), lambda: go_s2(WINDOW[1]),
    )
    deal_c1, _ = trains(
        1, "y", "z", stage_c1, lambda r, p: wc1.at[p, r], lambda n: wc1.at[pl.ds(0, n), 0], 2 * unit1, [WINDOW[2]],
        lambda: (c1_far(), c1_own()), lambda: go_c2(WINDOW[3]),
    )
    deal_s2, go_s2 = trains(
        2, "z", "y", stage_s2, lambda r, p: ws2.at[r, p], lambda n: ws2.at[0, pl.ds(0, n)], 2 * unit1, [0],
        lambda: (state_own(), state_far()),
    )
    deal_c2, go_c2 = trains(
        3, "y", "z", stage_c2, lambda r, p: wc2.at[p, r], lambda n: wc2.at[pl.ds(0, n), 0], unit1, [0],
        lambda: (conv_own(), conv_far()),
    )

    def begin():
        after("s1", ws1.at[0, pl.ds(0, 3)])
        deal_s1()
        after("c1", wc1.at[0, pl.ds(0, 3)])
        deal_c1()

    at(0.0, begin)
    at(WHEN[0], lambda: (after("s2", ws2.at[0, pl.ds(0, 3)]), deal_s2()))
    at(WHEN[1], lambda: (after("c2", wc2.at[0, pl.ds(0, 3)]), deal_c2()))

    step = normed.shape[3]

    def measure():
        for name in ("raw", *SMALL):
            after(name)
        def body(i, carry):
            part = pl.ds(pl.multiple_of(i * 16, 16), 16)
            value = raw[part, :].astype(F32)
            mean = jnp.mean(value * value, axis=1, keepdims=True)
            scale[part, :] = jnp.broadcast_to(lax.rsqrt(mean + 1e-6), (16, 128))
            return carry
        lax.fori_loop(0, length // 16, body, 0, unroll=2)
        normalise(t)
        swap(1, "y", lambda: s1_far())
        at(WHEN[2], lambda: swap(2, "z", lambda: c1_far()))

    def swap(i, axis, done):
        for half in (0, 1):
            number = 2 * i - 2 + half
            relay(
                number, number, axis, normed.at[0], normed.at[i], half, length * step * 2, done
            )

    def relay(number, pair, axis, mine, theirs, half, size, done):
        part = pl.ds(half * length // 2, length // 2)
        hand_over(
            pair, axis, mine.at[t, part], theirs.at[t, part], theirs.at[t, part], size / 2,
            lambda: share(number, lambda c: theirs.at[c, part], size / 2, done),
        )

    def normalise(c):
        lanes = lanes_from(c, step)
        value = raw[:, lanes].astype(F32)
        normed[0, c] = (value * scale[:, 0:1] * norm_gain[:, lanes]).astype(BF)

    def normalise_all():
        def body(c, carry):
            pl.when(c != t)(lambda: normalise(c))
            return carry
        lax.fori_loop(0, 2 * CHIPS, body, 0)

    def spread():
        return ((iota((size, flat), 1) & (size - 1)) == iota((size, flat), 0)).astype(F32)

    def owner():
        return (iota((groups, flat), 1) // size) == iota((groups, flat), 0)

    def as_row(table):
        wide_table = jnp.dot(table, spread(), precision=HIGHEST, preferred_element_type=F32)
        return jnp.sum(jnp.where(owner(), wide_table, 0.0), axis=0, keepdims=True)

    def as_table(row):
        return lax.dot_general(
            jnp.where(owner(), row, 0.0), spread(), NT, precision=HIGHEST, preferred_element_type=F32
        )

    total_tokens = length * SIDE * SIDE

    def tables():
        rate = -as_row(decay_rate[...]) / total_tokens
        turn = as_row(frequency[...])
        rows[0:1, :] = as_row(initial_state[0])
        rows[1:2, :] = as_row(initial_state[1])
        magnitude = jnp.exp(rate)
        step_r = magnitude * jnp.cos(turn)
        step_i = magnitude * jnp.sin(turn)
        modulus = rate * rate + turn * turn
        lift = step_r - 1.0
        factor_r = (lift * rate + step_i * turn) / modulus
        factor_i = (step_i * rate - lift * turn) / modulus
        count = iota((8, flat), 0) + 1
        block_r, block_i = jnp.ones((8, flat), F32), jnp.zeros((8, flat), F32)
        square_r, square_i = step_r, step_i
        for place in range(4):
            chosen = ((count >> place) & 1) == 1
            next_r, next_i = rotate(block_r, block_i, square_r, square_i)
            block_r = jnp.where(chosen, next_r, block_r)
            block_i = jnp.where(chosen, next_i, block_i)
            if place < 3:
                square_r, square_i = rotate(square_r, square_i, square_r, square_i)
        rows[2:3, :], rows[3:4, :] = square_r, square_i
        rows[4:5, :], rows[5:6, :] = factor_r, factor_i

        def body(i, carry):
            now_r, now_i = carry
            part = pl.ds(pl.multiple_of(i * 8, 8), 8)
            power_r[part, :], power_i[part, :] = now_r, now_i
            inverse = 1.0 / (now_r * now_r + now_i * now_i)
            un_r, un_i = rotate(now_r * inverse, -now_i * inverse, rows[4:5, :], rows[5:6, :])
            undo_r[part, :], undo_i[part, :] = un_r, un_i
            return rotate(now_r, now_i, rows[2:3, :], rows[3:4, :])
        lax.fori_loop(0, length // 8, body, (block_r, block_i))

    def matrices():
        stretch = spread().astype(BF)
        def fill(source, sign, dest, lanes):
            for g in range(groups):
                copied = jnp.dot((sign * source[g]).astype(BF), stretch, preferred_element_type=F32)
                kept = iota((wide, flat), 1) // size == g
                dest[g * wide:(g + 1) * wide, lanes] = jnp.where(kept, copied, 0.0).astype(BF)
        fill(input_real, 1.0, drive_r, slice(0, flat))
        fill(input_imag, 1.0, drive_i, slice(0, flat))
        fill(output_real, 1.0, emit, slice(0, flat))
        fill(output_imag, -1.0, emit, slice(flat, 2 * flat))

    at(0.5, measure, 1.0)
    at(6.0, normalise_all, 1.5)
    at(8.0, tables, 1.4)
    at(9.0, matrices, 1.0)

    chunk = 256

    def project_in(i, weights):
        count = weights.shape[3]
        total = None
        for c in range(2 * CHIPS):
            term = jnp.dot(normed[i, c], weights[c].reshape(step, count), preferred_element_type=F32)
            total = term if total is None else total + term
        return total

    def feed_own():
        feed_half[odd["y"]] = project_in(0, ws1).astype(BF)
        recur_ready()

    def feed_far():
        feed_back[...] = project_in(1, ws1).astype(BF)
        hand_over(
            4, "y", feed_back, feed_half.at[odd["y"]], feed_half.at[1 - odd["y"]],
            length * part_width * 2, lambda: recur_ready(),
        )

    s1_own = when_all(1, lambda: at(clock[0], feed_own, 0.6))
    s1_far = when_all(3, lambda: at(clock[0], feed_far, 0.6))
    recur_ready = both(lambda: at(clock[0], recur, 1.4))

    def recur():
        feed[:, 0:part_width] = feed_half[0]
        feed[:, part_width:width] = feed_half[1]
        drive = feed[...]
        for j in range(flat // chunk):
            part = slice(j * chunk, (j + 1) * chunk)
            shift = slice(flat + j * chunk, flat + (j + 1) * chunk)
            push_r = jnp.dot(drive, drive_r[:, part], preferred_element_type=F32)
            push_i = jnp.dot(drive, drive_i[:, part], preferred_element_type=F32)
            back_r, back_i = rotate(undo_r[:, part], undo_i[:, part], push_r, push_i)
            scaled[:, part] = back_r.astype(BF)
            scaled[:, shift] = back_i.astype(BF)
        lower = (iota((length, length), 0) >= iota((length, length), 1)).astype(BF)
        for j in range(2 * flat // chunk):
            part = slice(j * chunk, (j + 1) * chunk)
            summed[:, part] = jnp.dot(lower, scaled[:, part], preferred_element_type=F32)
        end_r, end_i = rotate(
            power_r[length - 1:length, :], power_i[length - 1:length, :],
            summed[length - 1:length, 0:flat], summed[length - 1:length, flat:2 * flat],
        )
        finals[y, :, 0:flat], finals[y, :, flat:2 * flat] = end_r, end_i
        spread_out(0, "y", finals, 8 * flat, lambda: at(clock[0], scan_row, 0.1))

    def scan_row():
        span_r, span_i = power_r[length - 1:length, :], power_i[length - 1:length, :]
        zero = jnp.zeros((1, flat), F32)
        sum_r, sum_i, before_r, before_i = zero, zero, zero, zero
        jump_r, jump_i = zero + 1.0, zero
        mine_r, mine_i = zero, zero
        for yy in range(SIDE):
            before_r, before_i = jnp.where(y == yy, sum_r, before_r), jnp.where(y == yy, sum_i, before_i)
            mine_r, mine_i = jnp.where(y == yy, jump_r, mine_r), jnp.where(y == yy, jump_i, mine_i)
            next_r, next_i = rotate(span_r, span_i, sum_r, sum_i)
            sum_r = next_r + finals[yy, :, 0:flat]
            sum_i = next_i + finals[yy, :, flat:2 * flat]
            jump_r, jump_i = rotate(span_r, span_i, jump_r, jump_i)
        rows[6:7, :], rows[7:8, :] = before_r, before_i
        rows[8:9, :], rows[9:10, :] = mine_r, mine_i
        rows[10:11, :], rows[11:12, :] = jump_r, jump_i
        totals[z, :, 0:flat], totals[z, :, flat:2 * flat] = sum_r, sum_i
        spread_out(1, "z", totals, 8 * flat, lambda: at(clock[0], scan_all, 2.5))

    def scan_all():
        sum_r, sum_i = rows[0:1, :], rows[1:2, :]
        jump_r, jump_i = rows[10:11, :], rows[11:12, :]
        start_r, start_i = sum_r, sum_i
        for zz in range(SIDE):
            start_r, start_i = jnp.where(z == zz, sum_r, start_r), jnp.where(z == zz, sum_i, start_i)
            next_r, next_i = rotate(jump_r, jump_i, sum_r, sum_i)
            sum_r = next_r + totals[zz, :, 0:flat]
            sum_i = next_i + totals[zz, :, flat:2 * flat]
        final_state[0] = as_table(sum_r)
        final_state[1] = as_table(sum_i)
        load("final", final_state, final_out)
        lead_r, lead_i = rotate(rows[8:9, :], rows[9:10, :], start_r, start_i)
        entry_r, entry_i = lead_r + rows[6:7, :], lead_i + rows[7:8, :]
        for j in range(flat // chunk):
            part = slice(j * chunk, (j + 1) * chunk)
            shift = slice(flat + j * chunk, flat + (j + 1) * chunk)
            state_r, state_i = rotate(
                power_r[:, part], power_i[:, part],
                summed[:, part] + entry_r[:, part], summed[:, shift] + entry_i[:, part],
            )
            states[:, part] = state_r.astype(BF)
            states[:, shift] = state_i.astype(BF)
        answer = lax.dot_general(states[...], emit[...], NT, preferred_element_type=F32)
        answer = answer + skip_gain[...] * feed[...].astype(F32)
        act_all[0, t] = jax.nn.gelu(answer).astype(BF)
        exchange(4, 5, "y", act_all, lambda: state_own(), lambda half: state_far())

    def exchange(number, pair, axis, blocks, own, far):
        amount = length * width * 2
        for half in (0, 1):
            relay(
                number + 1 + half, pair + half, axis, blocks.at[0], blocks.at[1], half, amount,
                lambda half=half: far(half),
            )
        share(number, lambda c: blocks.at[0, c], amount, own)

    edge = halo.shape[1]
    kernel_size = conv_taps.shape[0]

    def gate(i):
        pair = project_in(i, wc1)
        return (pair[:, 0:part_width] * jax.nn.sigmoid(pair[:, part_width:width])).astype(BF)

    def gate_own():
        gated_half[odd["z"]] = gate(0)
        gate_ready()

    def gate_far():
        gated_back[...] = gate(2)
        hand_over(
            7, "z", gated_back, gated_half.at[odd["z"]], gated_half.at[1 - odd["z"]],
            length * part_width * 2, lambda: gate_ready(),
        )

    c1_own = when_all(1, lambda: at(clock[0], gate_own, 0.7))
    c1_far = when_all(3, lambda: at(clock[0], gate_far, 0.7))
    gate_ready = both(lambda: at(clock[0], pass_edge, 0.1))
    last = pl.ds(length - edge, edge)

    def pass_edge():
        start(
            remote(
                gated_half.at[:, last], halo, halo_sem.at[0], halo_sem.at[1],
                {"sp": following, "tp": t},
            )
        )
        at(transit(("y", 1), edge * width * 2), convolve, 0.7)
        for half in (0, 1):
            lanes = slice(half * part_width, (half + 1) * part_width)
            padded[edge:edge + length, lanes] = gated_half[half].astype(F32)

    def convolve():
        remote(
            gated_half.at[:, last], halo, halo_sem.at[0], halo_sem.at[1],
            {"sp": preceding, "tp": t},
        ).wait_recv()
        for half in (0, 1):
            lanes = slice(half * part_width, (half + 1) * part_width)
            padded[0:edge, lanes] = jnp.where(seq > 0, halo[half].astype(F32), 0.0)
        lag = edge - (kernel_size - 1)
        for lane in range(width // 128):
            lanes = slice(lane * 128, (lane + 1) * 128)
            answer = jnp.zeros((length, 128), F32)
            for b in range(8):
                tall = length + (8 if b else 0)
                part = jnp.zeros((tall, 128), F32)
                for a in range(edge // 8 + 1):
                    k = 8 * a + b - lag
                    if 0 <= k < kernel_size:
                        part = part + conv_taps[k:k + 1, lanes] * padded[8 * a:8 * a + tall, lanes]
                if b:
                    shifted[b, :, :] = part
                    answer = answer + shifted[b, b:b + length, :]
                else:
                    answer = answer + part
            conv_all[0, t, :, lanes] = answer.astype(BF)
        exchange(
            7, 8, "z", conv_all, lambda: at(clock[0], lambda: channel_norm(0, 0, length), 2.4),
            lambda half: at(
                clock[0], lambda: channel_norm(1, half * length // 2, length // 2), 1.2
            ),
        )

    def channel_norm(which, first, tall):
        count = 2 * CHIPS * width
        def body(i, carry):
            part = pl.ds(pl.multiple_of(first + i * 16, 16), 16)
            pieces = [conv_all[which, c, part, :].astype(F32) for c in range(2 * CHIPS)]
            total = pieces[0]
            for piece in pieces[1:]:
                total = total + piece
            mean = jnp.sum(total, axis=1, keepdims=True) / count
            pieces = [piece - mean for piece in pieces]
            total = pieces[0] * pieces[0]
            for piece in pieces[1:]:
                total = total + piece * piece
            scale = lax.rsqrt(jnp.sum(total, axis=1, keepdims=True) / count + 1e-5)
            for c, piece in enumerate(pieces):
                lanes = slice(c * width, (c + 1) * width)
                value = piece * scale * chan_gain[:, lanes] + chan_shift[:, lanes]
                conv_act[which, c, part, :] = jax.nn.silu(value).astype(BF)
            return carry
        lax.fori_loop(0, tall // 16, body, 0, unroll=2)
        (conv_far if which else conv_own)()

    def project(blocks, i, weights):
        count = weights.shape[3]
        total = None
        for c in range(2 * CHIPS):
            term = jnp.dot(
                blocks[i, c], weights[c].reshape(width, count), preferred_element_type=F32
            )
            total = term if total is None else total + term
        return total

    def state_out(i):
        pair = project(act_all, i, ws2)
        return pair[:, 0:part_columns] * jax.nn.sigmoid(pair[:, part_columns:columns])

    def state_out_own():
        state_half[odd["y"]] = state_out(0)
        finish_ready()

    def state_out_far():
        state_back[...] = state_out(1).astype(BF)
        hand_over(
            10, "y", state_back, state_got, state_got, length * part_columns * 2, state_returned
        )

    def state_returned():
        state_half[1 - odd["y"]] = state_got[...].astype(F32)
        finish_ready()

    def conv_out_own():
        conv_half[odd["z"]] = project(conv_act, 0, wc2)
        finish_ready()

    def conv_out_far():
        conv_back[...] = project(conv_act, 1, wc2).astype(BF)
        hand_over(11, "z", conv_back, conv_got, conv_got, length * part_columns * 2, conv_returned)

    def conv_returned():
        conv_half[1 - odd["z"]] = conv_got[...].astype(F32)
        finish_ready()

    state_own = both(lambda: at(clock[0], state_out_own, 0.8))
    state_far = when_all(3, lambda: at(clock[0], state_out_far, 0.8))
    conv_own = both(lambda: at(clock[0], conv_out_own, 0.6))
    conv_far = when_all(3, lambda: at(clock[0], conv_out_far, 0.6))
    finish_ready = when_all(4, lambda: at(clock[0], finish, 0.5))

    def finish():
        for half in (0, 1):
            lanes = slice(half * part_columns, (half + 1) * part_columns)
            result[:, lanes] = (state_half[half] + conv_half[half]).astype(BF)
        load("out", result, out)
        drain(1e9)
        for wait in closing:
            wait()
        after("final")
        after("out")

    run()


def local(
    tokens, norm_gain, conv_value, conv_gate, state_feed, conv_taps, chan_gain, chan_shift,
    conv_project, decay_rate, frequency, input_real, input_imag, output_real, output_imag,
    skip_gain, state_value, state_gate, initial_state,
):
    length, features = tokens.shape
    groups, size, wide = input_real.shape
    flat, width = groups * size, groups * wide
    deep1, columns = conv_value.shape[0], conv_project.shape[1]
    deep2 = conv_project.shape[0]
    edge = 32
    args = (
        tokens, norm_gain.reshape(1, -1), conv_value, conv_gate, state_feed, conv_taps,
        chan_gain.reshape(1, -1), chan_shift.reshape(1, -1), conv_project, decay_rate, frequency,
        jnp.swapaxes(input_real, 1, 2), jnp.swapaxes(input_imag, 1, 2), output_real, output_imag,
        skip_gain.reshape(1, -1), state_value, state_gate, initial_state,
    )
    anywhere = pl.BlockSpec(memory_space=pl.ANY)
    vmem = pltpu.VMEM
    dma = pltpu.SemaphoreType.DMA
    many = 2 * CHIPS
    return pl.pallas_call(
        kernel,
        out_shape=(
            jax.ShapeDtypeStruct((length, columns), BF),
            jax.ShapeDtypeStruct(initial_state.shape, F32),
        ),
        in_specs=[anywhere] * len(args),
        out_specs=(anywhere, anywhere),
        scratch_shapes=[
            *(vmem(args[i].shape, args[i].dtype) for i in SMALL),
            vmem((SIDE, SIDE, deep1, width // 2), BF),
            vmem((SIDE, SIDE, deep1, width), BF),
            vmem((SIDE, SIDE, deep2, columns), BF),
            vmem((SIDE, SIDE, deep2, columns // 2), BF),
            vmem((2, deep1, width // 2), BF),
            vmem((2, deep1, width), BF),
            vmem((2, deep2, columns), BF),
            vmem((2, deep2, columns // 2), BF),
            vmem((length, features), BF),
            vmem((length, 128), F32),
            vmem((3, many, length, features // many), BF),
            vmem((length, columns), BF),
            vmem(initial_state.shape, F32),
            *(vmem((length, flat), F32) for _ in range(4)),
            vmem((width, flat), BF),
            vmem((width, flat), BF),
            vmem((width, 2 * flat), BF),
            vmem((length, width), BF),
            vmem((length, 2 * flat), BF),
            vmem((length, 2 * flat), F32),
            vmem((length, 2 * flat), BF),
            vmem((16, flat), F32),
            vmem((SIDE, 1, 2 * flat), F32),
            vmem((SIDE, 1, 2 * flat), F32),
            vmem((2, length, width // 2), BF),
            vmem((length, width // 2), BF),
            vmem((2, length, width // 2), BF),
            vmem((length, width // 2), BF),
            vmem((2, edge, width // 2), BF),
            vmem((edge + length, width), F32),
            vmem((8, length + 8, 128), F32),
            *(vmem((2, many, length, width), BF) for _ in range(3)),
            *(
                vmem(shape, held)
                for _ in range(2)
                for shape, held in (
                    ((2, length, columns // 2), F32),
                    ((length, columns // 2), BF),
                    ((length, columns // 2), BF),
                )
            ),
            dma((20,)),
            dma((4,)),
            dma((4, 23)),
            dma((2,)),
            dma((2,)),
            dma((2,)),
            dma((10,)),
            dma((10, 4)),
            dma((12,)),
            dma((12,)),
            dma((4,)),
            dma((4, 2)),
        ],
        compiler_params=pltpu.CompilerParams(
            collective_id=0, has_side_effects=True, vmem_limit_bytes=62 * 1024 * 1024
        ),
        name="mixer",
    )(*args)


def solution(mesh):
    in_specs = (
        P("sp", None), P(), P("sp", "tp"), P("sp", "tp"), P("sp", "tp"), P(None, "tp"), P(), P(),
        P("sp", "tp"), P("tp", None), P("tp", None), P("tp", None, None), P("tp", None, None),
        P("tp", None, None), P("tp", None, None), P("tp"), P("sp", "tp"), P("sp", "tp"),
        P(None, "tp", None),
    )
    out_specs = (P("sp", "tp"), P(None, "tp", None))
    return jax.shard_map(local, mesh=mesh, in_specs=in_specs, out_specs=out_specs, check_vma=False)
```

```python
import heapq

import jax
import jax.numpy as jnp
from jax import lax
from jax.experimental import pallas as pl
from jax.experimental.pallas import tpu as pltpu
from jax.sharding import PartitionSpec as P

BF, F32 = jnp.bfloat16, jnp.float32
HIGHEST = lax.Precision.HIGHEST
MESH = pl.DeviceIdType.MESH
SIDE = 8
WINDOW = (3, 3, 3, 2)
WHEN = (16.0, 14.0, 16.0)
CLASSES = ((0,), (1, 7, 2, 6), (3, 5, 4))
CHIPS = 4
NT = (((1,), (1,)), ((), ()))


def hops(direction, half):
    return SIDE // 2 if (direction > 0) == (half == 0) else SIDE // 2 - 1


def slot_of(direction, half, k):
    return k if direction > 0 else hops(1, half) + k


def rotate(first_real, first_imag, second_real, second_imag):
    return (
        first_real * second_real - first_imag * second_imag,
        first_real * second_imag + first_imag * second_real,
    )


def iota(shape, dim):
    return lax.broadcasted_iota(jnp.int32, shape, dim)


SMALL = (1, 5, 6, 7, 9, 10, 11, 12, 13, 14, 15, 18)


def kernel(*refs):
    (
        tokens, norm_gain, conv_value, conv_gate, state_feed, conv_taps, chan_gain, chan_shift,
        conv_project, decay_rate, frequency, input_real, input_imag, output_real, output_imag,
        skip_gain, state_value, state_gate, initial_state, out, final_out,
    ) = refs[:21]
    small = refs[21:21 + len(SMALL)]
    (
        ws1, wc1, ws2, wc2, stage_s1, stage_c1, stage_s2, stage_c2, raw, scale, normed, result,
        final_state, power_r, power_i, undo_r, undo_i, drive_r, drive_i, emit, feed, scaled, summed,
        states, rows, finals, totals, feed_half, feed_back, gated_half, gated_back, halo, padded,
        shifted, conv_all, act_all, conv_act, state_half, state_back, state_got, conv_half, conv_back,
        conv_got,
        load_sem, ring_send, ring_recv, scan_send, scan_recv, halo_sem, tp_send, tp_recv, pair_send,
        pair_recv, deal_send, deal_recv,
    ) = refs[21 + len(SMALL):]
    seq = lax.axis_index("sp")
    t = lax.axis_index("tp")
    z, y = seq // SIDE, seq % SIDE
    chip, core = t // 2, t % 2
    length = tokens.shape[0]
    groups, wide, size = input_real.shape
    flat = groups * size
    width = groups * wide
    part_width = width // 2
    columns = out.shape[1]
    part_columns = columns // 2

    def device(zz, yy, tt):
        return {"sp": zz * SIDE + yy, "tp": tt}

    def step_to(at, by, count):
        return lax.rem(at + by + count, count)

    def remote(src, dst, send, recv, to):
        return pltpu.make_async_remote_copy(
            src_ref=src, dst_ref=dst, send_sem=send, recv_sem=recv, device_id=to, device_id_type=MESH
        )

    queue = []
    sent = []
    free = {}
    clock = [0.0, 0]

    def at(time, fn, cost=0.0):
        heapq.heappush(queue, (time, clock[1], cost, fn))
        clock[1] += 1

    def run():
        while queue:
            time, _, cost, fn = heapq.heappop(queue)
            clock[0] = max(clock[0], time)
            fn()
            clock[0] += cost

    def start(moving):
        moving.start()
        sent.append((clock[0], moving))

    closing = []

    def drain(before):
        kept = []
        for time, moving in sent:
            if time < before:
                moving.wait_send()
            else:
                kept.append((time, moving))
        sent[:] = kept

    def transit(link, size, count=1, rate=50e3):
        begin = max(clock[0], free.get(link, 0.0))
        free[link] = begin + size * count / rate
        return free[link] + (0.8 if link == "core" else 2.3) + 0.6 * (count - (link == "core"))

    def when_all(number, fn):
        left = [number]

        def one():
            left[0] -= 1
            if left[0] == 0:
                fn()
        return one

    loads, counted = {}, []

    def load(name, src, dst):
        if name not in counted:
            counted.append(name)
        moving = pltpu.make_async_copy(src, dst, load_sem.at[counted.index(name)])
        moving.start()
        loads[name] = moving

    def bytes_of(ref, sem):
        pltpu.make_async_copy(ref, ref, sem).wait()

    def after(name, three=None):
        if three is None:
            loads[name].wait()
        else:
            bytes_of(three, load_sem.at[counted.index(name)])

    here = {"z": z, "y": y}
    odd = {"z": z % 2, "y": y % 2}

    def lanes_from(half, count):
        return pl.ds(pl.multiple_of(half * count, count), count)

    def staged(name, axis, pieces, stage, own, count):
        for half in (0, 1):
            for i, source in enumerate(pieces):
                load(
                    name, source.at[:, half * count:(half + 1) * count],
                    stage.at[half, :, i * count:(i + 1) * count],
                )
        for i, source in enumerate(pieces):
            load(
                name, source.at[:, lanes_from(odd[axis], count)], own.at[:, i * count:(i + 1) * count]
            )

    staged("s1", "y", (state_feed,), stage_s1, ws1.at[z, y], part_width)
    staged("c1", "z", (conv_value, conv_gate), stage_c1, wc1.at[z, y], part_width)
    load("raw", tokens, raw)
    for i, place in enumerate(SMALL):
        load(place, refs[place], small[i])
    (
        norm_gain, conv_taps, chan_gain, chan_shift, decay_rate, frequency, input_real, input_imag,
        output_real, output_imag, skip_gain, initial_state,
    ) = small
    staged("s2", "y", (state_value, state_gate), stage_s2, ws2.at[z, y], part_columns)
    staged("c2", "z", (conv_project,), stage_c2, wc2.at[z, y], part_columns)

    barrier = pltpu.get_barrier_semaphore()
    following = lax.rem(seq + 1, SIDE * SIDE)
    preceding = lax.rem(seq + SIDE * SIDE - 1, SIDE * SIDE)
    partners = []
    for d in range(1, SIDE):
        partners.append(device(z, step_to(y, d, SIDE), t))
        partners.append(device(step_to(z, d, SIDE), y, t))
    for d in range(1, 2 * CHIPS):
        partners.append(device(z, y, step_to(t, d, 2 * CHIPS)))
    partners.append({"sp": following, "tp": t})
    partners.append({"sp": preceding, "tp": t})
    for partner in partners:
        pl.semaphore_signal(barrier, inc=1, device_id=partner, device_id_type=MESH)
    pl.semaphore_wait(barrier, len(partners))

    def beside(axis, by):
        moved = step_to(here[axis], by, SIDE)
        return device(moved, y, t) if axis == "z" else device(z, moved, t)

    def spread_out(number, axis, blocks, size, done):
        position = here[axis]
        all_others = blocks.at[pl.ds(0, SIDE - 1)]
        latest = 0.0
        for d in (4, 3, 5, 2, 6, 1, 7):
            remote(
                blocks.at[position], blocks.at[position], scan_send.at[number],
                scan_recv.at[number], beside(axis, d),
            ).start()
            direction, count = (1, d) if d <= SIDE // 2 else (-1, SIDE - d)
            latest = max(latest, transit((axis, direction), size, count))

        def arrived():
            bytes_of(all_others, scan_recv.at[number])
            done()
        at(latest, arrived)
        closing.append(lambda: bytes_of(all_others, scan_send.at[number]))

    def trains(number, axis, across, stage, block, several, size, window, done, nearly=None):
        position, lane = here[axis], here[across]
        members = [
            (which, direction, k)
            for which in range(len(CLASSES)) for direction in (1, -1) for k in range(SIDE // 2)
            if any(k < hops(direction, d % 2) for d in CLASSES[which])
        ]
        finished = when_all(len(members), done)
        passed = when_all(len(CLASSES), nearly or (lambda: None))
        ready, active = [], [0]
        left = [len(c) * (SIDE - 1) for c in CLASSES]

        def dealt(d, source, to):
            half = odd[across] if d % 2 == 0 else 1 - odd[across]
            return remote(
                stage.at[half], block(position, source), deal_send.at[number],
                deal_recv.at[number, int(d in CLASSES[-1])], to,
            )

        def slot(which, direction, k):
            return members.index((which, direction, k))

        def copy(which, d, direction, k, source):
            held = block(source, step_to(lane, -d, SIDE))
            return remote(
                held, held, ring_send.at[number], ring_recv.at[number, slot(which, direction, k)],
                beside(axis, direction),
            )

        def send(which, direction, k):
            time = 0.0
            for d in CLASSES[which]:
                if k < hops(direction, d % 2):
                    copy(which, d, direction, k, step_to(position, -direction * k, SIDE)).start()
                    time = transit((axis, direction), size)
                    left[which] -= 1
            at(time, lambda: arrived(which, direction, k))
            if left[which] == 0:
                active[0] -= 1
                passed()

        def arrived(which, direction, k):
            count = sum(k < hops(direction, d % 2) for d in CLASSES[which])
            bytes_of(several(count), ring_recv.at[number, slot(which, direction, k)])
            if any(k + 1 < hops(direction, d % 2) for d in CLASSES[which]):
                send(which, direction, k + 1)
                inject()
            finished()

        def inject():
            while ready and active[0] < window[0]:
                which = ready.pop(0)
                active[0] += 1
                for direction in (1, -1):
                    send(which, direction, 0)

        def received(which):
            count = len(CLASSES[2]) if which else SIDE - 1 - len(CLASSES[2])
            bytes_of(several(count), deal_recv.at[number, which])
            ready.extend([2] if which else list(range(1, len(CLASSES) - 1)))
            inject()

        def deal():
            for which, members_of in enumerate(((1, 7, 2, 6), CLASSES[-1])):
                time = 0.0
                for d in members_of:
                    dealt(d, lane, beside(across, d)).start()
                    direction, count = (1, d) if d <= SIDE // 2 else (-1, SIDE - d)
                    time = max(time, transit((across, direction), size, count))
                at(time, lambda which=which: received(which))
            ready.insert(0, 0)
            inject()

        def go(amount):
            window[0] = amount
            inject()

        closing.append(lambda: bytes_of(block(pl.ds(0, SIDE - 1), pl.ds(0, SIDE)), ring_send.at[number]))
        closing.append(lambda: bytes_of(several(SIDE - 1), deal_send.at[number]))
        return deal, go

    def mate(axis):
        other_one = here[axis] + 1 - 2 * odd[axis]
        return device(other_one, y, t) if axis == "z" else device(z, other_one, t)

    def hand_over(number, axis, src, dst, landing, size, done):
        start(remote(src, dst, pair_send.at[number], pair_recv.at[number], mate(axis)))
        time = max(transit((axis, 1), size), transit((axis, -1), size))

        def arrived():
            remote(src, landing, pair_send.at[number], pair_recv.at[number], mate(axis)).wait_recv()
            done()
        at(time, arrived)

    other = t + 1 - 2 * core

    def share(number, block, size, done):
        near_sem = tp_recv.at[number, 0]

        def copy(slot, source, to):
            return remote(
                block(source), block(source), tp_send.at[number], tp_recv.at[number, slot],
                device(z, y, to),
            )

        def near():
            bytes_of(block(pl.ds(0, CHIPS)), near_sem)
            done()

        latest = [0.0]
        all_near = when_all(4, lambda: at(latest[0], near))

        def to_core(source):
            copy(0, source, other).start()
            latest[0] = max(latest[0], transit("core", size, 1, 200e3))
            all_near()

        def far(d):
            source = step_to(chip, -d, CHIPS) * 2 + core
            copy(d, source, source).wait_recv()
            to_core(source)

        for d in (1, 3, 2):
            copy(d, t, step_to(chip, d, CHIPS) * 2 + core).start()
            if d == 2:
                time = 0.6 + max(transit(("x", hop), size) for hop in (1, -1))
            else:
                time = transit(("x", 2 - d), size)
            at(time, lambda d=d: far(d))
        to_core(t)
        closing.append(lambda: bytes_of(block(pl.ds(0, 2 * CHIPS - 1)), tp_send.at[number]))

    unit1 = ws1.shape[2] * part_width * 2

    def both(fn):
        return when_all(2, fn)

    deal_s1, _ = trains(
        0, "z", "y", stage_s1, lambda r, p: ws1.at[r, p], lambda n: ws1.at[0, pl.ds(0, n)], unit1, [WINDOW[0]],
        lambda: (s1_far(), s1_own()), lambda: go_s2(WINDOW[1]),
    )
    deal_c1, _ = trains(
        1, "y", "z", stage_c1, lambda r, p: wc1.at[p, r], lambda n: wc1.at[pl.ds(0, n), 0], 2 * unit1, [WINDOW[2]],
        lambda: (c1_far(), c1_own()), lambda: go_c2(WINDOW[3]),
    )
    deal_s2, go_s2 = trains(
        2, "z", "y", stage_s2, lambda r, p: ws2.at[r, p], lambda n: ws2.at[0, pl.ds(0, n)], 2 * unit1, [0],
        lambda: (state_own(), state_far()),
    )
    deal_c2, go_c2 = trains(
        3, "y", "z", stage_c2, lambda r, p: wc2.at[p, r], lambda n: wc2.at[pl.ds(0, n), 0], unit1, [0],
        lambda: (conv_own(), conv_far()),
    )

    def begin():
        after("s1", ws1.at[0, pl.ds(0, 3)])
        deal_s1()
        after("c1", wc1.at[0, pl.ds(0, 3)])
        deal_c1()

    at(0.0, begin)
    at(WHEN[0], lambda: (after("s2", ws2.at[0, pl.ds(0, 3)]), deal_s2()))
    at(WHEN[1], lambda: (after("c2", wc2.at[0, pl.ds(0, 3)]), deal_c2()))

    step = normed.shape[3]

    def measure():
        for name in ("raw", *SMALL):
            after(name)
        def body(i, carry):
            part = pl.ds(pl.multiple_of(i * 16, 16), 16)
            value = raw[part, :].astype(F32)
            mean = jnp.mean(value * value, axis=1, keepdims=True)
            scale[part, :] = jnp.broadcast_to(lax.rsqrt(mean + 1e-6), (16, 128))
            return carry
        lax.fori_loop(0, length // 16, body, 0, unroll=2)
        normalise(t)
        swap(1, "y", lambda: s1_far())
        at(WHEN[2], lambda: swap(2, "z", lambda: c1_far()))

    def swap(i, axis, done):
        for half in (0, 1):
            number = 2 * i - 2 + half
            relay(
                number, number, axis, normed.at[0], normed.at[i], half, length * step * 2, done
            )

    def relay(number, pair, axis, mine, theirs, half, size, done):
        part = pl.ds(half * length // 2, length // 2)
        hand_over(
            pair, axis, mine.at[t, part], theirs.at[t, part], theirs.at[t, part], size / 2,
            lambda: share(number, lambda c: theirs.at[c, part], size / 2, done),
        )

    def normalise(c):
        lanes = lanes_from(c, step)
        value = raw[:, lanes].astype(F32)
        normed[0, c] = (value * scale[:, 0:1] * norm_gain[:, lanes]).astype(BF)

    def normalise_all():
        def body(c, carry):
            pl.when(c != t)(lambda: normalise(c))
            return carry
        lax.fori_loop(0, 2 * CHIPS, body, 0)

    def spread():
        return ((iota((size, flat), 1) & (size - 1)) == iota((size, flat), 0)).astype(F32)

    def owner():
        return (iota((groups, flat), 1) // size) == iota((groups, flat), 0)

    def as_row(table):
        wide_table = jnp.dot(table, spread(), precision=HIGHEST, preferred_element_type=F32)
        return jnp.sum(jnp.where(owner(), wide_table, 0.0), axis=0, keepdims=True)

    def as_table(row):
        return lax.dot_general(
            jnp.where(owner(), row, 0.0), spread(), NT, precision=HIGHEST, preferred_element_type=F32
        )

    total_tokens = length * SIDE * SIDE

    def tables():
        rate = -as_row(decay_rate[...]) / total_tokens
        turn = as_row(frequency[...])
        rows[0:1, :] = as_row(initial_state[0])
        rows[1:2, :] = as_row(initial_state[1])
        magnitude = jnp.exp(rate)
        step_r = magnitude * jnp.cos(turn)
        step_i = magnitude * jnp.sin(turn)
        modulus = rate * rate + turn * turn
        lift = step_r - 1.0
        factor_r = (lift * rate + step_i * turn) / modulus
        factor_i = (step_i * rate - lift * turn) / modulus
        count = iota((8, flat), 0) + 1
        block_r, block_i = jnp.ones((8, flat), F32), jnp.zeros((8, flat), F32)
        square_r, square_i = step_r, step_i
        for place in range(4):
            chosen = ((count >> place) & 1) == 1
            next_r, next_i = rotate(block_r, block_i, square_r, square_i)
            block_r = jnp.where(chosen, next_r, block_r)
            block_i = jnp.where(chosen, next_i, block_i)
            if place < 3:
                square_r, square_i = rotate(square_r, square_i, square_r, square_i)
        rows[2:3, :], rows[3:4, :] = square_r, square_i
        rows[4:5, :], rows[5:6, :] = factor_r, factor_i

        def body(i, carry):
            now_r, now_i = carry
            part = pl.ds(pl.multiple_of(i * 8, 8), 8)
            power_r[part, :], power_i[part, :] = now_r, now_i
            inverse = 1.0 / (now_r * now_r + now_i * now_i)
            un_r, un_i = rotate(now_r * inverse, -now_i * inverse, rows[4:5, :], rows[5:6, :])
            undo_r[part, :], undo_i[part, :] = un_r, un_i
            return rotate(now_r, now_i, rows[2:3, :], rows[3:4, :])
        lax.fori_loop(0, length // 8, body, (block_r, block_i))

    def matrices():
        stretch = spread().astype(BF)
        def fill(source, sign, dest, lanes):
            for g in range(groups):
                copied = jnp.dot((sign * source[g]).astype(BF), stretch, preferred_element_type=F32)
                kept = iota((wide, flat), 1) // size == g
                dest[g * wide:(g + 1) * wide, lanes] = jnp.where(kept, copied, 0.0).astype(BF)
        fill(input_real, 1.0, drive_r, slice(0, flat))
        fill(input_imag, 1.0, drive_i, slice(0, flat))
        fill(output_real, 1.0, emit, slice(0, flat))
        fill(output_imag, -1.0, emit, slice(flat, 2 * flat))

    at(0.5, measure, 1.0)
    at(6.0, normalise_all, 1.5)
    at(8.0, tables, 1.4)
    at(9.0, matrices, 1.2)

    chunk = 256

    def project_in(i, weights):
        count = weights.shape[3]
        total = None
        for c in range(2 * CHIPS):
            term = jnp.dot(normed[i, c], weights[c].reshape(step, count), preferred_element_type=F32)
            total = term if total is None else total + term
        return total

    def feed_own():
        feed_half[odd["y"]] = project_in(0, ws1).astype(BF)
        recur_ready()

    def feed_far():
        feed_back[...] = project_in(1, ws1).astype(BF)
        hand_over(
            4, "y", feed_back, feed_half.at[odd["y"]], feed_half.at[1 - odd["y"]],
            length * part_width * 2, lambda: recur_ready(),
        )

    s1_own = when_all(1, lambda: at(clock[0], feed_own, 0.6))
    s1_far = when_all(3, lambda: at(clock[0], feed_far, 0.7))
    recur_ready = both(lambda: at(clock[0], recur, 0.8))

    def recur():
        feed[:, 0:part_width] = feed_half[0]
        feed[:, part_width:width] = feed_half[1]
        drive = feed[...]
        for j in range(flat // chunk):
            part = slice(j * chunk, (j + 1) * chunk)
            shift = slice(flat + j * chunk, flat + (j + 1) * chunk)
            push_r = jnp.dot(drive, drive_r[:, part], preferred_element_type=F32)
            push_i = jnp.dot(drive, drive_i[:, part], preferred_element_type=F32)
            back_r, back_i = rotate(undo_r[:, part], undo_i[:, part], push_r, push_i)
            scaled[:, part] = back_r.astype(BF)
            scaled[:, shift] = back_i.astype(BF)
        lower = (iota((length, length), 0) >= iota((length, length), 1)).astype(BF)
        for j in range(2 * flat // chunk):
            part = slice(j * chunk, (j + 1) * chunk)
            summed[:, part] = jnp.dot(lower, scaled[:, part], preferred_element_type=F32)
        end_r, end_i = rotate(
            power_r[length - 1:length, :], power_i[length - 1:length, :],
            summed[length - 1:length, 0:flat], summed[length - 1:length, flat:2 * flat],
        )
        finals[y, :, 0:flat], finals[y, :, flat:2 * flat] = end_r, end_i
        spread_out(0, "y", finals, 8 * flat, lambda: at(clock[0], scan_row, 0.1))

    def scan_row():
        span_r, span_i = power_r[length - 1:length, :], power_i[length - 1:length, :]
        zero = jnp.zeros((1, flat), F32)
        sum_r, sum_i, before_r, before_i = zero, zero, zero, zero
        jump_r, jump_i = zero + 1.0, zero
        mine_r, mine_i = zero, zero
        for yy in range(SIDE):
            before_r, before_i = jnp.where(y == yy, sum_r, before_r), jnp.where(y == yy, sum_i, before_i)
            mine_r, mine_i = jnp.where(y == yy, jump_r, mine_r), jnp.where(y == yy, jump_i, mine_i)
            next_r, next_i = rotate(span_r, span_i, sum_r, sum_i)
            sum_r = next_r + finals[yy, :, 0:flat]
            sum_i = next_i + finals[yy, :, flat:2 * flat]
            jump_r, jump_i = rotate(span_r, span_i, jump_r, jump_i)
        rows[6:7, :], rows[7:8, :] = before_r, before_i
        rows[8:9, :], rows[9:10, :] = mine_r, mine_i
        rows[10:11, :], rows[11:12, :] = jump_r, jump_i
        totals[z, :, 0:flat], totals[z, :, flat:2 * flat] = sum_r, sum_i
        spread_out(1, "z", totals, 8 * flat, lambda: at(clock[0], scan_all, 1.2))

    def scan_all():
        sum_r, sum_i = rows[0:1, :], rows[1:2, :]
        jump_r, jump_i = rows[10:11, :], rows[11:12, :]
        start_r, start_i = sum_r, sum_i
        for zz in range(SIDE):
            start_r, start_i = jnp.where(z == zz, sum_r, start_r), jnp.where(z == zz, sum_i, start_i)
            next_r, next_i = rotate(jump_r, jump_i, sum_r, sum_i)
            sum_r = next_r + totals[zz, :, 0:flat]
            sum_i = next_i + totals[zz, :, flat:2 * flat]
        final_state[0] = as_table(sum_r)
        final_state[1] = as_table(sum_i)
        load("final", final_state, final_out)
        lead_r, lead_i = rotate(rows[8:9, :], rows[9:10, :], start_r, start_i)
        entry_r, entry_i = lead_r + rows[6:7, :], lead_i + rows[7:8, :]
        for j in range(flat // chunk):
            part = slice(j * chunk, (j + 1) * chunk)
            shift = slice(flat + j * chunk, flat + (j + 1) * chunk)
            state_r, state_i = rotate(
                power_r[:, part], power_i[:, part],
                summed[:, part] + entry_r[:, part], summed[:, shift] + entry_i[:, part],
            )
            states[:, part] = state_r.astype(BF)
            states[:, shift] = state_i.astype(BF)
        answer = lax.dot_general(states[...], emit[...], NT, preferred_element_type=F32)
        answer = answer + skip_gain[...] * feed[...].astype(F32)
        act_all[0, t] = jax.nn.gelu(answer).astype(BF)
        exchange(4, 5, "y", act_all, lambda: state_own(), lambda half: state_far())

    def exchange(number, pair, axis, blocks, own, far):
        amount = length * width * 2
        for half in (0, 1):
            relay(
                number + 1 + half, pair + half, axis, blocks.at[0], blocks.at[1], half, amount,
                lambda half=half: far(half),
            )
        share(number, lambda c: blocks.at[0, c], amount, own)

    edge = halo.shape[1]
    kernel_size = conv_taps.shape[0]

    def gate(i):
        pair = project_in(i, wc1)
        return (pair[:, 0:part_width] * jax.nn.sigmoid(pair[:, part_width:width])).astype(BF)

    def gate_own():
        gated_half[odd["z"]] = gate(0)
        gate_ready()

    def gate_far():
        gated_back[...] = gate(2)
        hand_over(
            7, "z", gated_back, gated_half.at[odd["z"]], gated_half.at[1 - odd["z"]],
            length * part_width * 2, lambda: gate_ready(),
        )

    c1_own = when_all(1, lambda: at(clock[0], gate_own, 1.0))
    c1_far = when_all(3, lambda: at(clock[0], gate_far, 1.0))
    gate_ready = both(lambda: at(clock[0], pass_edge, 0.1))
    last = pl.ds(length - edge, edge)

    def pass_edge():
        start(
            remote(
                gated_half.at[:, last], halo, halo_sem.at[0], halo_sem.at[1],
                {"sp": following, "tp": t},
            )
        )
        at(transit(("y", 1), edge * width * 2), convolve, 1.0)
        for half in (0, 1):
            lanes = slice(half * part_width, (half + 1) * part_width)
            padded[edge:edge + length, lanes] = gated_half[half].astype(F32)

    def convolve():
        remote(
            gated_half.at[:, last], halo, halo_sem.at[0], halo_sem.at[1],
            {"sp": preceding, "tp": t},
        ).wait_recv()
        for half in (0, 1):
            lanes = slice(half * part_width, (half + 1) * part_width)
            padded[0:edge, lanes] = jnp.where(seq > 0, halo[half].astype(F32), 0.0)
        lag = edge - (kernel_size - 1)
        for lane in range(width // 128):
            lanes = slice(lane * 128, (lane + 1) * 128)
            answer = jnp.zeros((length, 128), F32)
            for b in range(8):
                tall = length + (8 if b else 0)
                part = jnp.zeros((tall, 128), F32)
                for a in range(edge // 8 + 1):
                    k = 8 * a + b - lag
                    if 0 <= k < kernel_size:
                        part = part + conv_taps[k:k + 1, lanes] * padded[8 * a:8 * a + tall, lanes]
                if b:
                    shifted[b, :, :] = part
                    answer = answer + shifted[b, b:b + length, :]
                else:
                    answer = answer + part
            conv_all[0, t, :, lanes] = answer.astype(BF)
        exchange(
            7, 8, "z", conv_all, lambda: at(clock[0], lambda: channel_norm(0, 0, length), 1.5),
            lambda half: at(
                clock[0], lambda: channel_norm(1, half * length // 2, length // 2), 0.8
            ),
        )

    def channel_norm(which, first, tall):
        count = 2 * CHIPS * width
        def body(i, carry):
            part = pl.ds(pl.multiple_of(first + i * 16, 16), 16)
            pieces = [conv_all[which, c, part, :].astype(F32) for c in range(2 * CHIPS)]
            total = pieces[0]
            for piece in pieces[1:]:
                total = total + piece
            mean = jnp.sum(total, axis=1, keepdims=True) / count
            pieces = [piece - mean for piece in pieces]
            total = pieces[0] * pieces[0]
            for piece in pieces[1:]:
                total = total + piece * piece
            scale = lax.rsqrt(jnp.sum(total, axis=1, keepdims=True) / count + 1e-5)
            for c, piece in enumerate(pieces):
                lanes = slice(c * width, (c + 1) * width)
                value = piece * scale * chan_gain[:, lanes] + chan_shift[:, lanes]
                conv_act[which, c, part, :] = jax.nn.silu(value).astype(BF)
            return carry
        lax.fori_loop(0, tall // 16, body, 0, unroll=2)
        (conv_far if which else conv_own)()

    def project(blocks, i, weights):
        count = weights.shape[3]
        total = None
        for c in range(2 * CHIPS):
            term = jnp.dot(
                blocks[i, c], weights[c].reshape(width, count), preferred_element_type=F32
            )
            total = term if total is None else total + term
        return total

    def state_out(i):
        pair = project(act_all, i, ws2)
        return pair[:, 0:part_columns] * jax.nn.sigmoid(pair[:, part_columns:columns])

    def state_out_own():
        state_half[odd["y"]] = state_out(0)
        finish_ready()

    def state_out_far():
        state_back[...] = state_out(1).astype(BF)
        hand_over(
            10, "y", state_back, state_got, state_got, length * part_columns * 2, state_returned
        )

    def state_returned():
        state_half[1 - odd["y"]] = state_got[...].astype(F32)
        finish_ready()

    def conv_out_own():
        conv_half[odd["z"]] = project(conv_act, 0, wc2)
        finish_ready()

    def conv_out_far():
        conv_back[...] = project(conv_act, 1, wc2).astype(BF)
        hand_over(11, "z", conv_back, conv_got, conv_got, length * part_columns * 2, conv_returned)

    def conv_returned():
        conv_half[1 - odd["z"]] = conv_got[...].astype(F32)
        finish_ready()

    state_own = both(lambda: at(clock[0], state_out_own, 1.0))
    state_far = when_all(3, lambda: at(clock[0], state_out_far, 1.0))
    conv_own = both(lambda: at(clock[0], conv_out_own, 0.6))
    conv_far = when_all(3, lambda: at(clock[0], conv_out_far, 0.6))
    finish_ready = when_all(4, lambda: at(clock[0], finish, 0.5))

    def finish():
        for half in (0, 1):
            lanes = slice(half * part_columns, (half + 1) * part_columns)
            result[:, lanes] = (state_half[half] + conv_half[half]).astype(BF)
        load("out", result, out)
        drain(1e9)
        for wait in closing:
            wait()
        after("final")
        after("out")

    run()


def local(
    tokens, norm_gain, conv_value, conv_gate, state_feed, conv_taps, chan_gain, chan_shift,
    conv_project, decay_rate, frequency, input_real, input_imag, output_real, output_imag,
    skip_gain, state_value, state_gate, initial_state,
):
    length, features = tokens.shape
    groups, size, wide = input_real.shape
    flat, width = groups * size, groups * wide
    deep1, columns = conv_value.shape[0], conv_project.shape[1]
    deep2 = conv_project.shape[0]
    edge = 32
    args = (
        tokens, norm_gain.reshape(1, -1), conv_value, conv_gate, state_feed, conv_taps,
        chan_gain.reshape(1, -1), chan_shift.reshape(1, -1), conv_project, decay_rate, frequency,
        jnp.swapaxes(input_real, 1, 2), jnp.swapaxes(input_imag, 1, 2), output_real, output_imag,
        skip_gain.reshape(1, -1), state_value, state_gate, initial_state,
    )
    anywhere = pl.BlockSpec(memory_space=pl.ANY)
    vmem = pltpu.VMEM
    dma = pltpu.SemaphoreType.DMA
    many = 2 * CHIPS
    return pl.pallas_call(
        kernel,
        out_shape=(
            jax.ShapeDtypeStruct((length, columns), BF),
            jax.ShapeDtypeStruct(initial_state.shape, F32),
        ),
        in_specs=[anywhere] * len(args),
        out_specs=(anywhere, anywhere),
        scratch_shapes=[
            *(vmem(args[i].shape, args[i].dtype) for i in SMALL),
            vmem((SIDE, SIDE, deep1, width // 2), BF),
            vmem((SIDE, SIDE, deep1, width), BF),
            vmem((SIDE, SIDE, deep2, columns), BF),
            vmem((SIDE, SIDE, deep2, columns // 2), BF),
            vmem((2, deep1, width // 2), BF),
            vmem((2, deep1, width), BF),
            vmem((2, deep2, columns), BF),
            vmem((2, deep2, columns // 2), BF),
            vmem((length, features), BF),
            vmem((length, 128), F32),
            vmem((3, many, length, features // many), BF),
            vmem((length, columns), BF),
            vmem(initial_state.shape, F32),
            *(vmem((length, flat), F32) for _ in range(4)),
            vmem((width, flat), BF),
            vmem((width, flat), BF),
            vmem((width, 2 * flat), BF),
            vmem((length, width), BF),
            vmem((length, 2 * flat), BF),
            vmem((length, 2 * flat), F32),
            vmem((length, 2 * flat), BF),
            vmem((16, flat), F32),
            vmem((SIDE, 1, 2 * flat), F32),
            vmem((SIDE, 1, 2 * flat), F32),
            vmem((2, length, width // 2), BF),
            vmem((length, width // 2), BF),
            vmem((2, length, width // 2), BF),
            vmem((length, width // 2), BF),
            vmem((2, edge, width // 2), BF),
            vmem((edge + length, width), F32),
            vmem((8, length + 8, 128), F32),
            *(vmem((2, many, length, width), BF) for _ in range(3)),
            *(
                vmem(shape, held)
                for _ in range(2)
                for shape, held in (
                    ((2, length, columns // 2), F32),
                    ((length, columns // 2), BF),
                    ((length, columns // 2), BF),
                )
            ),
            dma((20,)),
            dma((4,)),
            dma((4, 23)),
            dma((2,)),
            dma((2,)),
            dma((2,)),
            dma((10,)),
            dma((10, 4)),
            dma((12,)),
            dma((12,)),
            dma((4,)),
            dma((4, 2)),
        ],
        compiler_params=pltpu.CompilerParams(
            collective_id=0, has_side_effects=True, vmem_limit_bytes=62 * 1024 * 1024
        ),
        name="mixer",
    )(*args)


def solution(mesh):
    in_specs = (
        P("sp", None), P(), P("sp", "tp"), P("sp", "tp"), P("sp", "tp"), P(None, "tp"), P(), P(),
        P("sp", "tp"), P("tp", None), P("tp", None), P("tp", None, None), P("tp", None, None),
        P("tp", None, None), P("tp", None, None), P("tp"), P("sp", "tp"), P("sp", "tp"),
        P(None, "tp", None),
    )
    out_specs = (P("sp", "tp"), P(None, "tp", None))
    return jax.shard_map(local, mesh=mesh, in_specs=in_specs, out_specs=out_specs, check_vma=False)
```

```python
import heapq

import jax
import jax.numpy as jnp
from jax import lax
from jax.experimental import pallas as pl
from jax.experimental.pallas import tpu as pltpu
from jax.sharding import PartitionSpec as P

BF, F32 = jnp.bfloat16, jnp.float32
HIGHEST = lax.Precision.HIGHEST
MESH = pl.DeviceIdType.MESH
SIDE = 8
WINDOW = (3, 3, 3, 3)
WHEN = (10.0, 18.0, 12.0)
CLASSES = ((0,), (1, 7, 2, 6), (3, 5, 4))
CHIPS = 4
NT = (((1,), (1,)), ((), ()))


def hops(direction, half):
    return SIDE // 2 if (direction > 0) == (half == 0) else SIDE // 2 - 1


def slot_of(direction, half, k):
    return k if direction > 0 else hops(1, half) + k


def rotate(first_real, first_imag, second_real, second_imag):
    return (
        first_real * second_real - first_imag * second_imag,
        first_real * second_imag + first_imag * second_real,
    )


def iota(shape, dim):
    return lax.broadcasted_iota(jnp.int32, shape, dim)


SMALL = (1, 5, 6, 7, 9, 10, 11, 12, 13, 14, 15, 18)


def kernel(*refs):
    (
        tokens, norm_gain, conv_value, conv_gate, state_feed, conv_taps, chan_gain, chan_shift,
        conv_project, decay_rate, frequency, input_real, input_imag, output_real, output_imag,
        skip_gain, state_value, state_gate, initial_state, out, final_out,
    ) = refs[:21]
    small = refs[21:21 + len(SMALL)]
    (
        ws1, wc1, ws2, wc2, stage_s1, stage_c1, stage_s2, stage_c2, raw, scale, normed, result,
        final_half, power_r, power_i, undo_r, undo_i, drive_r, drive_i, emit, scaled, summed,
        states, rows, finals, totals, feed_block, gated_block, halo, padded,
        shifted, conv_all, act_all, conv_act, state_half, state_back, state_got, conv_half, conv_back,
        conv_got,
        load_sem, ring_send, ring_recv, scan_send, scan_recv, halo_sem, tp_send, tp_recv, pair_send,
        pair_recv, deal_send, deal_recv,
    ) = refs[21 + len(SMALL):]
    seq = lax.axis_index("sp")
    t = lax.axis_index("tp")
    z, y = seq // SIDE, seq % SIDE
    chip, core = t // 2, t % 2
    length = tokens.shape[0]
    groups, wide, size = input_real.shape
    width = groups * wide
    part_width = width // 2
    groups = groups // 2
    flat = groups * size
    columns = out.shape[1]
    part_columns = columns // 2

    def device(zz, yy, tt):
        return {"sp": zz * SIDE + yy, "tp": tt}

    def step_to(at, by, count):
        return lax.rem(at + by + count, count)

    def remote(src, dst, send, recv, to):
        return pltpu.make_async_remote_copy(
            src_ref=src, dst_ref=dst, send_sem=send, recv_sem=recv, device_id=to, device_id_type=MESH
        )

    queue = []
    sent = []
    free = {}
    clock = [0.0, 0]

    def at(time, fn, cost=0.0):
        heapq.heappush(queue, (time, clock[1], cost, fn))
        clock[1] += 1

    def run():
        while queue:
            time, _, cost, fn = heapq.heappop(queue)
            clock[0] = max(clock[0], time)
            fn()
            clock[0] += cost

    def start(moving):
        moving.start()
        sent.append((clock[0], moving))

    closing = []

    def drain(before):
        kept = []
        for time, moving in sent:
            if time < before:
                moving.wait_send()
            else:
                kept.append((time, moving))
        sent[:] = kept

    def transit(link, size, count=1, rate=50e3):
        begin = max(clock[0], free.get(link, 0.0))
        free[link] = begin + size * count / rate
        return free[link] + (0.8 if link == "core" else 2.3) + 0.6 * (count - (link == "core"))

    def when_all(number, fn):
        left = [number]

        def one():
            left[0] -= 1
            if left[0] == 0:
                fn()
        return one

    loads, counted = {}, []

    def load(name, src, dst):
        if name not in counted:
            counted.append(name)
        moving = pltpu.make_async_copy(src, dst, load_sem.at[counted.index(name)])
        moving.start()
        loads[name] = moving

    def bytes_of(ref, sem):
        pltpu.make_async_copy(ref, ref, sem).wait()

    def after(name, three=None):
        if three is None:
            loads[name].wait()
        else:
            bytes_of(three, load_sem.at[counted.index(name)])

    here = {"z": z, "y": y}
    odd = {"z": z % 2, "y": y % 2}

    def lanes_from(half, count):
        return pl.ds(pl.multiple_of(half * count, count), count)

    def staged(name, axis, pieces, stage, own, count):
        for half in (0, 1):
            for i, source in enumerate(pieces):
                load(
                    name, source.at[:, half * count:(half + 1) * count],
                    stage.at[half, :, i * count:(i + 1) * count],
                )
        for i, source in enumerate(pieces):
            load(
                name, source.at[:, lanes_from(odd[axis], count)], own.at[:, i * count:(i + 1) * count]
            )

    staged("s1", "y", (state_feed,), stage_s1, ws1.at[z, y], part_width)
    staged("c1", "z", (conv_value, conv_gate), stage_c1, wc1.at[z, y], part_width)
    load("raw", tokens, raw)
    for i, place in enumerate(SMALL):
        load(place, refs[place], small[i])
    (
        norm_gain, conv_taps, chan_gain, chan_shift, decay_rate, frequency, input_real, input_imag,
        output_real, output_imag, skip_gain, initial_state,
    ) = small
    staged("s2", "y", (state_value, state_gate), stage_s2, ws2.at[z, y], part_columns)
    staged("c2", "z", (conv_project,), stage_c2, wc2.at[z, y], part_columns)

    barrier = pltpu.get_barrier_semaphore()
    at_end, at_start = y // (SIDE - 1), (SIDE - 1 - y) // (SIDE - 1)
    following = device(step_to(z, 2 * at_end, SIDE), step_to(y, 1, SIDE), t)
    preceding = device(step_to(z, -2 * at_start, SIDE), step_to(y, -1, SIDE), t)
    partners = []
    for d in range(1, SIDE):
        partners.append(device(z, step_to(y, d, SIDE), t))
        partners.append(device(step_to(z, d, SIDE), y, t))
    for d in range(1, 2 * CHIPS):
        partners.append(device(z, y, step_to(t, d, 2 * CHIPS)))
    partners.append(following)
    partners.append(preceding)
    for partner in partners:
        pl.semaphore_signal(barrier, inc=1, device_id=partner, device_id_type=MESH)
    pl.semaphore_wait(barrier, len(partners))

    def beside(axis, by):
        moved = step_to(here[axis], by, SIDE)
        return device(moved, y, t) if axis == "z" else device(z, moved, t)

    def spread_out(number, axis, blocks, size, stride, done):
        position = here[axis] // stride
        all_others = blocks.at[pl.ds(0, SIDE // stride - 1)]
        latest = 0.0
        for d in (4, 3, 5, 2, 6, 1, 7):
            if d % stride == 0:
                remote(
                    blocks.at[position], blocks.at[position], scan_send.at[number],
                    scan_recv.at[number], beside(axis, d),
                ).start()
                direction, count = (1, d) if d <= SIDE // 2 else (-1, SIDE - d)
                latest = max(latest, transit((axis, direction), size, count))

        def arrived():
            bytes_of(all_others, scan_recv.at[number])
            done()
        at(latest, arrived)
        closing.append(lambda: bytes_of(all_others, scan_send.at[number]))

    def trains(number, axis, across, stage, block, several, size, window, done, nearly=None):
        position, lane = here[axis], here[across]
        members = [
            (which, direction, k)
            for which in range(len(CLASSES)) for direction in (1, -1) for k in range(SIDE // 2)
            if any(k < hops(direction, d % 2) for d in CLASSES[which])
        ]
        finished = when_all(len(members), done)
        passed = when_all(len(CLASSES), nearly or (lambda: None))
        ready, active = [], [0]
        left = [len(c) * (SIDE - 1) for c in CLASSES]

        def dealt(d, source, to):
            half = odd[across] if d % 2 == 0 else 1 - odd[across]
            return remote(
                stage.at[half], block(position, source), deal_send.at[number],
                deal_recv.at[number, int(d in CLASSES[-1])], to,
            )

        def slot(which, direction, k):
            return members.index((which, direction, k))

        def copy(which, d, direction, k, source):
            held = block(source, step_to(lane, -d, SIDE))
            return remote(
                held, held, ring_send.at[number], ring_recv.at[number, slot(which, direction, k)],
                beside(axis, direction),
            )

        def send(which, direction, k):
            time = 0.0
            for d in CLASSES[which]:
                if k < hops(direction, d % 2):
                    copy(which, d, direction, k, step_to(position, -direction * k, SIDE)).start()
                    time = transit((axis, direction), size)
                    left[which] -= 1
            at(time, lambda: arrived(which, direction, k))
            if left[which] == 0:
                active[0] -= 1
                passed()

        def arrived(which, direction, k):
            count = sum(k < hops(direction, d % 2) for d in CLASSES[which])
            bytes_of(several(count), ring_recv.at[number, slot(which, direction, k)])
            if any(k + 1 < hops(direction, d % 2) for d in CLASSES[which]):
                send(which, direction, k + 1)
                inject()
            finished()

        def inject():
            while ready and active[0] < window[0]:
                which = ready.pop(0)
                active[0] += 1
                for direction in (1, -1):
                    send(which, direction, 0)

        def received(which):
            count = len(CLASSES[2]) if which else SIDE - 1 - len(CLASSES[2])
            bytes_of(several(count), deal_recv.at[number, which])
            ready.extend([2] if which else list(range(1, len(CLASSES) - 1)))
            inject()

        def deal():
            for which, members_of in enumerate(((1, 7, 2, 6), CLASSES[-1])):
                time = 0.0
                for d in members_of:
                    dealt(d, lane, beside(across, d)).start()
                    direction, count = (1, d) if d <= SIDE // 2 else (-1, SIDE - d)
                    time = max(time, transit((across, direction), size, count))
                at(time, lambda which=which: received(which))
            ready.insert(0, 0)
            inject()

        def go(amount):
            window[0] = amount
            inject()

        closing.append(lambda: bytes_of(block(pl.ds(0, SIDE - 1), pl.ds(0, SIDE)), ring_send.at[number]))
        closing.append(lambda: bytes_of(several(SIDE - 1), deal_send.at[number]))
        return deal, go

    def mate(axis):
        other_one = here[axis] + 1 - 2 * odd[axis]
        return device(other_one, y, t) if axis == "z" else device(z, other_one, t)

    def hand_over(number, axis, src, dst, landing, size, done):
        start(remote(src, dst, pair_send.at[number], pair_recv.at[number], mate(axis)))
        time = max(transit((axis, 1), size), transit((axis, -1), size))

        def arrived():
            remote(src, landing, pair_send.at[number], pair_recv.at[number], mate(axis)).wait_recv()
            done()
        at(time, arrived)

    other = t + 1 - 2 * core

    def share(number, block, size, done):
        near_sem = tp_recv.at[number, 0]

        def copy(slot, source, to):
            return remote(
                block(source), block(source), tp_send.at[number], tp_recv.at[number, slot],
                device(z, y, to),
            )

        def near():
            bytes_of(block(pl.ds(0, CHIPS)), near_sem)
            done()

        latest = [0.0]
        all_near = when_all(4, lambda: at(latest[0], near))

        def to_core(source):
            copy(0, source, other).start()
            latest[0] = max(latest[0], transit("core", size, 1, 200e3))
            all_near()

        def far(d):
            source = step_to(chip, -d, CHIPS) * 2 + core
            copy(d, source, source).wait_recv()
            to_core(source)

        for d in (1, 3, 2):
            copy(d, t, step_to(chip, d, CHIPS) * 2 + core).start()
            if d == 2:
                time = 0.6 + max(transit(("x", hop), size) for hop in (1, -1))
            else:
                time = transit(("x", 2 - d), size)
            at(time, lambda d=d: far(d))
        to_core(t)
        closing.append(lambda: bytes_of(block(pl.ds(0, 2 * CHIPS - 1)), tp_send.at[number]))

    unit1 = ws1.shape[2] * part_width * 2

    def both(fn):
        return when_all(2, fn)

    deal_s1, _ = trains(
        0, "z", "y", stage_s1, lambda r, p: ws1.at[r, p], lambda n: ws1.at[0, pl.ds(0, n)], unit1, [WINDOW[0]],
        lambda: (s1_far(), s1_own()), lambda: go_s2(WINDOW[1]),
    )
    deal_c1, _ = trains(
        1, "y", "z", stage_c1, lambda r, p: wc1.at[p, r], lambda n: wc1.at[pl.ds(0, n), 0], 2 * unit1, [WINDOW[2]],
        lambda: (c1_far(), c1_own()), lambda: go_c2(WINDOW[3]),
    )
    deal_s2, go_s2 = trains(
        2, "z", "y", stage_s2, lambda r, p: ws2.at[r, p], lambda n: ws2.at[0, pl.ds(0, n)], 2 * unit1, [0],
        lambda: (state_own(), state_far()),
    )
    deal_c2, go_c2 = trains(
        3, "y", "z", stage_c2, lambda r, p: wc2.at[p, r], lambda n: wc2.at[pl.ds(0, n), 0], unit1, [0],
        lambda: (conv_own(), conv_far()),
    )

    def begin():
        after("s1", ws1.at[0, pl.ds(0, 3)])
        deal_s1()
        after("c1", wc1.at[0, pl.ds(0, 3)])
        deal_c1()

    at(0.0, begin)
    at(WHEN[0], lambda: (after("s2", ws2.at[0, pl.ds(0, 3)]), deal_s2()))
    at(WHEN[1], lambda: (after("c2", wc2.at[0, pl.ds(0, 3)]), deal_c2()))

    step = normed.shape[3]

    def measure():
        for name in ("raw", *SMALL):
            after(name)
        def body(i, carry):
            part = pl.ds(pl.multiple_of(i * 16, 16), 16)
            value = raw[part, :].astype(F32)
            mean = jnp.mean(value * value, axis=1, keepdims=True)
            scale[part, :] = jnp.broadcast_to(lax.rsqrt(mean + 1e-6), (16, 128))
            return carry
        lax.fori_loop(0, length // 16, body, 0, unroll=2)
        normalise(t)
        swap(1, "y", lambda: s1_far())
        at(WHEN[2], lambda: swap(2, "z", lambda: c1_far()))

    def swap(i, axis, done):
        for half in (0, 1):
            number = 2 * i - 2 + half
            relay(
                number, number, axis, normed.at[0], normed.at[i], half, length * step * 2, done
            )

    def relay(number, pair, axis, mine, theirs, half, size, done):
        part = pl.ds(half * length // 2, length // 2)
        hand_over(
            pair, axis, mine.at[t, part], theirs.at[t, part], theirs.at[t, part], size / 2,
            lambda: share(number, lambda c: theirs.at[c, part], size / 2, done),
        )

    def normalise(c):
        lanes = lanes_from(c, step)
        value = raw[:, lanes].astype(F32)
        normed[0, c] = (value * scale[:, 0:1] * norm_gain[:, lanes]).astype(BF)

    def normalise_all():
        def body(c, carry):
            pl.when(c != t)(lambda: normalise(c))
            return carry
        lax.fori_loop(0, 2 * CHIPS, body, 0)

    def spread():
        return ((iota((size, flat), 1) & (size - 1)) == iota((size, flat), 0)).astype(F32)

    def owner():
        return (iota((groups, flat), 1) // size) == iota((groups, flat), 0)

    def as_row(table):
        wide_table = jnp.dot(table, spread(), precision=HIGHEST, preferred_element_type=F32)
        return jnp.sum(jnp.where(owner(), wide_table, 0.0), axis=0, keepdims=True)

    def as_table(row):
        return lax.dot_general(
            jnp.where(owner(), row, 0.0), spread(), NT, precision=HIGHEST, preferred_element_type=F32
        )

    total_tokens = length * SIDE * SIDE

    own_groups = lanes_from(odd["y"], groups)

    def tables():
        rate = -as_row(decay_rate[own_groups, :]) / total_tokens
        turn = as_row(frequency[own_groups, :])
        rows[0:1, :] = as_row(initial_state[0, own_groups, :])
        rows[1:2, :] = as_row(initial_state[1, own_groups, :])
        magnitude = jnp.exp(rate)
        step_r = magnitude * jnp.cos(turn)
        step_i = magnitude * jnp.sin(turn)
        modulus = rate * rate + turn * turn
        lift = step_r - 1.0
        factor_r = (lift * rate + step_i * turn) / modulus
        factor_i = (step_i * rate - lift * turn) / modulus
        count = iota((8, flat), 0) + 1
        block_r, block_i = jnp.ones((8, flat), F32), jnp.zeros((8, flat), F32)
        square_r, square_i = step_r, step_i
        for place in range(4):
            chosen = ((count >> place) & 1) == 1
            next_r, next_i = rotate(block_r, block_i, square_r, square_i)
            block_r = jnp.where(chosen, next_r, block_r)
            block_i = jnp.where(chosen, next_i, block_i)
            if place < 3:
                square_r, square_i = rotate(square_r, square_i, square_r, square_i)
        rows[2:3, :], rows[3:4, :] = square_r, square_i
        rows[4:5, :], rows[5:6, :] = factor_r, factor_i

        def body(i, carry):
            now_r, now_i = carry
            part = pl.ds(pl.multiple_of(i * 8, 8), 8)
            power_r[part, :], power_i[part, :] = now_r, now_i
            inverse = 1.0 / (now_r * now_r + now_i * now_i)
            un_r, un_i = rotate(now_r * inverse, -now_i * inverse, rows[4:5, :], rows[5:6, :])
            undo_r[part, :], undo_i[part, :] = un_r, un_i
            return rotate(now_r, now_i, rows[2:3, :], rows[3:4, :])
        lax.fori_loop(0, length // 8, body, (block_r, block_i))

    def matrices():
        stretch = spread().astype(BF)
        def fill(source, sign, dest, lanes):
            for g in range(groups):
                copied = jnp.dot((sign * source[odd["y"] * groups + g]).astype(BF), stretch, preferred_element_type=F32)
                kept = iota((wide, flat), 1) // size == g
                dest[g * wide:(g + 1) * wide, lanes] = jnp.where(kept, copied, 0.0).astype(BF)
        fill(input_real, 1.0, drive_r, slice(0, flat))
        fill(input_imag, 1.0, drive_i, slice(0, flat))
        fill(output_real, 1.0, emit, slice(0, flat))
        fill(output_imag, -1.0, emit, slice(flat, 2 * flat))

    at(0.5, measure, 1.0)
    at(6.0, normalise_all, 1.5)
    at(8.0, tables, 1.4)
    at(9.0, matrices, 1.2)

    chunk = 256

    def project_in(i, weights):
        count = weights.shape[3]
        total = None
        for c in range(2 * CHIPS):
            term = jnp.dot(normed[i, c], weights[c].reshape(step, count), preferred_element_type=F32)
            total = term if total is None else total + term
        return total

    def feed_own():
        feed_block[odd["y"]] = project_in(0, ws1).astype(BF)
        recur_ready()

    def feed_far():
        feed_block[1 - odd["y"]] = project_in(1, ws1).astype(BF)
        recur_ready()

    s1_own = when_all(1, lambda: at(clock[0], feed_own, 0.6))
    s1_far = when_all(3, lambda: at(clock[0], feed_far, 0.7))
    recur_ready = both(lambda: at(clock[0], recur, 0.8))
    end = slice(length - 1, length)

    def recur():
        drive = feed_block[...].reshape(2 * length, part_width)
        for j in range(flat // chunk):
            part = slice(j * chunk, (j + 1) * chunk)
            shift = slice(flat + j * chunk, flat + (j + 1) * chunk)
            push_r = jnp.dot(drive, drive_r[:, part], preferred_element_type=F32)
            push_i = jnp.dot(drive, drive_i[:, part], preferred_element_type=F32)
            for b in (0, 1):
                span = slice(b * length, (b + 1) * length)
                back_r, back_i = rotate(
                    undo_r[:, part], undo_i[:, part], push_r[span, :], push_i[span, :]
                )
                scaled[b, :, part] = back_r.astype(BF)
                scaled[b, :, shift] = back_i.astype(BF)
        lower = (iota((length, length), 0) >= iota((length, length), 1)).astype(BF)
        for b in (0, 1):
            for j in range(2 * flat // chunk):
                part = slice(j * chunk, (j + 1) * chunk)
                summed[b, :, part] = jnp.dot(lower, scaled[b, :, part], preferred_element_type=F32)
        span_r, span_i = power_r[end, :], power_i[end, :]
        first_r, first_i = rotate(span_r, span_i, summed[0, end, 0:flat], summed[0, end, flat:2 * flat])
        second_r, second_i = rotate(span_r, span_i, summed[1, end, 0:flat], summed[1, end, flat:2 * flat])
        rows[12:13, :], rows[13:14, :] = first_r, first_i
        moved_r, moved_i = rotate(span_r, span_i, first_r, first_i)
        finals[y // 2, :, 0:flat] = moved_r + second_r
        finals[y // 2, :, flat:2 * flat] = moved_i + second_i
        spread_out(0, "y", finals, 8 * flat, 2, lambda: at(clock[0], scan_row, 0.1))

    def scan_row():
        span_r, span_i = power_r[end, :], power_i[end, :]
        span_r, span_i = rotate(span_r, span_i, span_r, span_i)
        zero = jnp.zeros((1, flat), F32)
        sum_r, sum_i, before_r, before_i = zero, zero, zero, zero
        jump_r, jump_i = zero + 1.0, zero
        mine_r, mine_i = zero, zero
        for yy in range(SIDE // 2):
            here_now = y // 2 == yy
            before_r, before_i = jnp.where(here_now, sum_r, before_r), jnp.where(here_now, sum_i, before_i)
            mine_r, mine_i = jnp.where(here_now, jump_r, mine_r), jnp.where(here_now, jump_i, mine_i)
            next_r, next_i = rotate(span_r, span_i, sum_r, sum_i)
            sum_r = next_r + finals[yy, :, 0:flat]
            sum_i = next_i + finals[yy, :, flat:2 * flat]
            jump_r, jump_i = rotate(span_r, span_i, jump_r, jump_i)
        rows[6:7, :], rows[7:8, :] = before_r, before_i
        rows[8:9, :], rows[9:10, :] = mine_r, mine_i
        rows[10:11, :], rows[11:12, :] = jump_r, jump_i
        totals[z, :, 0:flat], totals[z, :, flat:2 * flat] = sum_r, sum_i
        spread_out(1, "z", totals, 8 * flat, 1, lambda: at(clock[0], scan_all, 1.2))

    def scan_all():
        sum_r, sum_i = rows[0:1, :], rows[1:2, :]
        jump_r, jump_i = rows[10:11, :], rows[11:12, :]
        start_r, start_i = sum_r, sum_i
        for zz in range(SIDE):
            start_r, start_i = jnp.where(z == zz, sum_r, start_r), jnp.where(z == zz, sum_i, start_i)
            next_r, next_i = rotate(jump_r, jump_i, sum_r, sum_i)
            sum_r = next_r + totals[zz, :, 0:flat]
            sum_i = next_i + totals[zz, :, flat:2 * flat]
        final_half[odd["y"], 0] = as_table(sum_r)
        final_half[odd["y"], 1] = as_table(sum_i)
        hand_over(
            4, "y", final_half.at[odd["y"]], final_half.at[odd["y"]], final_half.at[1 - odd["y"]],
            8 * flat, store_final,
        )
        lead_r, lead_i = rotate(rows[8:9, :], rows[9:10, :], start_r, start_i)
        entry_r, entry_i = lead_r + rows[6:7, :], lead_i + rows[7:8, :]
        next_r, next_i = rotate(power_r[end, :], power_i[end, :], entry_r, entry_i)
        entries = ((entry_r, entry_i), (next_r + rows[12:13, :], next_i + rows[13:14, :]))
        for b in (0, 1):
            into_r, into_i = entries[b]
            for j in range(flat // chunk):
                part = slice(j * chunk, (j + 1) * chunk)
                shift = slice(flat + j * chunk, flat + (j + 1) * chunk)
                state_r, state_i = rotate(
                    power_r[:, part], power_i[:, part],
                    summed[b, :, part] + into_r[:, part], summed[b, :, shift] + into_i[:, part],
                )
                states[b, :, part] = state_r.astype(BF)
                states[b, :, shift] = state_i.astype(BF)
        answer = lax.dot_general(
            states[...].reshape(2 * length, 2 * flat), emit[...], NT, preferred_element_type=F32
        )
        direct = skip_gain[:, lanes_from(odd["y"], part_width)]
        answer = answer + direct * feed_block[...].reshape(2 * length, part_width).astype(F32)
        act_all[odd["y"], t] = jax.nn.gelu(answer).astype(BF).reshape(2, length, part_width)
        exchange(
            4, 5, "y", act_all, lambda: (state_far(), state_own()),
            lambda own: state_own() if own else state_far(),
        )

    def store_final():
        for half in (0, 1):
            load(
                "final" + str(half), final_half.at[half],
                final_out.at[:, pl.ds(half * groups, groups)],
            )

    def exchange(number, pair, axis, blocks, shared, relayed):
        amount = 2 * length * part_width * 2
        mine = odd[axis]

        def relay_block(i):
            sent_block, got_block = (mine, 1 - mine) if i == 0 else (1 - mine, mine)
            hand_over(
                pair + i, axis, blocks.at[mine, t, sent_block], blocks.at[mine, t, sent_block],
                blocks.at[1 - mine, t, got_block], amount / 2,
                lambda: share(
                    number + 1 + i, lambda c: blocks.at[1 - mine, c, got_block], amount / 2,
                    lambda: relayed(i),
                ),
            )

        relay_block(0)
        relay_block(1)
        share(number, lambda c: blocks.at[mine, c], amount, shared)

    edge = halo.shape[1]
    kernel_size = conv_taps.shape[0]

    def gate(i):
        pair = project_in(i, wc1)
        return (pair[:, 0:part_width] * jax.nn.sigmoid(pair[:, part_width:width])).astype(BF)

    def gate_own():
        gated_block[odd["z"]] = gate(0)
        gate_ready()

    def gate_far():
        gated_block[1 - odd["z"]] = gate(2)
        gate_ready()

    c1_own = when_all(1, lambda: at(clock[0], gate_own, 1.0))
    c1_far = when_all(3, lambda: at(clock[0], gate_far, 1.0))
    gate_ready = both(lambda: at(clock[0], pass_edge, 0.1))
    last = pl.ds(length - edge, edge)

    def pass_edge():
        for b, to, slot in (
            (0, beside("y", 1), at_end),
            (1, following, 1 - at_end),
        ):
            start(
                remote(
                    gated_block.at[b, last], halo.at[slot], halo_sem.at[b], halo_sem.at[2 + slot], to
                )
            )
        at(transit(("y", 1), 2 * edge * part_width * 2), convolve, 1.0)
        for b in (0, 1):
            padded[b, edge:edge + length, :] = gated_block[b].astype(F32)

    def convolve():
        for slot in (0, 1):
            bytes_of(halo.at[slot], halo_sem.at[2 + slot])
        padded[0, 0:edge, :] = jnp.where(z // 2 + y > 0, halo[0].astype(F32), 0.0)
        padded[1, 0:edge, :] = halo[1].astype(F32)
        taps = conv_taps[:, lanes_from(odd["z"], part_width)]
        lag = edge - (kernel_size - 1)
        for block in (0, 1):
            answer = jnp.zeros((length, part_width), F32)
            for b in range(8):
                tall = length + (8 if b else 0)
                part = jnp.zeros((tall, part_width), F32)
                for a in range(edge // 8 + 1):
                    k = 8 * a + b - lag
                    if 0 <= k < kernel_size:
                        part = part + taps[k:k + 1, :] * padded[block, 8 * a:8 * a + tall, :]
                if b:
                    shifted[b, :, :] = part
                    answer = answer + shifted[b, b:b + length, :]
                else:
                    answer = answer + part
            conv_all[odd["z"], t, block] = answer.astype(BF)
        exchange(
            7, 8, "z", conv_all, lambda: (norm_far(), norm_own()),
            lambda own: norm_own() if own else norm_far(),
        )

    def channel_norm(which, own):
        count = 2 * CHIPS * width
        def body(i, carry):
            part = pl.ds(pl.multiple_of(i * 16, 16), 16)
            pieces = [
                conv_all[c % 2, c // 2, which, part, :].astype(F32) for c in range(4 * CHIPS)
            ]
            total = pieces[0]
            for piece in pieces[1:]:
                total = total + piece
            mean = jnp.sum(total, axis=1, keepdims=True) / count
            pieces = [piece - mean for piece in pieces]
            total = pieces[0] * pieces[0]
            for piece in pieces[1:]:
                total = total + piece * piece
            scale = lax.rsqrt(jnp.sum(total, axis=1, keepdims=True) / count + 1e-5)
            for c, piece in enumerate(pieces):
                lanes = slice(c * part_width, (c + 1) * part_width)
                value = piece * scale * chan_gain[:, lanes] + chan_shift[:, lanes]
                half = slice(c % 2 * part_width, (c % 2 + 1) * part_width)
                conv_act[which, c // 2, part, half] = jax.nn.silu(value).astype(BF)
            return carry
        lax.fori_loop(0, length // 16, body, 0, unroll=2)
        (conv_own if own else conv_far)()

    norm_own = both(lambda: at(clock[0], lambda: channel_norm(odd["z"], True), 1.5))
    norm_far = both(lambda: at(clock[0], lambda: channel_norm(1 - odd["z"], False), 1.5))

    def project(piece, weights):
        count = weights.shape[3]
        total = None
        for c in range(2 * CHIPS):
            term = jnp.dot(piece(c), weights[c].reshape(width, count), preferred_element_type=F32)
            total = term if total is None else total + term
        return total

    def state_out(i):
        pair = project(
            lambda c: jnp.concatenate([act_all[0, c, i], act_all[1, c, i]], axis=1), ws2
        )
        return pair[:, 0:part_columns] * jax.nn.sigmoid(pair[:, part_columns:columns])

    def state_out_own():
        state_half[odd["y"]] = state_out(odd["y"])
        finish_ready()

    def state_out_far():
        state_back[...] = state_out(1 - odd["y"]).astype(BF)
        hand_over(
            10, "y", state_back, state_got, state_got, length * part_columns * 2, state_returned
        )

    def state_returned():
        state_half[1 - odd["y"]] = state_got[...].astype(F32)
        finish_ready()

    def conv_out_own():
        conv_half[odd["z"]] = project(lambda c: conv_act[odd["z"], c], wc2)
        finish_ready()

    def conv_out_far():
        conv_back[...] = project(lambda c: conv_act[1 - odd["z"], c], wc2).astype(BF)
        hand_over(11, "z", conv_back, conv_got, conv_got, length * part_columns * 2, conv_returned)

    def conv_returned():
        conv_half[1 - odd["z"]] = conv_got[...].astype(F32)
        finish_ready()

    state_own = when_all(3, lambda: at(clock[0], state_out_own, 1.0))
    state_far = when_all(3, lambda: at(clock[0], state_out_far, 1.0))
    conv_own = both(lambda: at(clock[0], conv_out_own, 0.6))
    conv_far = both(lambda: at(clock[0], conv_out_far, 0.6))
    finish_ready = when_all(4, lambda: at(clock[0], finish, 0.5))

    def finish():
        for half in (0, 1):
            lanes = slice(half * part_columns, (half + 1) * part_columns)
            result[:, lanes] = (state_half[half] + conv_half[half]).astype(BF)
        load("out", result, out)
        drain(1e9)
        for wait in closing:
            wait()
        after("final0")
        after("final1")
        after("out")

    run()


def local(
    tokens, norm_gain, conv_value, conv_gate, state_feed, conv_taps, chan_gain, chan_shift,
    conv_project, decay_rate, frequency, input_real, input_imag, output_real, output_imag,
    skip_gain, state_value, state_gate, initial_state,
):
    length, features = tokens.shape
    groups, size, wide = input_real.shape
    flat, width = groups // 2 * size, groups * wide
    deep1, columns = conv_value.shape[0], conv_project.shape[1]
    deep2 = conv_project.shape[0]
    edge = 32
    args = (
        tokens, norm_gain.reshape(1, -1), conv_value, conv_gate, state_feed, conv_taps,
        chan_gain.reshape(1, -1), chan_shift.reshape(1, -1), conv_project, decay_rate, frequency,
        jnp.swapaxes(input_real, 1, 2), jnp.swapaxes(input_imag, 1, 2), output_real, output_imag,
        skip_gain.reshape(1, -1), state_value, state_gate, initial_state,
    )
    anywhere = pl.BlockSpec(memory_space=pl.ANY)
    vmem = pltpu.VMEM
    dma = pltpu.SemaphoreType.DMA
    many = 2 * CHIPS
    return pl.pallas_call(
        kernel,
        out_shape=(
            jax.ShapeDtypeStruct((length, columns), BF),
            jax.ShapeDtypeStruct(initial_state.shape, F32),
        ),
        in_specs=[anywhere] * len(args),
        out_specs=(anywhere, anywhere),
        scratch_shapes=[
            *(vmem(args[i].shape, args[i].dtype) for i in SMALL),
            vmem((SIDE, SIDE, deep1, width // 2), BF),
            vmem((SIDE, SIDE, deep1, width), BF),
            vmem((SIDE, SIDE, deep2, columns), BF),
            vmem((SIDE, SIDE, deep2, columns // 2), BF),
            vmem((2, deep1, width // 2), BF),
            vmem((2, deep1, width), BF),
            vmem((2, deep2, columns), BF),
            vmem((2, deep2, columns // 2), BF),
            vmem((length, features), BF),
            vmem((length, 128), F32),
            vmem((3, many, length, features // many), BF),
            vmem((length, columns), BF),
            vmem((2, 2, groups // 2, size), F32),
            *(vmem((length, flat), F32) for _ in range(4)),
            vmem((width // 2, flat), BF),
            vmem((width // 2, flat), BF),
            vmem((width // 2, 2 * flat), BF),
            vmem((2, length, 2 * flat), BF),
            vmem((2, length, 2 * flat), F32),
            vmem((2, length, 2 * flat), BF),
            vmem((16, flat), F32),
            vmem((SIDE // 2, 1, 2 * flat), F32),
            vmem((SIDE, 1, 2 * flat), F32),
            vmem((2, length, width // 2), BF),
            vmem((2, length, width // 2), BF),
            vmem((2, edge, width // 2), BF),
            vmem((2, edge + length, width // 2), F32),
            vmem((8, length + 8, width // 2), F32),
            vmem((2, many, 2, length, width // 2), BF),
            vmem((2, many, 2, length, width // 2), BF),
            vmem((2, many, length, width), BF),
            *(
                vmem(shape, held)
                for _ in range(2)
                for shape, held in (
                    ((2, length, columns // 2), F32),
                    ((length, columns // 2), BF),
                    ((length, columns // 2), BF),
                )
            ),
            dma((20,)),
            dma((4,)),
            dma((4, 23)),
            dma((2,)),
            dma((2,)),
            dma((4,)),
            dma((10,)),
            dma((10, 4)),
            dma((12,)),
            dma((12,)),
            dma((4,)),
            dma((4, 2)),
        ],
        compiler_params=pltpu.CompilerParams(
            collective_id=0, has_side_effects=True, vmem_limit_bytes=62 * 1024 * 1024
        ),
        name="mixer",
    )(*args)


def solution(mesh):
    in_specs = (
        P("sp", None), P(), P("sp", "tp"), P("sp", "tp"), P("sp", "tp"), P(None, "tp"), P(), P(),
        P("sp", "tp"), P("tp", None), P("tp", None), P("tp", None, None), P("tp", None, None),
        P("tp", None, None), P("tp", None, None), P("tp"), P("sp", "tp"), P("sp", "tp"),
        P(None, "tp", None),
    )
    out_specs = (P("sp", "tp"), P(None, "tp", None))
    return jax.shard_map(local, mesh=mesh, in_specs=in_specs, out_specs=out_specs, check_vma=False)
```

```python
import heapq

import jax
import jax.numpy as jnp
from jax import lax
from jax.experimental import pallas as pl
from jax.experimental.pallas import tpu as pltpu
from jax.sharding import PartitionSpec as P

BF, F32 = jnp.bfloat16, jnp.float32
HIGHEST = lax.Precision.HIGHEST
MESH = pl.DeviceIdType.MESH
SIDE = 8
WINDOW = (3, 2, 3, 3)
WHEN = (24.0, 30.0, 2.0)
CLASSES = ((0,), (1, 7, 2, 6), (3, 5, 4))
CHIPS = 4
NT = (((1,), (1,)), ((), ()))


def hops(direction, half):
    return SIDE // 2 if (direction > 0) == (half == 0) else SIDE // 2 - 1


def slot_of(direction, half, k):
    return k if direction > 0 else hops(1, half) + k


def rotate(first_real, first_imag, second_real, second_imag):
    return (
        first_real * second_real - first_imag * second_imag,
        first_real * second_imag + first_imag * second_real,
    )


def iota(shape, dim):
    return lax.broadcasted_iota(jnp.int32, shape, dim)


SMALL = (1, 5, 6, 7, 9, 10, 11, 12, 13, 14, 15, 18)


def kernel(*refs):
    (
        tokens, norm_gain, conv_value, conv_gate, state_feed, conv_taps, chan_gain, chan_shift,
        conv_project, decay_rate, frequency, input_real, input_imag, output_real, output_imag,
        skip_gain, state_value, state_gate, initial_state, out, final_out,
    ) = refs[:21]
    small = refs[21:21 + len(SMALL)]
    (
        ws1, wc1, ws2, wc2, stage_s1, stage_c1, stage_s2, stage_c2, raw, scale, normed, result,
        final_half, power_r, power_i, undo_r, undo_i, drive_r, drive_i, emit, scaled, summed,
        states, rows, finals, totals, feed_block, gated_block, halo, padded,
        shifted, conv_all, act_all, conv_act, state_half, state_back, state_got, conv_half, conv_back,
        conv_got,
        load_sem, ring_send, ring_recv, scan_send, scan_recv, halo_sem, tp_send, tp_recv, pair_send,
        pair_recv, deal_send, deal_recv,
    ) = refs[21 + len(SMALL):]
    seq = lax.axis_index("sp")
    t = lax.axis_index("tp")
    z, y = seq // SIDE, seq % SIDE
    chip, core = t // 2, t % 2
    length = tokens.shape[0]
    groups, wide, size = input_real.shape
    width = groups * wide
    part_width = width // 2
    groups = groups // 2
    flat = groups * size
    columns = out.shape[1]
    part_columns = columns // 2

    def device(zz, yy, tt):
        return {"sp": zz * SIDE + yy, "tp": tt}

    def step_to(at, by, count):
        return lax.rem(at + by + count, count)

    def remote(src, dst, send, recv, to):
        return pltpu.make_async_remote_copy(
            src_ref=src, dst_ref=dst, send_sem=send, recv_sem=recv, device_id=to, device_id_type=MESH
        )

    queue = []
    sent = []
    free = {}
    clock = [0.0, 0]

    def at(time, fn, cost=0.0):
        heapq.heappush(queue, (time, clock[1], cost, fn))
        clock[1] += 1

    def run():
        while queue:
            time, _, cost, fn = heapq.heappop(queue)
            clock[0] = max(clock[0], time)
            fn()
            clock[0] += cost

    def start(moving):
        moving.start()
        sent.append((clock[0], moving))

    closing = []

    def drain(before):
        kept = []
        for time, moving in sent:
            if time < before:
                moving.wait_send()
            else:
                kept.append((time, moving))
        sent[:] = kept

    def transit(link, size, count=1, rate=50e3):
        begin = max(clock[0], free.get(link, 0.0))
        free[link] = begin + size * count / rate
        fixed = 1.5 if link == "core" else 4.0 if link[0] == "x" else 2.9
        return free[link] + fixed + 0.6 * (count - 1)

    def when_all(number, fn):
        left = [number]

        def one():
            left[0] -= 1
            if left[0] == 0:
                fn()
        return one

    loads, counted = {}, []

    def load(name, src, dst):
        if name not in counted:
            counted.append(name)
        moving = pltpu.make_async_copy(src, dst, load_sem.at[counted.index(name)])
        moving.start()
        loads[name] = moving

    def bytes_of(ref, sem):
        pltpu.make_async_copy(ref, ref, sem).wait()

    def after(name, three=None):
        if three is None:
            loads[name].wait()
        else:
            bytes_of(three, load_sem.at[counted.index(name)])

    here = {"z": z, "y": y}
    odd = {"z": z % 2, "y": y % 2}

    def lanes_from(half, count):
        return pl.ds(pl.multiple_of(half * count, count), count)

    def staged(name, axis, pieces, stage, own, count):
        for half in (0, 1):
            for i, source in enumerate(pieces):
                load(
                    name, source.at[:, half * count:(half + 1) * count],
                    stage.at[half, :, i * count:(i + 1) * count],
                )
        for i, source in enumerate(pieces):
            load(
                name, source.at[:, lanes_from(odd[axis], count)], own.at[:, i * count:(i + 1) * count]
            )

    staged("s1", "y", (state_feed,), stage_s1, ws1.at[z, y], part_width)
    staged("c1", "z", (conv_value, conv_gate), stage_c1, wc1.at[z, y], part_width)
    load("raw", tokens, raw)
    for i, place in enumerate(SMALL):
        load(place, refs[place], small[i])
    (
        norm_gain, conv_taps, chan_gain, chan_shift, decay_rate, frequency, input_real, input_imag,
        output_real, output_imag, skip_gain, initial_state,
    ) = small
    staged("s2", "y", (state_value, state_gate), stage_s2, ws2.at[z, y], part_columns)
    staged("c2", "z", (conv_project,), stage_c2, wc2.at[z, y], part_columns)

    barrier = pltpu.get_barrier_semaphore()
    at_end, at_start = y // (SIDE - 1), (SIDE - 1 - y) // (SIDE - 1)
    following = device(step_to(z, 2 * at_end, SIDE), step_to(y, 1, SIDE), t)
    preceding = device(step_to(z, -2 * at_start, SIDE), step_to(y, -1, SIDE), t)
    partners = []
    for d in range(1, SIDE):
        partners.append(device(z, step_to(y, d, SIDE), t))
        partners.append(device(step_to(z, d, SIDE), y, t))
    for d in range(1, 2 * CHIPS):
        partners.append(device(z, y, step_to(t, d, 2 * CHIPS)))
    partners.append(following)
    partners.append(preceding)
    for partner in partners:
        pl.semaphore_signal(barrier, inc=1, device_id=partner, device_id_type=MESH)
    pl.semaphore_wait(barrier, len(partners))

    def beside(axis, by):
        moved = step_to(here[axis], by, SIDE)
        return device(moved, y, t) if axis == "z" else device(z, moved, t)

    def spread_out(number, axis, blocks, size, stride, done):
        position = here[axis] // stride
        all_others = blocks.at[pl.ds(0, SIDE // stride - 1)]
        latest = 0.0
        for d in (4, 3, 5, 2, 6, 1, 7):
            if d % stride == 0:
                remote(
                    blocks.at[position], blocks.at[position], scan_send.at[number],
                    scan_recv.at[number], beside(axis, d),
                ).start()
                direction, count = (1, d) if d <= SIDE // 2 else (-1, SIDE - d)
                latest = max(latest, transit((axis, direction), size, count))

        def arrived():
            bytes_of(all_others, scan_recv.at[number])
            done()
        at(latest, arrived)
        closing.append(lambda: bytes_of(all_others, scan_send.at[number]))

    def trains(number, axis, across, stage, block, several, size, window, done, nearly=None):
        position, lane = here[axis], here[across]
        members = [
            (which, direction, k)
            for which in range(len(CLASSES)) for direction in (1, -1) for k in range(SIDE // 2)
            if any(k < hops(direction, d % 2) for d in CLASSES[which])
        ]
        finished = when_all(len(members), done)
        passed = when_all(len(CLASSES), nearly or (lambda: None))
        ready, active = [], [0]
        left = [len(c) * (SIDE - 1) for c in CLASSES]

        def dealt(d, source, to):
            half = odd[across] if d % 2 == 0 else 1 - odd[across]
            return remote(
                stage.at[half], block(position, source), deal_send.at[number],
                deal_recv.at[number, int(d in CLASSES[-1])], to,
            )

        def slot(which, direction, k):
            return members.index((which, direction, k))

        def copy(which, d, direction, k, source):
            held = block(source, step_to(lane, -d, SIDE))
            return remote(
                held, held, ring_send.at[number], ring_recv.at[number, slot(which, direction, k)],
                beside(axis, direction),
            )

        def send(which, direction, k):
            time = 0.0
            for d in CLASSES[which]:
                if k < hops(direction, d % 2):
                    copy(which, d, direction, k, step_to(position, -direction * k, SIDE)).start()
                    time = transit((axis, direction), size)
                    left[which] -= 1
            at(time, lambda: arrived(which, direction, k))
            if left[which] == 0:
                active[0] -= 1
                passed()

        def arrived(which, direction, k):
            count = sum(k < hops(direction, d % 2) for d in CLASSES[which])
            bytes_of(several(count), ring_recv.at[number, slot(which, direction, k)])
            if any(k + 1 < hops(direction, d % 2) for d in CLASSES[which]):
                send(which, direction, k + 1)
                inject()
            finished()

        def inject():
            while ready and active[0] < window[0]:
                which = ready.pop(0)
                active[0] += 1
                for direction in (1, -1):
                    send(which, direction, 0)

        def received(which):
            count = len(CLASSES[2]) if which else SIDE - 1 - len(CLASSES[2])
            bytes_of(several(count), deal_recv.at[number, which])
            ready.extend([2] if which else list(range(1, len(CLASSES) - 1)))
            inject()

        def deal():
            for which, members_of in enumerate(((1, 7, 2, 6), CLASSES[-1])):
                time = 0.0
                for d in members_of:
                    dealt(d, lane, beside(across, d)).start()
                    direction, count = (1, d) if d <= SIDE // 2 else (-1, SIDE - d)
                    time = max(time, transit((across, direction), size, count))
                at(time, lambda which=which: received(which))
            ready.insert(0, 0)
            inject()

        def go(amount):
            window[0] = amount
            inject()

        closing.append(lambda: bytes_of(block(pl.ds(0, SIDE - 1), pl.ds(0, SIDE)), ring_send.at[number]))
        closing.append(lambda: bytes_of(several(SIDE - 1), deal_send.at[number]))
        return deal, go

    def mate(axis):
        other_one = here[axis] + 1 - 2 * odd[axis]
        return device(other_one, y, t) if axis == "z" else device(z, other_one, t)

    def hand_over(number, axis, src, dst, landing, size, done):
        start(remote(src, dst, pair_send.at[number], pair_recv.at[number], mate(axis)))
        time = 0.6 + max(transit((axis, 1), size), transit((axis, -1), size))

        def arrived():
            remote(src, landing, pair_send.at[number], pair_recv.at[number], mate(axis)).wait_recv()
            done()
        at(time, arrived)

    other = t + 1 - 2 * core

    def share(number, block, size, done, later=None):
        near_sem = tp_recv.at[number, 0]

        def copy(slot, source, to):
            return remote(
                block(source), block(source), tp_send.at[number], tp_recv.at[number, slot],
                device(z, y, to),
            )

        def near():
            if later is None:
                bytes_of(block(pl.ds(0, CHIPS)), near_sem)
            else:
                later.append(lambda: bytes_of(block(pl.ds(0, CHIPS)), near_sem))
            done()

        latest = [0.0]
        all_near = when_all(4, lambda: at(latest[0], near))

        def to_core(source):
            copy(0, source, other).start()
            latest[0] = max(latest[0], transit("core", size, 1, 200e3))
            all_near()

        def far(d):
            source = step_to(chip, -d, CHIPS) * 2 + core
            copy(d, source, source).wait_recv()
            to_core(source)

        for d in (1, 3, 2):
            copy(d, t, step_to(chip, d, CHIPS) * 2 + core).start()
            if d == 2:
                time = 0.6 + max(transit(("x", hop), size) for hop in (1, -1))
            else:
                time = transit(("x", 2 - d), size)
            at(time, lambda d=d: far(d))
        to_core(t)
        closing.append(lambda: bytes_of(block(pl.ds(0, 2 * CHIPS - 1)), tp_send.at[number]))

    unit1 = ws1.shape[2] * part_width * 2

    def both(fn):
        return when_all(2, fn)

    deal_s1, _ = trains(
        0, "z", "y", stage_s1, lambda r, p: ws1.at[r, p], lambda n: ws1.at[0, pl.ds(0, n)], unit1, [WINDOW[0]],
        lambda: (s1_far(), s1_own()), lambda: go_s2(WINDOW[1]),
    )
    deal_c1, _ = trains(
        1, "y", "z", stage_c1, lambda r, p: wc1.at[p, r], lambda n: wc1.at[pl.ds(0, n), 0], 2 * unit1, [WINDOW[2]],
        lambda: (c1_far(), c1_own()), lambda: go_c2(WINDOW[3]),
    )
    deal_s2, go_s2 = trains(
        2, "z", "y", stage_s2, lambda r, p: ws2.at[r, p], lambda n: ws2.at[0, pl.ds(0, n)], 2 * unit1, [0],
        lambda: (state_own(), state_far()),
    )
    deal_c2, go_c2 = trains(
        3, "y", "z", stage_c2, lambda r, p: wc2.at[p, r], lambda n: wc2.at[pl.ds(0, n), 0], unit1, [0],
        lambda: (conv_own(), conv_far()),
    )

    def begin():
        after("s1", ws1.at[0, pl.ds(0, 3)])
        deal_s1()
        after("c1", wc1.at[0, pl.ds(0, 3)])
        deal_c1()

    at(0.0, begin)
    at(WHEN[0], lambda: (after("s2", ws2.at[0, pl.ds(0, 3)]), deal_s2()))
    at(WHEN[1], lambda: (after("c2", wc2.at[0, pl.ds(0, 3)]), deal_c2()))

    step = normed.shape[3]

    def measure():
        for name in ("raw", *SMALL):
            after(name)
        def body(i, carry):
            part = pl.ds(pl.multiple_of(i * 16, 16), 16)
            value = raw[part, :].astype(F32)
            mean = jnp.mean(value * value, axis=1, keepdims=True)
            scale[part, :] = jnp.broadcast_to(lax.rsqrt(mean + 1e-6), (16, 128))
            return carry
        lax.fori_loop(0, length // 16, body, 0, unroll=2)
        normalise(t)
        swap(1, "y", lambda: s1_far())
        at(WHEN[2], lambda: swap(2, "z", lambda: c1_far()))

    owed = {"y": [], "z": []}

    def swap(i, axis, done):
        for half in (0, 1):
            number = 2 * i - 2 + half
            part = pl.ds(half * length // 2, length // 2)
            block = normed.at[i, t, part]
            hand_over(
                number, axis, normed.at[0, t, part], block, block, length * step,
                lambda number=number, part=part: share(
                    number, lambda c: normed.at[i, c, part], length * step, done, owed[axis]
                ),
            )

    def normalise(c):
        lanes = lanes_from(c, step)
        value = raw[:, lanes].astype(F32)
        normed[0, c] = (value * scale[:, 0:1] * norm_gain[:, lanes]).astype(BF)

    def normalise_all():
        def body(c, carry):
            pl.when(c != t)(lambda: normalise(c))
            return carry
        lax.fori_loop(0, 2 * CHIPS, body, 0)

    def spread():
        return ((iota((size, flat), 1) & (size - 1)) == iota((size, flat), 0)).astype(F32)

    def owner():
        return (iota((groups, flat), 1) // size) == iota((groups, flat), 0)

    def as_row(table):
        wide_table = jnp.dot(table, spread(), precision=HIGHEST, preferred_element_type=F32)
        return jnp.sum(jnp.where(owner(), wide_table, 0.0), axis=0, keepdims=True)

    def as_table(row):
        return lax.dot_general(
            jnp.where(owner(), row, 0.0), spread(), NT, precision=HIGHEST, preferred_element_type=F32
        )

    total_tokens = length * SIDE * SIDE

    own_groups = lanes_from(odd["y"], groups)

    def tables():
        rate = -as_row(decay_rate[own_groups, :]) / total_tokens
        turn = as_row(frequency[own_groups, :])
        rows[0:1, :] = as_row(initial_state[0, own_groups, :])
        rows[1:2, :] = as_row(initial_state[1, own_groups, :])
        magnitude = jnp.exp(rate)
        step_r = magnitude * jnp.cos(turn)
        step_i = magnitude * jnp.sin(turn)
        modulus = rate * rate + turn * turn
        lift = step_r - 1.0
        factor_r = (lift * rate + step_i * turn) / modulus
        factor_i = (step_i * rate - lift * turn) / modulus
        count = iota((8, flat), 0) + 1
        block_r, block_i = jnp.ones((8, flat), F32), jnp.zeros((8, flat), F32)
        square_r, square_i = step_r, step_i
        for place in range(4):
            chosen = ((count >> place) & 1) == 1
            next_r, next_i = rotate(block_r, block_i, square_r, square_i)
            block_r = jnp.where(chosen, next_r, block_r)
            block_i = jnp.where(chosen, next_i, block_i)
            if place < 3:
                square_r, square_i = rotate(square_r, square_i, square_r, square_i)
        rows[2:3, :], rows[3:4, :] = square_r, square_i
        rows[4:5, :], rows[5:6, :] = factor_r, factor_i

        def body(i, carry):
            now_r, now_i = carry
            part = pl.ds(pl.multiple_of(i * 8, 8), 8)
            power_r[part, :], power_i[part, :] = now_r, now_i
            inverse = 1.0 / (now_r * now_r + now_i * now_i)
            un_r, un_i = rotate(now_r * inverse, -now_i * inverse, rows[4:5, :], rows[5:6, :])
            undo_r[part, :], undo_i[part, :] = un_r, un_i
            return rotate(now_r, now_i, rows[2:3, :], rows[3:4, :])
        lax.fori_loop(0, length // 8, body, (block_r, block_i))

    def matrices():
        stretch = spread().astype(BF)
        def fill(source, sign, dest, lanes):
            for g in range(groups):
                copied = jnp.dot((sign * source[odd["y"] * groups + g]).astype(BF), stretch, preferred_element_type=F32)
                kept = iota((wide, flat), 1) // size == g
                dest[g * wide:(g + 1) * wide, lanes] = jnp.where(kept, copied, 0.0).astype(BF)
        fill(input_real, 1.0, drive_r, slice(0, flat))
        fill(input_imag, 1.0, drive_i, slice(0, flat))
        fill(output_real, 1.0, emit, slice(0, flat))
        fill(output_imag, -1.0, emit, slice(flat, 2 * flat))

    at(0.5, measure, 1.0)
    at(6.0, normalise_all, 1.5)
    at(8.0, tables, 1.4)
    at(9.0, matrices, 1.2)

    chunk = 256

    def project_in(i, weights):
        count = weights.shape[3]
        total = None
        for c in range(2 * CHIPS):
            term = jnp.dot(normed[i, c], weights[c].reshape(step, count), preferred_element_type=F32)
            total = term if total is None else total + term
        return total

    def feed_own():
        feed_block[odd["y"]] = project_in(0, ws1).astype(BF)
        recur_ready()

    def feed_far():
        for wait in owed["y"]:
            wait()
        feed_block[1 - odd["y"]] = project_in(1, ws1).astype(BF)
        recur_ready()

    s1_own = when_all(1, lambda: at(clock[0], feed_own, 0.6))
    s1_far = when_all(3, lambda: at(clock[0], feed_far, 0.7))
    recur_ready = both(lambda: at(clock[0], recur, 0.8))
    end = slice(length - 1, length)

    def recur():
        drive = feed_block[...].reshape(2 * length, part_width)
        for j in range(flat // chunk):
            part = slice(j * chunk, (j + 1) * chunk)
            shift = slice(flat + j * chunk, flat + (j + 1) * chunk)
            push_r = jnp.dot(drive, drive_r[:, part], preferred_element_type=F32)
            push_i = jnp.dot(drive, drive_i[:, part], preferred_element_type=F32)
            for b in (0, 1):
                span = slice(b * length, (b + 1) * length)
                back_r, back_i = rotate(
                    undo_r[:, part], undo_i[:, part], push_r[span, :], push_i[span, :]
                )
                scaled[b, :, part] = back_r.astype(BF)
                scaled[b, :, shift] = back_i.astype(BF)
        lower = (iota((length, length), 0) >= iota((length, length), 1)).astype(BF)
        for b in (0, 1):
            for j in range(2 * flat // chunk):
                part = slice(j * chunk, (j + 1) * chunk)
                summed[b, :, part] = jnp.dot(lower, scaled[b, :, part], preferred_element_type=F32)
        span_r, span_i = power_r[end, :], power_i[end, :]
        first_r, first_i = rotate(span_r, span_i, summed[0, end, 0:flat], summed[0, end, flat:2 * flat])
        second_r, second_i = rotate(span_r, span_i, summed[1, end, 0:flat], summed[1, end, flat:2 * flat])
        rows[12:13, :], rows[13:14, :] = first_r, first_i
        moved_r, moved_i = rotate(span_r, span_i, first_r, first_i)
        finals[y // 2, :, 0:flat] = moved_r + second_r
        finals[y // 2, :, flat:2 * flat] = moved_i + second_i
        spread_out(0, "y", finals, 8 * flat, 2, lambda: at(clock[0], scan_row, 0.1))

    def scan_row():
        span_r, span_i = power_r[end, :], power_i[end, :]
        span_r, span_i = rotate(span_r, span_i, span_r, span_i)
        zero = jnp.zeros((1, flat), F32)
        sum_r, sum_i, before_r, before_i = zero, zero, zero, zero
        jump_r, jump_i = zero + 1.0, zero
        mine_r, mine_i = zero, zero
        for yy in range(SIDE // 2):
            here_now = y // 2 == yy
            before_r, before_i = jnp.where(here_now, sum_r, before_r), jnp.where(here_now, sum_i, before_i)
            mine_r, mine_i = jnp.where(here_now, jump_r, mine_r), jnp.where(here_now, jump_i, mine_i)
            next_r, next_i = rotate(span_r, span_i, sum_r, sum_i)
            sum_r = next_r + finals[yy, :, 0:flat]
            sum_i = next_i + finals[yy, :, flat:2 * flat]
            jump_r, jump_i = rotate(span_r, span_i, jump_r, jump_i)
        rows[6:7, :], rows[7:8, :] = before_r, before_i
        rows[8:9, :], rows[9:10, :] = mine_r, mine_i
        rows[10:11, :], rows[11:12, :] = jump_r, jump_i
        totals[z, :, 0:flat], totals[z, :, flat:2 * flat] = sum_r, sum_i
        spread_out(1, "z", totals, 8 * flat, 1, lambda: at(clock[0], scan_all, 1.2))

    def scan_all():
        sum_r, sum_i = rows[0:1, :], rows[1:2, :]
        jump_r, jump_i = rows[10:11, :], rows[11:12, :]
        start_r, start_i = sum_r, sum_i
        for zz in range(SIDE):
            start_r, start_i = jnp.where(z == zz, sum_r, start_r), jnp.where(z == zz, sum_i, start_i)
            next_r, next_i = rotate(jump_r, jump_i, sum_r, sum_i)
            sum_r = next_r + totals[zz, :, 0:flat]
            sum_i = next_i + totals[zz, :, flat:2 * flat]
        final_half[odd["y"], 0] = as_table(sum_r)
        final_half[odd["y"], 1] = as_table(sum_i)
        hand_over(
            4, "y", final_half.at[odd["y"]], final_half.at[odd["y"]], final_half.at[1 - odd["y"]],
            8 * flat, store_final,
        )
        lead_r, lead_i = rotate(rows[8:9, :], rows[9:10, :], start_r, start_i)
        entry_r, entry_i = lead_r + rows[6:7, :], lead_i + rows[7:8, :]
        next_r, next_i = rotate(power_r[end, :], power_i[end, :], entry_r, entry_i)
        entries = ((entry_r, entry_i), (next_r + rows[12:13, :], next_i + rows[13:14, :]))
        for b in (0, 1):
            into_r, into_i = entries[b]
            for j in range(flat // chunk):
                part = slice(j * chunk, (j + 1) * chunk)
                shift = slice(flat + j * chunk, flat + (j + 1) * chunk)
                state_r, state_i = rotate(
                    power_r[:, part], power_i[:, part],
                    summed[b, :, part] + into_r[:, part], summed[b, :, shift] + into_i[:, part],
                )
                states[b, :, part] = state_r.astype(BF)
                states[b, :, shift] = state_i.astype(BF)
        answer = lax.dot_general(
            states[...].reshape(2 * length, 2 * flat), emit[...], NT, preferred_element_type=F32
        )
        direct = skip_gain[:, lanes_from(odd["y"], part_width)]
        answer = answer + direct * feed_block[...].reshape(2 * length, part_width).astype(F32)
        act_all[odd["y"], t] = jax.nn.gelu(answer).astype(BF).reshape(2, length, part_width)
        exchange(
            4, 5, "y", act_all, lambda: (state_far(), state_own()),
            lambda own: state_own() if own else state_far(),
        )

    def store_final():
        for half in (0, 1):
            load(
                "final" + str(half), final_half.at[half],
                final_out.at[:, pl.ds(half * groups, groups)],
            )

    def exchange(number, pair, axis, blocks, shared, relayed):
        amount = 2 * length * part_width * 2
        mine = odd[axis]

        def relay_block(i):
            sent_block, got_block = (mine, 1 - mine) if i == 0 else (1 - mine, mine)
            hand_over(
                pair + i, axis, blocks.at[mine, t, sent_block], blocks.at[mine, t, sent_block],
                blocks.at[1 - mine, t, got_block], amount / 2,
                lambda: share(
                    number + 1 + i, lambda c: blocks.at[1 - mine, c, got_block], amount / 2,
                    lambda: relayed(i),
                ),
            )

        relay_block(0)
        relay_block(1)
        share(number, lambda c: blocks.at[mine, c], amount, shared)

    edge = halo.shape[1]
    kernel_size = conv_taps.shape[0]

    def gate(i):
        pair = project_in(i, wc1)
        return (pair[:, 0:part_width] * jax.nn.sigmoid(pair[:, part_width:width])).astype(BF)

    def gate_own():
        gated_block[odd["z"]] = gate(0)
        gate_ready()

    def gate_far():
        for wait in owed["z"]:
            wait()
        gated_block[1 - odd["z"]] = gate(2)
        gate_ready()

    c1_own = when_all(1, lambda: at(clock[0], gate_own, 1.0))
    c1_far = when_all(3, lambda: at(clock[0], gate_far, 1.0))
    gate_ready = both(lambda: at(clock[0], pass_edge, 0.1))
    last = pl.ds(length - edge, edge)

    def pass_edge():
        for b, to, slot in (
            (0, beside("y", 1), at_end),
            (1, following, 1 - at_end),
        ):
            start(
                remote(
                    gated_block.at[b, last], halo.at[slot], halo_sem.at[b], halo_sem.at[2 + slot], to
                )
            )
        at(transit(("y", 1), 2 * edge * part_width * 2), convolve, 1.0)
        for b in (0, 1):
            padded[b, edge:edge + length, :] = gated_block[b].astype(F32)

    def convolve():
        for slot in (0, 1):
            bytes_of(halo.at[slot], halo_sem.at[2 + slot])
        padded[0, 0:edge, :] = jnp.where(z // 2 + y > 0, halo[0].astype(F32), 0.0)
        padded[1, 0:edge, :] = halo[1].astype(F32)
        taps = conv_taps[:, lanes_from(odd["z"], part_width)]
        lag = edge - (kernel_size - 1)
        for block in (0, 1):
            answer = jnp.zeros((length, part_width), F32)
            for b in range(8):
                tall = length + (8 if b else 0)
                part = jnp.zeros((tall, part_width), F32)
                for a in range(edge // 8 + 1):
                    k = 8 * a + b - lag
                    if 0 <= k < kernel_size:
                        part = part + taps[k:k + 1, :] * padded[block, 8 * a:8 * a + tall, :]
                if b:
                    shifted[b, :, :] = part
                    answer = answer + shifted[b, b:b + length, :]
                else:
                    answer = answer + part
            conv_all[odd["z"], t, block] = answer.astype(BF)
        exchange(
            7, 8, "z", conv_all, lambda: (norm_far(), norm_own()),
            lambda own: norm_own() if own else norm_far(),
        )

    def channel_norm(which, own):
        count = 2 * CHIPS * width
        def body(i, carry):
            part = pl.ds(pl.multiple_of(i * 16, 16), 16)
            pieces = [
                conv_all[c % 2, c // 2, which, part, :].astype(F32) for c in range(4 * CHIPS)
            ]
            total = pieces[0]
            for piece in pieces[1:]:
                total = total + piece
            mean = jnp.sum(total, axis=1, keepdims=True) / count
            pieces = [piece - mean for piece in pieces]
            total = pieces[0] * pieces[0]
            for piece in pieces[1:]:
                total = total + piece * piece
            scale = lax.rsqrt(jnp.sum(total, axis=1, keepdims=True) / count + 1e-5)
            for c, piece in enumerate(pieces):
                lanes = slice(c * part_width, (c + 1) * part_width)
                value = piece * scale * chan_gain[:, lanes] + chan_shift[:, lanes]
                half = slice(c % 2 * part_width, (c % 2 + 1) * part_width)
                conv_act[which, c // 2, part, half] = jax.nn.silu(value).astype(BF)
            return carry
        lax.fori_loop(0, length // 16, body, 0, unroll=2)
        (conv_own if own else conv_far)()

    norm_own = both(lambda: at(clock[0], lambda: channel_norm(odd["z"], True), 1.5))
    norm_far = both(lambda: at(clock[0], lambda: channel_norm(1 - odd["z"], False), 1.5))

    def project(piece, weights):
        count = weights.shape[3]
        total = None
        for c in range(2 * CHIPS):
            term = jnp.dot(piece(c), weights[c].reshape(width, count), preferred_element_type=F32)
            total = term if total is None else total + term
        return total

    def state_out(i):
        pair = project(
            lambda c: jnp.concatenate([act_all[0, c, i], act_all[1, c, i]], axis=1), ws2
        )
        return pair[:, 0:part_columns] * jax.nn.sigmoid(pair[:, part_columns:columns])

    def state_out_own():
        state_half[odd["y"]] = state_out(odd["y"])
        finish_ready()

    def state_out_far():
        state_back[...] = state_out(1 - odd["y"]).astype(BF)
        hand_over(
            10, "y", state_back, state_got, state_got, length * part_columns * 2, state_returned
        )

    def state_returned():
        state_half[1 - odd["y"]] = state_got[...].astype(F32)
        finish_ready()

    def conv_out_own():
        conv_half[odd["z"]] = project(lambda c: conv_act[odd["z"], c], wc2)
        finish_ready()

    def conv_out_far():
        conv_back[...] = project(lambda c: conv_act[1 - odd["z"], c], wc2).astype(BF)
        hand_over(11, "z", conv_back, conv_got, conv_got, length * part_columns * 2, conv_returned)

    def conv_returned():
        conv_half[1 - odd["z"]] = conv_got[...].astype(F32)
        finish_ready()

    state_own = when_all(3, lambda: at(clock[0], state_out_own, 1.0))
    state_far = when_all(3, lambda: at(clock[0], state_out_far, 1.0))
    conv_own = both(lambda: at(clock[0], conv_out_own, 0.6))
    conv_far = both(lambda: at(clock[0], conv_out_far, 0.6))
    finish_ready = when_all(4, lambda: at(clock[0], finish, 0.5))

    def finish():
        for half in (0, 1):
            lanes = slice(half * part_columns, (half + 1) * part_columns)
            result[:, lanes] = (state_half[half] + conv_half[half]).astype(BF)
        load("out", result, out)
        drain(1e9)
        for wait in closing:
            wait()
        after("final0")
        after("final1")
        after("out")

    run()


def settle(mixed, final, out, final_out):
    out[...] = mixed[...]
    final_out[...] = final[...]


def local(
    tokens, norm_gain, conv_value, conv_gate, state_feed, conv_taps, chan_gain, chan_shift,
    conv_project, decay_rate, frequency, input_real, input_imag, output_real, output_imag,
    skip_gain, state_value, state_gate, initial_state,
):
    length, features = tokens.shape
    groups, size, wide = input_real.shape
    flat, width = groups // 2 * size, groups * wide
    deep1, columns = conv_value.shape[0], conv_project.shape[1]
    deep2 = conv_project.shape[0]
    edge = 32
    args = (
        tokens, norm_gain.reshape(1, -1), conv_value, conv_gate, state_feed, conv_taps,
        chan_gain.reshape(1, -1), chan_shift.reshape(1, -1), conv_project, decay_rate, frequency,
        jnp.swapaxes(input_real, 1, 2), jnp.swapaxes(input_imag, 1, 2), output_real, output_imag,
        skip_gain.reshape(1, -1), state_value, state_gate, initial_state,
    )
    anywhere = pl.BlockSpec(memory_space=pl.ANY)
    vmem = pltpu.VMEM
    dma = pltpu.SemaphoreType.DMA
    many = 2 * CHIPS
    mixed, final = pl.pallas_call(
        kernel,
        out_shape=(
            jax.ShapeDtypeStruct((length, columns), BF),
            jax.ShapeDtypeStruct(initial_state.shape, F32),
        ),
        in_specs=[anywhere] * len(args),
        out_specs=(anywhere, anywhere),
        scratch_shapes=[
            *(vmem(args[i].shape, args[i].dtype) for i in SMALL),
            vmem((SIDE, SIDE, deep1, width // 2), BF),
            vmem((SIDE, SIDE, deep1, width), BF),
            vmem((SIDE, SIDE, deep2, columns), BF),
            vmem((SIDE, SIDE, deep2, columns // 2), BF),
            vmem((2, deep1, width // 2), BF),
            vmem((2, deep1, width), BF),
            vmem((2, deep2, columns), BF),
            vmem((2, deep2, columns // 2), BF),
            vmem((length, features), BF),
            vmem((length, 128), F32),
            vmem((3, many, length, features // many), BF),
            vmem((length, columns), BF),
            vmem((2, 2, groups // 2, size), F32),
            *(vmem((length, flat), F32) for _ in range(4)),
            vmem((width // 2, flat), BF),
            vmem((width // 2, flat), BF),
            vmem((width // 2, 2 * flat), BF),
            vmem((2, length, 2 * flat), BF),
            vmem((2, length, 2 * flat), F32),
            vmem((2, length, 2 * flat), BF),
            vmem((16, flat), F32),
            vmem((SIDE // 2, 1, 2 * flat), F32),
            vmem((SIDE, 1, 2 * flat), F32),
            vmem((2, length, width // 2), BF),
            vmem((2, length, width // 2), BF),
            vmem((2, edge, width // 2), BF),
            vmem((2, edge + length, width // 2), F32),
            vmem((8, length + 8, width // 2), F32),
            vmem((2, many, 2, length, width // 2), BF),
            vmem((2, many, 2, length, width // 2), BF),
            vmem((2, many, length, width), BF),
            *(
                vmem(shape, held)
                for _ in range(2)
                for shape, held in (
                    ((2, length, columns // 2), F32),
                    ((length, columns // 2), BF),
                    ((length, columns // 2), BF),
                )
            ),
            dma((20,)),
            dma((4,)),
            dma((4, 23)),
            dma((2,)),
            dma((2,)),
            dma((4,)),
            dma((10,)),
            dma((10, 4)),
            dma((12,)),
            dma((12,)),
            dma((4,)),
            dma((4, 2)),
        ],
        compiler_params=pltpu.CompilerParams(
            collective_id=0, has_side_effects=True, vmem_limit_bytes=62 * 1024 * 1024
        ),
        name="mixer",
    )(*args)
    return pl.pallas_call(
        settle,
        out_shape=(
            jax.ShapeDtypeStruct(mixed.shape, mixed.dtype),
            jax.ShapeDtypeStruct(final.shape, final.dtype),
        ),
        in_specs=[pl.BlockSpec(memory_space=vmem)] * 2,
        out_specs=(pl.BlockSpec(memory_space=vmem),) * 2,
        name="settle",
    )(mixed, final)


def solution(mesh):
    in_specs = (
        P("sp", None), P(), P("sp", "tp"), P("sp", "tp"), P("sp", "tp"), P(None, "tp"), P(), P(),
        P("sp", "tp"), P("tp", None), P("tp", None), P("tp", None, None), P("tp", None, None),
        P("tp", None, None), P("tp", None, None), P("tp"), P("sp", "tp"), P("sp", "tp"),
        P(None, "tp", None),
    )
    out_specs = (P("sp", "tp"), P(None, "tp", None))
    return jax.shard_map(local, mesh=mesh, in_specs=in_specs, out_specs=out_specs, check_vma=False)
```

```python
import heapq

import jax
import jax.numpy as jnp
from jax import lax
from jax.experimental import pallas as pl
from jax.experimental.pallas import tpu as pltpu
from jax.sharding import PartitionSpec as P

BF, F32 = jnp.bfloat16, jnp.float32
HIGHEST = lax.Precision.HIGHEST
MESH = pl.DeviceIdType.MESH
SIDE = 8
WINDOW = (3, 2, 3, 3)
WHEN = (24.0, 30.0, 2.0)
CLASSES = ((0,), (1, 7, 2, 6), (3, 5, 4))
CHIPS = 4
NT = (((1,), (1,)), ((), ()))


def hops(direction, half):
    return SIDE // 2 if (direction > 0) == (half == 0) else SIDE // 2 - 1


def slot_of(direction, half, k):
    return k if direction > 0 else hops(1, half) + k


def rotate(first_real, first_imag, second_real, second_imag):
    return (
        first_real * second_real - first_imag * second_imag,
        first_real * second_imag + first_imag * second_real,
    )


def iota(shape, dim):
    return lax.broadcasted_iota(jnp.int32, shape, dim)


SMALL = (1, 5, 6, 7, 9, 10, 11, 12, 13, 14, 15, 18)


def kernel(*refs):
    (
        tokens, norm_gain, conv_value, conv_gate, state_feed, conv_taps, chan_gain, chan_shift,
        conv_project, decay_rate, frequency, input_real, input_imag, output_real, output_imag,
        skip_gain, state_value, state_gate, initial_state, out, final_out,
    ) = refs[:21]
    small = refs[21:21 + len(SMALL)]
    (
        ws1, wc1, ws2, wc2, stage_s1, stage_c1, stage_s2, stage_c2, raw, scale, normed, result,
        final_half, power_r, power_i, undo_r, undo_i, drive_r, drive_i, emit, scaled, summed,
        states, rows, finals, totals, feed_block, gated_block, halo, padded,
        shifted, conv_all, act_all, conv_act, state_half, state_back, state_got, conv_half, conv_back,
        conv_got,
        load_sem, ring_send, ring_recv, scan_send, scan_recv, halo_sem, tp_send, tp_recv, pair_send,
        pair_recv, deal_send, deal_recv,
    ) = refs[21 + len(SMALL):]
    seq = lax.axis_index("sp")
    t = lax.axis_index("tp")
    z, y = seq // SIDE, seq % SIDE
    chip, core = t // 2, t % 2
    length = tokens.shape[0]
    groups, wide, size = input_real.shape
    width = groups * wide
    part_width = width // 2
    groups = groups // 2
    flat = groups * size
    columns = out.shape[1]
    part_columns = columns // 2

    def device(zz, yy, tt):
        return {"sp": zz * SIDE + yy, "tp": tt}

    def step_to(at, by, count):
        return lax.rem(at + by + count, count)

    def remote(src, dst, send, recv, to):
        return pltpu.make_async_remote_copy(
            src_ref=src, dst_ref=dst, send_sem=send, recv_sem=recv, device_id=to, device_id_type=MESH
        )

    queue = []
    sent = []
    free = {}
    clock = [0.0, 0]

    def at(time, fn, cost=0.0):
        heapq.heappush(queue, (time, clock[1], cost, fn))
        clock[1] += 1

    def run():
        while queue:
            time, _, cost, fn = heapq.heappop(queue)
            clock[0] = max(clock[0], time)
            fn()
            clock[0] += cost

    def start(moving):
        moving.start()
        sent.append((clock[0], moving))

    closing = []

    def drain(before):
        kept = []
        for time, moving in sent:
            if time < before:
                moving.wait_send()
            else:
                kept.append((time, moving))
        sent[:] = kept

    def transit(link, size, count=1, rate=50e3):
        begin = max(clock[0], free.get(link, 0.0))
        free[link] = begin + size * count / rate
        fixed = 1.5 if link == "core" else 4.0 if link[0] == "x" else 2.9
        return free[link] + fixed + 0.6 * (count - 1)

    def when_all(number, fn):
        left = [number]

        def one():
            left[0] -= 1
            if left[0] == 0:
                fn()
        return one

    loads, counted = {}, []

    def load(name, src, dst):
        if name not in counted:
            counted.append(name)
        moving = pltpu.make_async_copy(src, dst, load_sem.at[counted.index(name)])
        moving.start()
        loads[name] = moving

    def bytes_of(ref, sem):
        pltpu.make_async_copy(ref, ref, sem).wait()

    def after(name, three=None):
        if three is None:
            loads[name].wait()
        else:
            bytes_of(three, load_sem.at[counted.index(name)])

    here = {"z": z, "y": y}
    odd = {"z": z % 2, "y": y % 2}

    def lanes_from(half, count):
        return pl.ds(pl.multiple_of(half * count, count), count)

    def staged(name, axis, pieces, stage, own, count):
        for half in (0, 1):
            for i, source in enumerate(pieces):
                load(
                    name, source.at[:, half * count:(half + 1) * count],
                    stage.at[half, :, i * count:(i + 1) * count],
                )
        for i, source in enumerate(pieces):
            load(
                name, source.at[:, lanes_from(odd[axis], count)], own.at[:, i * count:(i + 1) * count]
            )

    staged("s1", "y", (state_feed,), stage_s1, ws1.at[z, y], part_width)
    staged("c1", "z", (conv_value, conv_gate), stage_c1, wc1.at[z, y], part_width)
    load("raw", tokens, raw)
    for i, place in enumerate(SMALL):
        load(place, refs[place], small[i])
    (
        norm_gain, conv_taps, chan_gain, chan_shift, decay_rate, frequency, input_real, input_imag,
        output_real, output_imag, skip_gain, initial_state,
    ) = small
    staged("s2", "y", (state_value, state_gate), stage_s2, ws2.at[z, y], part_columns)
    staged("c2", "z", (conv_project,), stage_c2, wc2.at[z, y], part_columns)

    barrier = pltpu.get_barrier_semaphore()
    at_end, at_start = y // (SIDE - 1), (SIDE - 1 - y) // (SIDE - 1)
    following = device(step_to(z, 2 * at_end, SIDE), step_to(y, 1, SIDE), t)
    preceding = device(step_to(z, -2 * at_start, SIDE), step_to(y, -1, SIDE), t)
    partners = []
    for d in range(1, SIDE):
        partners.append(device(z, step_to(y, d, SIDE), t))
        partners.append(device(step_to(z, d, SIDE), y, t))
    for d in range(1, 2 * CHIPS):
        partners.append(device(z, y, step_to(t, d, 2 * CHIPS)))
    partners.append(following)
    partners.append(preceding)
    for partner in partners:
        pl.semaphore_signal(barrier, inc=1, device_id=partner, device_id_type=MESH)
    def row_scales():
        after("raw")
        def body(i, carry):
            part = pl.ds(pl.multiple_of(i * 16, 16), 16)
            value = raw[part, :].astype(F32)
            mean = jnp.mean(value * value, axis=1, keepdims=True)
            scale[part, :] = jnp.broadcast_to(lax.rsqrt(mean + 1e-6), (16, 128))
            return carry
        lax.fori_loop(0, length // 16, body, 0, unroll=2)

    row_scales()
    pl.semaphore_wait(barrier, len(partners))

    def beside(axis, by):
        moved = step_to(here[axis], by, SIDE)
        return device(moved, y, t) if axis == "z" else device(z, moved, t)

    def spread_out(number, axis, blocks, size, stride, done):
        position = here[axis] // stride
        all_others = blocks.at[pl.ds(0, SIDE // stride - 1)]
        latest = 0.0
        for d in (4, 3, 5, 2, 6, 1, 7):
            if d % stride == 0:
                remote(
                    blocks.at[position], blocks.at[position], scan_send.at[number],
                    scan_recv.at[number], beside(axis, d),
                ).start()
                direction, count = (1, d) if d <= SIDE // 2 else (-1, SIDE - d)
                latest = max(latest, transit((axis, direction), size, count))

        def arrived():
            bytes_of(all_others, scan_recv.at[number])
            done()
        at(latest, arrived)
        closing.append(lambda: bytes_of(all_others, scan_send.at[number]))

    def trains(number, axis, across, stage, block, several, size, window, done, nearly=None):
        position, lane = here[axis], here[across]
        members = [
            (which, direction, k)
            for which in range(len(CLASSES)) for direction in (1, -1) for k in range(SIDE // 2)
            if any(k < hops(direction, d % 2) for d in CLASSES[which])
        ]
        finished = when_all(len(members), done)
        passed = when_all(len(CLASSES), nearly or (lambda: None))
        ready, active = [], [0]
        left = [len(c) * (SIDE - 1) for c in CLASSES]

        def dealt(d, source, to):
            half = odd[across] if d % 2 == 0 else 1 - odd[across]
            return remote(
                stage.at[half], block(position, source), deal_send.at[number],
                deal_recv.at[number, int(d in CLASSES[-1])], to,
            )

        def slot(which, direction, k):
            return members.index((which, direction, k))

        def copy(which, d, direction, k, source):
            held = block(source, step_to(lane, -d, SIDE))
            return remote(
                held, held, ring_send.at[number], ring_recv.at[number, slot(which, direction, k)],
                beside(axis, direction),
            )

        def send(which, direction, k):
            time = 0.0
            for d in CLASSES[which]:
                if k < hops(direction, d % 2):
                    copy(which, d, direction, k, step_to(position, -direction * k, SIDE)).start()
                    time = transit((axis, direction), size)
                    left[which] -= 1
            at(time, lambda: arrived(which, direction, k))
            if left[which] == 0:
                active[0] -= 1
                passed()

        def arrived(which, direction, k):
            count = sum(k < hops(direction, d % 2) for d in CLASSES[which])
            bytes_of(several(count), ring_recv.at[number, slot(which, direction, k)])
            if any(k + 1 < hops(direction, d % 2) for d in CLASSES[which]):
                send(which, direction, k + 1)
                inject()
            finished()

        def inject():
            while ready and active[0] < window[0]:
                which = ready.pop(0)
                active[0] += 1
                for direction in (1, -1):
                    send(which, direction, 0)

        def received(which):
            count = len(CLASSES[2]) if which else SIDE - 1 - len(CLASSES[2])
            bytes_of(several(count), deal_recv.at[number, which])
            ready.extend([2] if which else list(range(1, len(CLASSES) - 1)))
            inject()

        def deal():
            for which, members_of in enumerate(((1, 7, 2, 6), CLASSES[-1])):
                time = 0.0
                for d in members_of:
                    dealt(d, lane, beside(across, d)).start()
                    direction, count = (1, d) if d <= SIDE // 2 else (-1, SIDE - d)
                    time = max(time, transit((across, direction), size, count))
                at(time, lambda which=which: received(which))
            ready.insert(0, 0)
            inject()

        def go(amount):
            window[0] = amount
            inject()

        closing.append(lambda: bytes_of(block(pl.ds(0, SIDE - 1), pl.ds(0, SIDE)), ring_send.at[number]))
        closing.append(lambda: bytes_of(several(SIDE - 1), deal_send.at[number]))
        return deal, go

    def mate(axis):
        other_one = here[axis] + 1 - 2 * odd[axis]
        return device(other_one, y, t) if axis == "z" else device(z, other_one, t)

    def hand_over(number, axis, src, dst, landing, size, done):
        start(remote(src, dst, pair_send.at[number], pair_recv.at[number], mate(axis)))
        time = 0.6 + max(transit((axis, 1), size), transit((axis, -1), size))

        def arrived():
            remote(src, landing, pair_send.at[number], pair_recv.at[number], mate(axis)).wait_recv()
            done()
        at(time, arrived)

    other = t + 1 - 2 * core

    def share(number, block, size, done, later=None):
        near_sem = tp_recv.at[number, 0]

        def copy(slot, source, to):
            return remote(
                block(source), block(source), tp_send.at[number], tp_recv.at[number, slot],
                device(z, y, to),
            )

        def near():
            if later is None:
                bytes_of(block(pl.ds(0, CHIPS)), near_sem)
            else:
                later.append(lambda: bytes_of(block(pl.ds(0, CHIPS)), near_sem))
            done()

        latest = [0.0]
        all_near = when_all(4, lambda: at(latest[0], near))

        def to_core(source):
            copy(0, source, other).start()
            latest[0] = max(latest[0], transit("core", size, 1, 200e3))
            all_near()

        def far(d):
            source = step_to(chip, -d, CHIPS) * 2 + core
            copy(d, source, source).wait_recv()
            to_core(source)

        for d in (1, 3, 2):
            copy(d, t, step_to(chip, d, CHIPS) * 2 + core).start()
            if d == 2:
                time = 0.6 + max(transit(("x", hop), size) for hop in (1, -1))
            else:
                time = transit(("x", 2 - d), size)
            at(time, lambda d=d: far(d))
        to_core(t)
        closing.append(lambda: bytes_of(block(pl.ds(0, 2 * CHIPS - 1)), tp_send.at[number]))

    unit1 = ws1.shape[2] * part_width * 2

    def both(fn):
        return when_all(2, fn)

    deal_s1, _ = trains(
        0, "z", "y", stage_s1, lambda r, p: ws1.at[r, p], lambda n: ws1.at[0, pl.ds(0, n)], unit1, [WINDOW[0]],
        lambda: (s1_far(), s1_own()), lambda: go_s2(WINDOW[1]),
    )
    deal_c1, _ = trains(
        1, "y", "z", stage_c1, lambda r, p: wc1.at[p, r], lambda n: wc1.at[pl.ds(0, n), 0], 2 * unit1, [WINDOW[2]],
        lambda: (c1_far(), c1_own()), lambda: go_c2(WINDOW[3]),
    )
    deal_s2, go_s2 = trains(
        2, "z", "y", stage_s2, lambda r, p: ws2.at[r, p], lambda n: ws2.at[0, pl.ds(0, n)], 2 * unit1, [0],
        lambda: (state_own(), state_far()),
    )
    deal_c2, go_c2 = trains(
        3, "y", "z", stage_c2, lambda r, p: wc2.at[p, r], lambda n: wc2.at[pl.ds(0, n), 0], unit1, [0],
        lambda: (conv_own(), conv_far()),
    )

    def begin():
        after("s1", ws1.at[0, pl.ds(0, 3)])
        deal_s1()
        after("c1", wc1.at[0, pl.ds(0, 3)])
        deal_c1()

    at(0.0, begin)
    at(WHEN[0], lambda: (after("s2", ws2.at[0, pl.ds(0, 3)]), deal_s2()))
    at(WHEN[1], lambda: (after("c2", wc2.at[0, pl.ds(0, 3)]), deal_c2()))

    step = normed.shape[3]

    def measure():
        for name in SMALL:
            after(name)
        normalise(t)
        swap(1, "y", lambda: s1_far())
        at(WHEN[2], lambda: swap(2, "z", lambda: c1_far()))

    owed = {"y": [], "z": []}

    def swap(i, axis, done):
        for half in (0, 1):
            number = 2 * i - 2 + half
            part = pl.ds(half * length // 2, length // 2)
            block = normed.at[i, t, part]
            hand_over(
                number, axis, normed.at[0, t, part], block, block, length * step,
                lambda number=number, part=part: share(
                    number, lambda c: normed.at[i, c, part], length * step, done, owed[axis]
                ),
            )

    def normalise(c):
        lanes = lanes_from(c, step)
        value = raw[:, lanes].astype(F32)
        normed[0, c] = (value * scale[:, 0:1] * norm_gain[:, lanes]).astype(BF)

    def normalise_all():
        def body(c, carry):
            pl.when(c != t)(lambda: normalise(c))
            return carry
        lax.fori_loop(0, 2 * CHIPS, body, 0)

    def spread():
        return ((iota((size, flat), 1) & (size - 1)) == iota((size, flat), 0)).astype(F32)

    def owner():
        return (iota((groups, flat), 1) // size) == iota((groups, flat), 0)

    def as_row(table):
        wide_table = jnp.dot(table, spread(), precision=HIGHEST, preferred_element_type=F32)
        return jnp.sum(jnp.where(owner(), wide_table, 0.0), axis=0, keepdims=True)

    def as_table(row):
        return lax.dot_general(
            jnp.where(owner(), row, 0.0), spread(), NT, precision=HIGHEST, preferred_element_type=F32
        )

    total_tokens = length * SIDE * SIDE

    own_groups = lanes_from(odd["y"], groups)

    def tables():
        rate = -as_row(decay_rate[own_groups, :]) / total_tokens
        turn = as_row(frequency[own_groups, :])
        rows[0:1, :] = as_row(initial_state[0, own_groups, :])
        rows[1:2, :] = as_row(initial_state[1, own_groups, :])
        magnitude = jnp.exp(rate)
        step_r = magnitude * jnp.cos(turn)
        step_i = magnitude * jnp.sin(turn)
        modulus = rate * rate + turn * turn
        lift = step_r - 1.0
        factor_r = (lift * rate + step_i * turn) / modulus
        factor_i = (step_i * rate - lift * turn) / modulus
        count = iota((8, flat), 0) + 1
        block_r, block_i = jnp.ones((8, flat), F32), jnp.zeros((8, flat), F32)
        square_r, square_i = step_r, step_i
        for place in range(4):
            chosen = ((count >> place) & 1) == 1
            next_r, next_i = rotate(block_r, block_i, square_r, square_i)
            block_r = jnp.where(chosen, next_r, block_r)
            block_i = jnp.where(chosen, next_i, block_i)
            if place < 3:
                square_r, square_i = rotate(square_r, square_i, square_r, square_i)
        rows[2:3, :], rows[3:4, :] = square_r, square_i
        rows[4:5, :], rows[5:6, :] = factor_r, factor_i

        def body(i, carry):
            now_r, now_i = carry
            part = pl.ds(pl.multiple_of(i * 8, 8), 8)
            power_r[part, :], power_i[part, :] = now_r, now_i
            inverse = 1.0 / (now_r * now_r + now_i * now_i)
            un_r, un_i = rotate(now_r * inverse, -now_i * inverse, rows[4:5, :], rows[5:6, :])
            undo_r[part, :], undo_i[part, :] = un_r, un_i
            return rotate(now_r, now_i, rows[2:3, :], rows[3:4, :])
        lax.fori_loop(0, length // 8, body, (block_r, block_i))

    def matrices():
        stretch = spread().astype(BF)
        def fill(source, sign, dest, lanes):
            for g in range(groups):
                copied = jnp.dot((sign * source[odd["y"] * groups + g]).astype(BF), stretch, preferred_element_type=F32)
                kept = iota((wide, flat), 1) // size == g
                dest[g * wide:(g + 1) * wide, lanes] = jnp.where(kept, copied, 0.0).astype(BF)
        fill(input_real, 1.0, drive_r, slice(0, flat))
        fill(input_imag, 1.0, drive_i, slice(0, flat))
        fill(output_real, 1.0, emit, slice(0, flat))
        fill(output_imag, -1.0, emit, slice(flat, 2 * flat))

    at(0.3, measure, 0.2)
    at(6.0, normalise_all, 1.5)
    at(8.0, tables, 1.4)
    at(9.0, matrices, 1.2)

    chunk = 256

    def project_in(i, weights):
        count = weights.shape[3]
        total = None
        for c in range(2 * CHIPS):
            term = jnp.dot(normed[i, c], weights[c].reshape(step, count), preferred_element_type=F32)
            total = term if total is None else total + term
        return total

    def feed_own():
        feed_block[odd["y"]] = project_in(0, ws1).astype(BF)
        recur_ready()

    def feed_far():
        for wait in owed["y"]:
            wait()
        feed_block[1 - odd["y"]] = project_in(1, ws1).astype(BF)
        recur_ready()

    s1_own = when_all(1, lambda: at(clock[0], feed_own, 0.6))
    s1_far = when_all(3, lambda: at(clock[0], feed_far, 0.7))
    recur_ready = both(lambda: at(clock[0], recur, 0.8))
    end = slice(length - 1, length)

    def recur():
        drive = feed_block[...].reshape(2 * length, part_width)
        for j in range(flat // chunk):
            part = slice(j * chunk, (j + 1) * chunk)
            shift = slice(flat + j * chunk, flat + (j + 1) * chunk)
            push_r = jnp.dot(drive, drive_r[:, part], preferred_element_type=F32)
            push_i = jnp.dot(drive, drive_i[:, part], preferred_element_type=F32)
            for b in (0, 1):
                span = slice(b * length, (b + 1) * length)
                back_r, back_i = rotate(
                    undo_r[:, part], undo_i[:, part], push_r[span, :], push_i[span, :]
                )
                scaled[b, :, part] = back_r.astype(BF)
                scaled[b, :, shift] = back_i.astype(BF)
        lower = (iota((length, length), 0) >= iota((length, length), 1)).astype(BF)
        for b in (0, 1):
            for j in range(2 * flat // chunk):
                part = slice(j * chunk, (j + 1) * chunk)
                summed[b, :, part] = jnp.dot(lower, scaled[b, :, part], preferred_element_type=F32)
        span_r, span_i = power_r[end, :], power_i[end, :]
        first_r, first_i = rotate(span_r, span_i, summed[0, end, 0:flat], summed[0, end, flat:2 * flat])
        second_r, second_i = rotate(span_r, span_i, summed[1, end, 0:flat], summed[1, end, flat:2 * flat])
        rows[12:13, :], rows[13:14, :] = first_r, first_i
        moved_r, moved_i = rotate(span_r, span_i, first_r, first_i)
        finals[y // 2, :, 0:flat] = moved_r + second_r
        finals[y // 2, :, flat:2 * flat] = moved_i + second_i
        spread_out(0, "y", finals, 8 * flat, 2, lambda: at(clock[0], scan_row, 0.1))

    def scan_row():
        span_r, span_i = power_r[end, :], power_i[end, :]
        span_r, span_i = rotate(span_r, span_i, span_r, span_i)
        zero = jnp.zeros((1, flat), F32)
        sum_r, sum_i, before_r, before_i = zero, zero, zero, zero
        jump_r, jump_i = zero + 1.0, zero
        mine_r, mine_i = zero, zero
        for yy in range(SIDE // 2):
            here_now = y // 2 == yy
            before_r, before_i = jnp.where(here_now, sum_r, before_r), jnp.where(here_now, sum_i, before_i)
            mine_r, mine_i = jnp.where(here_now, jump_r, mine_r), jnp.where(here_now, jump_i, mine_i)
            next_r, next_i = rotate(span_r, span_i, sum_r, sum_i)
            sum_r = next_r + finals[yy, :, 0:flat]
            sum_i = next_i + finals[yy, :, flat:2 * flat]
            jump_r, jump_i = rotate(span_r, span_i, jump_r, jump_i)
        rows[6:7, :], rows[7:8, :] = before_r, before_i
        rows[8:9, :], rows[9:10, :] = mine_r, mine_i
        rows[10:11, :], rows[11:12, :] = jump_r, jump_i
        totals[z, :, 0:flat], totals[z, :, flat:2 * flat] = sum_r, sum_i
        spread_out(1, "z", totals, 8 * flat, 1, lambda: at(clock[0], scan_all, 1.2))

    def scan_all():
        sum_r, sum_i = rows[0:1, :], rows[1:2, :]
        jump_r, jump_i = rows[10:11, :], rows[11:12, :]
        start_r, start_i = sum_r, sum_i
        for zz in range(SIDE):
            start_r, start_i = jnp.where(z == zz, sum_r, start_r), jnp.where(z == zz, sum_i, start_i)
            next_r, next_i = rotate(jump_r, jump_i, sum_r, sum_i)
            sum_r = next_r + totals[zz, :, 0:flat]
            sum_i = next_i + totals[zz, :, flat:2 * flat]
        final_half[odd["y"], 0] = as_table(sum_r)
        final_half[odd["y"], 1] = as_table(sum_i)
        hand_over(
            4, "y", final_half.at[odd["y"]], final_half.at[odd["y"]], final_half.at[1 - odd["y"]],
            8 * flat, store_final,
        )
        lead_r, lead_i = rotate(rows[8:9, :], rows[9:10, :], start_r, start_i)
        entry_r, entry_i = lead_r + rows[6:7, :], lead_i + rows[7:8, :]
        next_r, next_i = rotate(power_r[end, :], power_i[end, :], entry_r, entry_i)
        entries = ((entry_r, entry_i), (next_r + rows[12:13, :], next_i + rows[13:14, :]))
        for b in (0, 1):
            into_r, into_i = entries[b]
            for j in range(flat // chunk):
                part = slice(j * chunk, (j + 1) * chunk)
                shift = slice(flat + j * chunk, flat + (j + 1) * chunk)
                state_r, state_i = rotate(
                    power_r[:, part], power_i[:, part],
                    summed[b, :, part] + into_r[:, part], summed[b, :, shift] + into_i[:, part],
                )
                states[b, :, part] = state_r.astype(BF)
                states[b, :, shift] = state_i.astype(BF)
        answer = lax.dot_general(
            states[...].reshape(2 * length, 2 * flat), emit[...], NT, preferred_element_type=F32
        )
        direct = skip_gain[:, lanes_from(odd["y"], part_width)]
        answer = answer + direct * feed_block[...].reshape(2 * length, part_width).astype(F32)
        act_all[odd["y"], t] = jax.nn.gelu(answer).astype(BF).reshape(2, length, part_width)
        exchange(
            4, 5, "y", act_all, lambda: (state_far(), state_own()),
            lambda own: state_own() if own else state_far(),
        )

    def store_final():
        for half in (0, 1):
            load(
                "final" + str(half), final_half.at[half],
                final_out.at[:, pl.ds(half * groups, groups)],
            )

    def exchange(number, pair, axis, blocks, shared, relayed):
        amount = 2 * length * part_width * 2
        mine = odd[axis]

        def relay_block(i):
            sent_block, got_block = (mine, 1 - mine) if i == 0 else (1 - mine, mine)
            hand_over(
                pair + i, axis, blocks.at[mine, t, sent_block], blocks.at[mine, t, sent_block],
                blocks.at[1 - mine, t, got_block], amount / 2,
                lambda: share(
                    number + 1 + i, lambda c: blocks.at[1 - mine, c, got_block], amount / 2,
                    lambda: relayed(i),
                ),
            )

        relay_block(0)
        relay_block(1)
        share(number, lambda c: blocks.at[mine, c], amount, shared)

    edge = halo.shape[1]
    kernel_size = conv_taps.shape[0]

    def gate(i):
        pair = project_in(i, wc1)
        return (pair[:, 0:part_width] * jax.nn.sigmoid(pair[:, part_width:width])).astype(BF)

    def gate_own():
        gated_block[odd["z"]] = gate(0)
        gate_ready()

    def gate_far():
        for wait in owed["z"]:
            wait()
        gated_block[1 - odd["z"]] = gate(2)
        gate_ready()

    c1_own = when_all(1, lambda: at(clock[0], gate_own, 1.0))
    c1_far = when_all(3, lambda: at(clock[0], gate_far, 1.0))
    gate_ready = both(lambda: at(clock[0], pass_edge, 0.1))
    last = pl.ds(length - edge, edge)

    def pass_edge():
        for b, to, slot in (
            (0, beside("y", 1), at_end),
            (1, following, 1 - at_end),
        ):
            start(
                remote(
                    gated_block.at[b, last], halo.at[slot], halo_sem.at[b], halo_sem.at[2 + slot], to
                )
            )
        at(transit(("y", 1), 2 * edge * part_width * 2), convolve, 1.0)
        for b in (0, 1):
            padded[b, edge:edge + length, :] = gated_block[b].astype(F32)

    def convolve():
        for slot in (0, 1):
            bytes_of(halo.at[slot], halo_sem.at[2 + slot])
        padded[0, 0:edge, :] = jnp.where(z // 2 + y > 0, halo[0].astype(F32), 0.0)
        padded[1, 0:edge, :] = halo[1].astype(F32)
        taps = conv_taps[:, lanes_from(odd["z"], part_width)]
        lag = edge - (kernel_size - 1)
        for block in (0, 1):
            answer = jnp.zeros((length, part_width), F32)
            for b in range(8):
                tall = length + (8 if b else 0)
                part = jnp.zeros((tall, part_width), F32)
                for a in range(edge // 8 + 1):
                    k = 8 * a + b - lag
                    if 0 <= k < kernel_size:
                        part = part + taps[k:k + 1, :] * padded[block, 8 * a:8 * a + tall, :]
                if b:
                    shifted[b, :, :] = part
                    answer = answer + shifted[b, b:b + length, :]
                else:
                    answer = answer + part
            conv_all[odd["z"], t, block] = answer.astype(BF)
        exchange(
            7, 8, "z", conv_all, lambda: (norm_far(), norm_own()),
            lambda own: norm_own() if own else norm_far(),
        )

    def channel_norm(which, own):
        count = 2 * CHIPS * width
        def body(i, carry):
            part = pl.ds(pl.multiple_of(i * 16, 16), 16)
            pieces = [
                conv_all[c % 2, c // 2, which, part, :].astype(F32) for c in range(4 * CHIPS)
            ]
            total = pieces[0]
            for piece in pieces[1:]:
                total = total + piece
            mean = jnp.sum(total, axis=1, keepdims=True) / count
            pieces = [piece - mean for piece in pieces]
            total = pieces[0] * pieces[0]
            for piece in pieces[1:]:
                total = total + piece * piece
            scale = lax.rsqrt(jnp.sum(total, axis=1, keepdims=True) / count + 1e-5)
            for c, piece in enumerate(pieces):
                lanes = slice(c * part_width, (c + 1) * part_width)
                value = piece * scale * chan_gain[:, lanes] + chan_shift[:, lanes]
                half = slice(c % 2 * part_width, (c % 2 + 1) * part_width)
                conv_act[which, c // 2, part, half] = jax.nn.silu(value).astype(BF)
            return carry
        lax.fori_loop(0, length // 16, body, 0, unroll=4)
        (conv_own if own else conv_far)()

    norm_own = both(lambda: at(clock[0], lambda: channel_norm(odd["z"], True), 1.5))
    norm_far = both(lambda: at(clock[0], lambda: channel_norm(1 - odd["z"], False), 1.5))

    def project(piece, weights):
        count = weights.shape[3]
        total = None
        for c in range(2 * CHIPS):
            term = jnp.dot(piece(c), weights[c].reshape(width, count), preferred_element_type=F32)
            total = term if total is None else total + term
        return total

    def state_out(i):
        pair = project(
            lambda c: jnp.concatenate([act_all[0, c, i], act_all[1, c, i]], axis=1), ws2
        )
        return pair[:, 0:part_columns] * jax.nn.sigmoid(pair[:, part_columns:columns])

    def state_out_own():
        state_half[odd["y"]] = state_out(odd["y"])
        finish_ready()

    def state_out_far():
        state_back[...] = state_out(1 - odd["y"]).astype(BF)
        hand_over(
            10, "y", state_back, state_got, state_got, length * part_columns * 2, state_returned
        )

    def state_returned():
        state_half[1 - odd["y"]] = state_got[...].astype(F32)
        finish_ready()

    def conv_out_own():
        conv_half[odd["z"]] = project(lambda c: conv_act[odd["z"], c], wc2)
        finish_ready()

    def conv_out_far():
        conv_back[...] = project(lambda c: conv_act[1 - odd["z"], c], wc2).astype(BF)
        hand_over(11, "z", conv_back, conv_got, conv_got, length * part_columns * 2, conv_returned)

    def conv_returned():
        conv_half[1 - odd["z"]] = conv_got[...].astype(F32)
        finish_ready()

    state_own = when_all(3, lambda: at(clock[0], state_out_own, 1.0))
    state_far = when_all(3, lambda: at(clock[0], state_out_far, 1.0))
    conv_own = both(lambda: at(clock[0], conv_out_own, 0.6))
    conv_far = both(lambda: at(clock[0], conv_out_far, 0.6))
    finish_ready = when_all(4, lambda: at(clock[0], finish, 0.5))

    def finish():
        for half in (0, 1):
            lanes = slice(half * part_columns, (half + 1) * part_columns)
            result[:, lanes] = (state_half[half] + conv_half[half]).astype(BF)
        load("out", result, out)
        drain(1e9)
        for wait in closing:
            wait()
        after("final0")
        after("final1")
        after("out")

    run()


def settle(mixed, final, out, final_out):
    out[...] = mixed[...]
    final_out[...] = final[...]


def local(
    tokens, norm_gain, conv_value, conv_gate, state_feed, conv_taps, chan_gain, chan_shift,
    conv_project, decay_rate, frequency, input_real, input_imag, output_real, output_imag,
    skip_gain, state_value, state_gate, initial_state,
):
    length, features = tokens.shape
    groups, size, wide = input_real.shape
    flat, width = groups // 2 * size, groups * wide
    deep1, columns = conv_value.shape[0], conv_project.shape[1]
    deep2 = conv_project.shape[0]
    edge = 32
    args = (
        tokens, norm_gain.reshape(1, -1), conv_value, conv_gate, state_feed, conv_taps,
        chan_gain.reshape(1, -1), chan_shift.reshape(1, -1), conv_project, decay_rate, frequency,
        jnp.swapaxes(input_real, 1, 2), jnp.swapaxes(input_imag, 1, 2), output_real, output_imag,
        skip_gain.reshape(1, -1), state_value, state_gate, initial_state,
    )
    anywhere = pl.BlockSpec(memory_space=pl.ANY)
    vmem = pltpu.VMEM
    dma = pltpu.SemaphoreType.DMA
    many = 2 * CHIPS
    mixed, final = pl.pallas_call(
        kernel,
        out_shape=(
            jax.ShapeDtypeStruct((length, columns), BF),
            jax.ShapeDtypeStruct(initial_state.shape, F32),
        ),
        in_specs=[anywhere] * len(args),
        out_specs=(anywhere, anywhere),
        scratch_shapes=[
            *(vmem(args[i].shape, args[i].dtype) for i in SMALL),
            vmem((SIDE, SIDE, deep1, width // 2), BF),
            vmem((SIDE, SIDE, deep1, width), BF),
            vmem((SIDE, SIDE, deep2, columns), BF),
            vmem((SIDE, SIDE, deep2, columns // 2), BF),
            vmem((2, deep1, width // 2), BF),
            vmem((2, deep1, width), BF),
            vmem((2, deep2, columns), BF),
            vmem((2, deep2, columns // 2), BF),
            vmem((length, features), BF),
            vmem((length, 128), F32),
            vmem((3, many, length, features // many), BF),
            vmem((length, columns), BF),
            vmem((2, 2, groups // 2, size), F32),
            *(vmem((length, flat), F32) for _ in range(4)),
            vmem((width // 2, flat), BF),
            vmem((width // 2, flat), BF),
            vmem((width // 2, 2 * flat), BF),
            vmem((2, length, 2 * flat), BF),
            vmem((2, length, 2 * flat), F32),
            vmem((2, length, 2 * flat), BF),
            vmem((16, flat), F32),
            vmem((SIDE // 2, 1, 2 * flat), F32),
            vmem((SIDE, 1, 2 * flat), F32),
            vmem((2, length, width // 2), BF),
            vmem((2, length, width // 2), BF),
            vmem((2, edge, width // 2), BF),
            vmem((2, edge + length, width // 2), F32),
            vmem((8, length + 8, width // 2), F32),
            vmem((2, many, 2, length, width // 2), BF),
            vmem((2, many, 2, length, width // 2), BF),
            vmem((2, many, length, width), BF),
            *(
                vmem(shape, held)
                for _ in range(2)
                for shape, held in (
                    ((2, length, columns // 2), F32),
                    ((length, columns // 2), BF),
                    ((length, columns // 2), BF),
                )
            ),
            dma((20,)),
            dma((4,)),
            dma((4, 23)),
            dma((2,)),
            dma((2,)),
            dma((4,)),
            dma((10,)),
            dma((10, 4)),
            dma((12,)),
            dma((12,)),
            dma((4,)),
            dma((4, 2)),
        ],
        compiler_params=pltpu.CompilerParams(
            collective_id=0, has_side_effects=True, vmem_limit_bytes=62 * 1024 * 1024
        ),
        name="mixer",
    )(*args)
    return pl.pallas_call(
        settle,
        out_shape=(
            jax.ShapeDtypeStruct(mixed.shape, mixed.dtype),
            jax.ShapeDtypeStruct(final.shape, final.dtype),
        ),
        in_specs=[pl.BlockSpec(memory_space=vmem)] * 2,
        out_specs=(pl.BlockSpec(memory_space=vmem),) * 2,
        name="settle",
    )(mixed, final)


def solution(mesh):
    in_specs = (
        P("sp", None), P(), P("sp", "tp"), P("sp", "tp"), P("sp", "tp"), P(None, "tp"), P(), P(),
        P("sp", "tp"), P("tp", None), P("tp", None), P("tp", None, None), P("tp", None, None),
        P("tp", None, None), P("tp", None, None), P("tp"), P("sp", "tp"), P("sp", "tp"),
        P(None, "tp", None),
    )
    out_specs = (P("sp", "tp"), P(None, "tp", None))
    return jax.shard_map(local, mesh=mesh, in_specs=in_specs, out_specs=out_specs, check_vma=False)
```
